32 devices in a mesh: sp: 8 (over z, x), tp: 4 (over y, core).
Axes of the slice: x: 2, y: 2, z: 4, core: 2. Of those that a mesh axis runs over, the one named last changes fastest.
Arguments:
- query: bfloat16 [2048, 1024], P('sp', 'tp'), may hold values from -6 to 6
- forget_logits: bfloat16 [2048, 1024], P('sp', 'tp'), may hold values from -5.5 to 5.5
- written_values: bfloat16 [2048, 1024], P('sp', 'tp'), may hold values from -6 to 6
- output_gate_logits: bfloat16 [2048, 1024], P('sp', 'tp'), may hold values from -6 to 6
- forget_floor_gap: float32 [1024], P('tp'), may hold values from 0 to 0.08
- extra_log_decay: float32 [2048, 1024], P('sp', 'tp'), may hold values from -0.7 to 0
- head_norm_gain: float32 [128], replicated, may hold values from 0.1 to 1.9
- output_weight: bfloat16 [1024, 2048], P('tp'), may hold values from -0.1875 to 0.1875
- residual: bfloat16 [2048, 2048], P(('sp', 'tp')), may hold values from -6 to 6
- mixer_norm_gain: float32 [2048], replicated, may hold values from 0.1 to 1.9
- mixer_up_weight: bfloat16 [2048, 8192], P('sp', 'tp'), may hold values from -0.125 to 0.125
- mixer_down_weight: bfloat16 [8192, 2048], P(('tp', 'sp')), may hold values from -0.0625 to 0.0625
Outputs:
- layer_out: bfloat16 [2048, 2048], P(('sp', 'tp'))
The draws below stay inside these ranges and needn't reach their ends.
All inputs are finite; a program needn't handle non-finite values.
Results may differ from the reference program's by a relative error of at most 0.015.
Values may be sent and summed in bfloat16 or wider, within the bound.
No kernel may reach another device: no remote copies, remote signals or barrier semaphores. Data moves between devices by JAX's collectives and lax.ppermute only.
A program may use at most 128 MiB of HBM per device.

```python
import jax
import jax.numpy as jnp
from jax import lax

D = 2048
FF = 8192
HEADS = 8
HEAD_K = 128
HEAD_V = 128
BLOCK = 64
TOK_DEV = 256
WIDTH = 1024
SEQ = 2048
N_SP = 8


def draw_forget_logits(key, part):
    noise_key, offset_key = jax.random.split(key)
    jitter = jnp.clip(jax.random.normal(noise_key, (SEQ, WIDTH), jnp.float32), -4.0, 4.0)
    offsets = jax.random.uniform(offset_key, (SEQ // TOK_DEV, 1, 1), jnp.float32, -1.5, 1.5)
    shifted = jitter.reshape(SEQ // TOK_DEV, TOK_DEV, WIDTH) + offsets
    return shifted.reshape(SEQ, WIDTH).astype(jnp.bfloat16)


def draw_forget_floor_gap(key, part):
    choose_key, slow_key, fast_key = jax.random.split(key, 3)
    slow_share = 0.5
    slow_head = jax.random.uniform(choose_key, (HEADS, 1), jnp.float32) < slow_share
    slow_gap = jnp.exp(jax.random.uniform(slow_key, (HEADS, HEAD_K), jnp.float32, jnp.log(0.2 / SEQ), jnp.log(1.0 / SEQ)))
    fast_gap = jnp.exp(jax.random.uniform(fast_key, (HEADS, HEAD_K), jnp.float32, jnp.log(0.02), jnp.log(0.08)))
    return jnp.where(slow_head, slow_gap, fast_gap).reshape(WIDTH).astype(jnp.float32)


def draw_extra_log_decay(key, part):
    place_key, level_key = jax.random.split(key)
    places = jax.random.randint(place_key, (3,), 0, SEQ)
    levels = jnp.log(jax.random.uniform(level_key, (3, WIDTH), jnp.float32, 0.5, 0.8))
    positions = jnp.arange(SEQ)[:, None]
    summed = jnp.zeros((SEQ, WIDTH), jnp.float32)
    for number in range(3):
        summed = summed + jnp.where(positions == places[number], levels[number][None, :], 0.0)
    return summed


def shard_levels(key, dims, pieces, low, top_value):
    level = 1.0
    for axis_at, parts in pieces:
        steps = jax.random.uniform(jax.random.fold_in(jax.random.fold_in(key, 6), axis_at), (parts,), jnp.float32, low / len(pieces), top_value / len(pieces))
        level = level * jnp.repeat(jnp.exp(steps), dims[axis_at] // parts).reshape((-1,) + (1,) * (len(dims) - 1 - axis_at))
    return level


def centred(key, dims, scale, limit, cuts=(), kind=jnp.bfloat16):
    result = scale * jax.random.normal(key, dims, jnp.float32)
    if cuts:
        result = result * shard_levels(key, dims, cuts, -0.22, 0.18)
    return jnp.clip(result, -limit, limit).astype(kind)


def setup_inputs(seed: int = 0) -> dict:
    streams_of = jax.random.split(jax.random.key(seed), 13)
    query = centred(streams_of[0], (SEQ, WIDTH), 1.0, 6.0, ((0, 8), (1, 4)))
    forget_logits = draw_forget_logits(jax.random.fold_in(streams_of[12], 71), 0)
    written_values = centred(streams_of[2], (SEQ, WIDTH), 1.0, 6.0, ((0, 8), (1, 4)))
    output_gate_logits = centred(streams_of[3], (SEQ, WIDTH), 1.0, 6.0, ((0, 8), (1, 4)))
    forget_floor_gap = draw_forget_floor_gap(jax.random.fold_in(streams_of[12], 71), 0)
    extra_log_decay = draw_extra_log_decay(jax.random.fold_in(streams_of[12], 71), 0)
    head_norm_gain = jnp.clip(1.0 + 0.18 * jax.random.normal(streams_of[6], (HEAD_V,), jnp.float32), 0.1, 1.9)
    output_weight = centred(streams_of[7], (WIDTH, D), WIDTH ** -0.5, 0.1875, ((0, 4),))
    residual = centred(streams_of[8], (SEQ, D), 1.0, 6.0, ((0, 32),))
    mixer_norm_gain = jnp.clip(1.0 + 0.18 * jax.random.normal(streams_of[9], (D,), jnp.float32), 0.1, 1.9)
    mixer_up_weight = centred(streams_of[10], (D, FF), D ** -0.5, 0.125, ((0, 8), (1, 4)))
    mixer_down_weight = centred(streams_of[11], (FF, D), FF ** -0.5, 0.0625, ((0, 32),))
    return {"query": query, "forget_logits": forget_logits, "written_values": written_values, "output_gate_logits": output_gate_logits, "forget_floor_gap": forget_floor_gap, "extra_log_decay": extra_log_decay, "head_norm_gain": head_norm_gain, "output_weight": output_weight, "residual": residual, "mixer_norm_gain": mixer_norm_gain, "mixer_up_weight": mixer_up_weight, "mixer_down_weight": mixer_down_weight}


norm_eps = 1e-06
highest_precision = lax.Precision.HIGHEST

def block_update(carry_forward_state, block_inputs):
    query_rows_block, gate_rows_block, value_rows_block, log_block = block_inputs
    cumulative_log = jnp.cumsum(log_block, axis=1)
    length = query_rows_block.shape[1]
    causal = jnp.arange(length)[:, None] >= jnp.arange(length)[None, :]
    across_blocks = jnp.einsum('dcj,djw->dcw', query_rows_block * jnp.exp(cumulative_log), carry_forward_state, precision=highest_precision)
    spread = cumulative_log[:, :, None, :] - cumulative_log[:, None, :, :]
    decay_table = jnp.exp(jnp.where(causal[None, :, :, None], spread, -jnp.inf))
    scores = jnp.einsum('htk,hsk,htsk->hts', query_rows_block, gate_rows_block, decay_table, precision=highest_precision)
    within = jnp.einsum('hts,hsv->htv', scores, value_rows_block, precision=highest_precision)
    final_log_total = cumulative_log[:, -1:, :]
    updated_state = jnp.exp(final_log_total[:, 0, :])[:, :, None] * carry_forward_state + jnp.einsum('tri,trw->tiw', gate_rows_block * jnp.exp(final_log_total - cumulative_log), value_rows_block, precision=highest_precision)
    return (updated_state, across_blocks + within)

def to_blocks(array, inner):
    length = array.shape[0]
    split_up = array.reshape(length // BLOCK, BLOCK, array.shape[1] // inner, inner)
    return jnp.transpose(split_up, (0, 2, 1, 3))

def from_blocks(blocked):
    joined = jnp.transpose(blocked, (0, 2, 1, 3))
    return joined.reshape(joined.shape[0] * joined.shape[1], joined.shape[2], joined.shape[3])

def prepare_inputs(query, forget_logits, written_values, forget_floor_gap, extra_log_decay):
    input_gate_value = forget_floor_gap[None, :] * jax.nn.sigmoid(-forget_logits.astype(jnp.float32))
    forget_log_rate = jnp.log1p(-input_gate_value) + extra_log_decay
    scaled_values = query.astype(jnp.float32) * HEAD_K ** (-0.5)
    return (scaled_values, input_gate_value, written_values.astype(jnp.float32), forget_log_rate)

def gate_out(recurrent, output_gate_logits, head_norm_gain):
    normal_part = recurrent * lax.rsqrt(lax.optimization_barrier(jnp.mean(recurrent * recurrent, axis=-1, keepdims=True)) + norm_eps)
    gating = jax.nn.silu(output_gate_logits.astype(jnp.float32)).reshape(recurrent.shape)
    mixed = normal_part * head_norm_gain * gating
    return mixed.reshape(recurrent.shape[0], -1).astype(jnp.bfloat16)

def normalize(stream, gain):
    scaled_rows = stream * lax.rsqrt(lax.optimization_barrier(jnp.mean(stream * stream, axis=-1, keepdims=True)) + norm_eps)
    return (scaled_rows * gain).astype(jnp.bfloat16)

def reference(query, forget_logits, written_values, output_gate_logits, forget_floor_gap, extra_log_decay, head_norm_gain, output_weight, residual, mixer_norm_gain, mixer_up_weight, mixer_down_weight):
    scaled_values, input_gate_value, value_rows, forget_log_rate = prepare_inputs(query, forget_logits, written_values, forget_floor_gap, extra_log_decay)
    head_count = query.shape[1] // HEAD_K
    start_state = jnp.zeros((head_count, HEAD_K, HEAD_V), jnp.float32)
    final_state, blocked = lax.scan(block_update, start_state, (to_blocks(scaled_values, HEAD_K), to_blocks(input_gate_value, HEAD_K), to_blocks(value_rows, HEAD_V), to_blocks(forget_log_rate, HEAD_K)))
    mixed = gate_out(from_blocks(blocked), output_gate_logits, head_norm_gain)
    branch = jnp.dot(mixed, output_weight, preferred_element_type=jnp.float32)
    stream = residual.astype(jnp.float32) + branch

    def channel_mix(row_block):
        normed = normalize(row_block, mixer_norm_gain)
        lifted = jnp.dot(normed, mixer_up_weight, preferred_element_type=jnp.float32)
        hidden = jnp.square(jax.nn.relu(lifted)).astype(jnp.bfloat16)
        return (row_block + jnp.dot(hidden, mixer_down_weight, preferred_element_type=jnp.float32)).astype(jnp.bfloat16)
    mapped = lax.map(channel_mix, stream.reshape(N_SP, TOK_DEV, stream.shape[1]))
    return mapped.reshape(stream.shape)
```

```python
import jax
import jax.numpy as jnp
from jax import lax
from jax.experimental import pallas as pl
from jax.experimental.pallas import tpu as pltpu
from jax.sharding import PartitionSpec as P

HEAD = 128
SUB = 64
EPS = 1e-06
HI = lax.Precision.HIGHEST
AXES = ("sp", "tp")
F32 = jnp.float32
BF16 = jnp.bfloat16


def kernel_call(body, out_shape, scratch=(), smem=0, n_in=0, name=None):
    specs = [pl.BlockSpec(memory_space=pltpu.SMEM)] * smem
    specs += [pl.BlockSpec(memory_space=pltpu.VMEM)] * (n_in - smem)
    many = isinstance(out_shape, (list, tuple))
    out_spec = pl.BlockSpec(memory_space=pltpu.VMEM)
    return pl.pallas_call(
        body,
        out_shape=out_shape,
        in_specs=specs,
        out_specs=[out_spec] * len(out_shape) if many else out_spec,
        scratch_shapes=list(scratch),
        compiler_params=pltpu.CompilerParams(vmem_limit_bytes=56 * 1024 * 1024),
        name=name,
    )


def exact_parts(x):
    first = x.astype(BF16)
    rest = x - first.astype(F32)
    second = rest.astype(BF16)
    third = (rest - second.astype(F32)).astype(BF16)
    return first, second, third


def gates_body(logits, values, gap, extra, gate_out, cum_out, packed):
    rows, width = logits.shape
    heads = width // HEAD
    z = logits[...].astype(F32)
    gate = gap[...] / (1.0 + jnp.exp(z))
    log_forget = jnp.log1p(-gate) + extra[...]
    r = lax.broadcasted_iota(jnp.int32, (rows, rows), 0)
    c = lax.broadcasted_iota(jnp.int32, (rows, rows), 1)
    lower = (r >= c).astype(F32)
    cum = jnp.dot(lower, log_forget, precision=HI, preferred_element_type=F32)
    gate_out[...] = gate
    cum_out[...] = cum
    total = cum[rows - 1 : rows, :]
    keys = gate * jnp.exp(total - cum)
    vals = values[...].astype(F32)
    for h in range(heads):
        ks = keys[:, h * HEAD : (h + 1) * HEAD]
        vs = vals[:, h * HEAD : (h + 1) * HEAD]
        state = lax.dot_general(
            ks, vs, (((0,), (0,)), ((), ())), precision=HI, preferred_element_type=F32
        )
        packed[h * HEAD : (h + 1) * HEAD, :] = state.astype(BF16)
    lines = []
    for h in range(heads):
        lines += list(exact_parts(total[:, h * HEAD : (h + 1) * HEAD]))
    pad = 16 - len(lines)
    tail = jnp.concatenate([x.astype(F32) for x in lines] + [jnp.zeros((pad, HEAD), F32)], axis=0)
    packed[heads * HEAD :, :] = tail.astype(BF16)


def local_body(query, gate, cum, values, out):
    rows, width = query.shape
    sub = min(SUB, rows)
    for h in range(width // HEAD):
        lanes = slice(h * HEAD, (h + 1) * HEAD)
        for i in range(rows // sub):
            lo, hi = i * sub, (i + 1) * sub
            mid = cum[lo + sub // 2 - 1 : lo + sub // 2, lanes]
            qs = query[lo:hi, lanes].astype(F32) * (HEAD**-0.5) * jnp.exp(cum[lo:hi, lanes] - mid)
            ks = gate[0:hi, lanes] * jnp.exp(mid - cum[0:hi, lanes])
            scores = lax.dot_general(
                qs, ks, (((1,), (1,)), ((), ())), precision=HI, preferred_element_type=F32
            )
            rr = lax.broadcasted_iota(jnp.int32, (sub, hi), 0) + lo
            cc = lax.broadcasted_iota(jnp.int32, (sub, hi), 1)
            scores = jnp.where(rr >= cc, scores, 0.0)
            out[lo:hi, lanes] = jnp.dot(
                scores, values[0:hi, lanes].astype(F32), precision=HI, preferred_element_type=F32
            )


def mix_body(n_cores, *refs):
    place = refs[0]
    query, cum, local, gate_logits, gain, weight = refs[1:7]
    states = refs[7:-3]
    keep, away, mixed = refs[-3:]
    rows, width = query.shape
    heads = width // HEAD
    for h in range(heads):
        lanes = slice(h * HEAD, (h + 1) * HEAD)
        arrived = jnp.zeros((HEAD, HEAD), F32)
        passed = jnp.zeros((1, HEAD), F32)
        decays = []
        for s in states:
            decays.append(passed)
            parts = s[heads * HEAD :, :].astype(F32)
            for k in range(3):
                passed = passed + parts[3 * h + k : 3 * h + k + 1, :]
        for s, d in zip(states, decays):
            column = jnp.transpose(jnp.broadcast_to(jnp.exp(d), (HEAD, HEAD)))
            arrived = arrived + column * s[h * HEAD : (h + 1) * HEAD, :].astype(F32)
        reach = query[:, lanes].astype(F32) * (HEAD**-0.5) * jnp.exp(cum[:, lanes])
        rec = local[:, lanes] + jnp.dot(reach, arrived, precision=HI, preferred_element_type=F32)
        scale = lax.rsqrt(jnp.mean(rec * rec, axis=-1, keepdims=True) + EPS)
        v = gate_logits[:, lanes].astype(F32)
        mixed[:, lanes] = rec * scale * gain[...] * (v / (1.0 + jnp.exp(-v)))
    y, c = place[2], place[3]
    n_y = 2
    own = rows // (n_y * n_cores)
    picked = []
    for e in range(n_cores):
        for k in range(n_y):
            t = lax.rem(y + k, n_y) * n_cores + lax.rem(c + e, n_cores)
            picked.append(mixed[pl.ds(pl.multiple_of(t * own, own), own), :])
    ordered = jnp.concatenate(picked, axis=0).astype(BF16)
    part = jnp.dot(ordered, weight[...], preferred_element_type=F32)
    cut = n_y * own
    keep[...] = part[:cut]
    away[...] = part[cut:].astype(BF16)


def norm_body(own, arrived, residual, gain, stream_out, normed_out):
    stream = own[...] + arrived[...].astype(F32) + residual[...].astype(F32)
    stream_out[...] = stream
    scale = lax.rsqrt(jnp.mean(stream * stream, axis=-1, keepdims=True) + EPS)
    normed = (stream * scale * gain[...]).astype(BF16)
    blocks, _, cols = normed_out.shape
    for i in range(blocks):
        normed_out[i] = normed[:, i * cols : (i + 1) * cols]


def mixer_body(n_a, n_cores, *refs):
    n_tok = n_a * n_cores
    place = refs[0]
    toks = refs[1 : 1 + n_tok]
    ups = refs[1 + n_tok : 1 + n_tok + 4 * n_a]
    downs = refs[1 + n_tok + 4 * n_a : -4]
    keep, away, rows_x, hid = refs[-4:]
    a, b = place[0], place[1]
    blocks, own, cols = toks[0].shape
    n_b = 2
    for i in range(n_tok):
        for k in range(blocks):
            rows_x[k, i * own : (i + 1) * own, :] = toks[i][k]
    for y in range(2):
        acc = None
        for e in range(n_a):
            for x in range(n_b):
                k = lax.rem(a - e + n_a, n_a) * n_b + lax.rem(b + x, n_b)
                term = jnp.dot(
                    rows_x[k], ups[(y * n_b + x) * n_a + e][...], preferred_element_type=F32
                )
                acc = term if acc is None else acc + term
        act = jnp.maximum(acc, 0.0)
        act = (act * act).astype(BF16)
        half = act.shape[1] // n_b
        for x in range(n_b):
            hid[y * n_b + x] = act[:, x * half : (x + 1) * half]
    halves = len(downs) // 4
    acc = None
    for y in range(2):
        for x in range(n_b):
            h = hid[y * n_b + lax.rem(b + x, n_b)]
            step = h.shape[1] // halves
            for k in range(halves):
                term = jnp.dot(
                    h[:, k * step : (k + 1) * step],
                    downs[(y * n_b + x) * halves + k][...],
                    preferred_element_type=F32,
                )
                acc = term if acc is None else acc + term
    cut = n_a * own
    keep[...] = acc[:cut]
    away[...] = acc[cut:].astype(BF16)


def solution(mesh):
    n_sp, n_tp = mesh.shape["sp"], mesh.shape["tp"]
    n_b, n_y = 2, 2
    n_a, n_c = n_sp // n_b, n_tp // n_y

    def flat(a, b, y, c):
        return (a % n_a * n_b + b % n_b) * n_tp + y % n_y * n_c + c % n_c

    def send(x, a=0, b=0, y=0, c=0):
        pairs = [
            (flat(i, j, k, m), flat(i + a, j + b, k + y, m + c))
            for i in range(n_a)
            for j in range(n_b)
            for k in range(n_y)
            for m in range(n_c)
        ]
        return lax.ppermute(x, AXES, pairs)

    def later(x, d):
        pairs = [
            (s * n_tp + t, (s + d) * n_tp + t) for s in range(n_sp - d) for t in range(n_tp)
        ]
        return lax.ppermute(x, AXES, pairs)

    def on_device(
        query,
        forget_logits,
        written_values,
        output_gate_logits,
        forget_floor_gap,
        extra_log_decay,
        head_norm_gain,
        output_weight,
        residual,
        mixer_norm_gain,
        mixer_up_weight,
        mixer_down_weight,
    ):
        sp, tp = lax.axis_index("sp"), lax.axis_index("tp")
        a, b, y, c = sp // n_b, sp % n_b, tp // n_c, tp % n_c
        place = jnp.stack([a, b, y, c]).astype(jnp.int32)
        rows, width = query.shape
        model = output_weight.shape[1]
        own = residual.shape[0]
        heads = width // HEAD

        up_rows, up_cols = mixer_up_weight.shape
        piece = up_cols // n_a
        mine = []
        for d in range(n_a):
            cut = lax.dynamic_slice(mixer_up_weight, (0, (a + d) % n_a * piece), (up_rows, piece))
            mine.append(cut if d == 0 else send(cut, a=d))
        over_b = [send(u, b=1) for u in mine]
        over_y = [send(u, y=1) for u in mine]
        both = [
            send(over_y[e], b=1) if e % 2 else send(over_b[e], y=1) for e in range(n_a)
        ]
        ups = mine + over_b + over_y + both
        half = mixer_down_weight.shape[0] // 2
        down = [mixer_down_weight[:half], mixer_down_weight[half:]]
        down_b = [send(u, b=1) for u in down]
        down_y = [send(u, y=1) for u in down]
        down_by = [send(down_b[0], y=1), send(down_y[1], b=1)]
        downs = down + down_b + down_y + down_by

        packed_rows = heads * HEAD + 16
        gate, cum, packed = kernel_call(
            gates_body,
            [
                jax.ShapeDtypeStruct((rows, width), F32),
                jax.ShapeDtypeStruct((rows, width), F32),
                jax.ShapeDtypeStruct((packed_rows, HEAD), BF16),
            ],
            n_in=4,
            name="gates",
        )(forget_logits, written_values, forget_floor_gap[None, :], extra_log_decay)
        states = [later(packed, d) for d in range(1, n_sp)]
        local = kernel_call(
            local_body, jax.ShapeDtypeStruct((rows, width), F32), n_in=4, name="local"
        )(query, gate, cum, written_values)
        cut_rows = n_y * own
        keep, away = kernel_call(
            lambda *refs: mix_body(n_c, *refs),
            [
                jax.ShapeDtypeStruct((cut_rows, model), F32),
                jax.ShapeDtypeStruct((rows - cut_rows, model), BF16),
            ],
            scratch=[pltpu.VMEM((rows, width), F32)],
            smem=1,
            n_in=7 + len(states),
            name="mix",
        )(
            place,
            query,
            cum,
            local,
            output_gate_logits,
            head_norm_gain[None, :],
            output_weight,
            *states,
        )
        for e in range(1, n_c):
            got = send(away[(e - 1) * cut_rows : e * cut_rows], c=e)
            keep = keep + got.astype(F32)
        other = send(keep[own:].astype(BF16), y=1)
        stream, normed = kernel_call(
            norm_body,
            [
                jax.ShapeDtypeStruct((own, model), F32),
                jax.ShapeDtypeStruct((n_sp, own, model // n_sp), BF16),
            ],
            n_in=4,
            name="norm",
        )(keep[:own], other, residual, mixer_norm_gain[None, :])

        line = [normed] + [send(normed, a=d) for d in range(1, n_a)]
        toks = list(line)
        for e in range(1, n_c):
            toks += [send(u, c=e) for u in line]
        group = n_a * own
        mixed_rows = n_c * group
        keep, away = kernel_call(
            lambda *refs: mixer_body(n_a, n_c, *refs),
            [
                jax.ShapeDtypeStruct((group, model), F32),
                jax.ShapeDtypeStruct((mixed_rows - group, model), BF16),
            ],
            scratch=[
                pltpu.VMEM((n_sp, mixed_rows, model // n_sp), BF16),
                pltpu.VMEM((n_y * n_b, mixed_rows, piece // n_b), BF16),
            ],
            smem=1,
            n_in=1 + len(toks) + len(ups) + len(downs),
            name="mixer",
        )(place, *toks, *ups, *downs)
        for e in range(1, n_c):
            got = send(away[(e - 1) * group : e * group], c=n_c - e)
            keep = keep + got.astype(F32)
        total = stream + keep[:own]
        for d in range(1, n_a):
            got = send(keep[d * own : (d + 1) * own].astype(BF16), a=n_a - d)
            total = total + got.astype(F32)
        return total.astype(BF16)

    return jax.shard_map(
        on_device,
        mesh=mesh,
        in_specs=(
            P("sp", "tp"),
            P("sp", "tp"),
            P("sp", "tp"),
            P("sp", "tp"),
            P("tp"),
            P("sp", "tp"),
            P(),
            P("tp", None),
            P(("sp", "tp"), None),
            P(),
            P("sp", "tp"),
            P(("tp", "sp"), None),
        ),
        out_specs=P(("sp", "tp"), None),
        check_vma=False,
    )
```

```python
import jax
import jax.numpy as jnp
from jax import lax
from jax.experimental import pallas as pl
from jax.experimental.pallas import tpu as pltpu
from jax.sharding import PartitionSpec as P


HEAD = 128
SUB = 64
EPS = 1e-06
HI = lax.Precision.HIGHEST
AXES = ("sp", "tp")
F32 = jnp.float32
BF16 = jnp.bfloat16


HEAD_K = 128
HEAD_V = 128
BLOCK = 64


def exact_parts(x):
    first = x.astype(BF16)
    rest = x - first.astype(F32)
    second = rest.astype(BF16)
    third = (rest - second.astype(F32)).astype(BF16)
    return first, second, third


def pack_logs(totals):
    lines = []
    for x in totals:
        lines += list(exact_parts(x))
    pad = 16 - len(lines)
    return jnp.concatenate(
        [x.astype(F32) for x in lines] + [jnp.zeros((pad, HEAD), F32)], axis=0
    ).astype(BF16)


def log_of(packed, heads, h):
    parts = packed[heads * HEAD :, :].astype(F32)
    return sum(parts[3 * h + k : 3 * h + k + 1, :] for k in range(3))


def as_column(row):
    return jnp.transpose(jnp.broadcast_to(row, (HEAD, HEAD)))


def gates_body(logits, values, gap, extra, gate_out, cum_out, packed):
    rows, width = logits.shape
    heads = width // HEAD
    z = logits[...].astype(F32)
    gate = gap[...] / (1.0 + jnp.exp(z))
    log_forget = jnp.log1p(-gate) + extra[...]
    r = lax.broadcasted_iota(jnp.int32, (rows, rows), 0)
    c = lax.broadcasted_iota(jnp.int32, (rows, rows), 1)
    lower = (r >= c).astype(F32)
    cum = jnp.dot(lower, log_forget, precision=HI, preferred_element_type=F32)
    gate_out[...] = gate
    cum_out[...] = cum
    total = cum[rows - 1 : rows, :]
    keys = gate * jnp.exp(total - cum)
    vals = values[...].astype(F32)
    for h in range(heads):
        ks = keys[:, h * HEAD : (h + 1) * HEAD]
        vs = vals[:, h * HEAD : (h + 1) * HEAD]
        state = lax.dot_general(
            ks, vs, (((0,), (0,)), ((), ())), precision=HI, preferred_element_type=F32
        )
        packed[h * HEAD : (h + 1) * HEAD, :] = state.astype(BF16)
    packed[heads * HEAD :, :] = pack_logs([total[:, h * HEAD : (h + 1) * HEAD] for h in range(heads)])


def local_body(query, gate, cum, values, out):
    rows, width = query.shape
    sub = min(SUB, rows)
    for h in range(width // HEAD):
        lanes = slice(h * HEAD, (h + 1) * HEAD)
        for i in range(rows // sub):
            lo, hi = i * sub, (i + 1) * sub
            mid = cum[lo + sub // 2 - 1 : lo + sub // 2, lanes]
            qs = query[lo:hi, lanes].astype(F32) * (HEAD**-0.5) * jnp.exp(cum[lo:hi, lanes] - mid)
            ks = gate[0:hi, lanes] * jnp.exp(mid - cum[0:hi, lanes])
            scores = lax.dot_general(
                qs, ks, (((1,), (1,)), ((), ())), precision=HI, preferred_element_type=F32
            )
            rr = lax.broadcasted_iota(jnp.int32, (sub, hi), 0) + lo
            cc = lax.broadcasted_iota(jnp.int32, (sub, hi), 1)
            scores = jnp.where(rr >= cc, scores, 0.0)
            out[lo:hi, lanes] = jnp.dot(
                scores, values[0:hi, lanes].astype(F32), precision=HI, preferred_element_type=F32
            )


def kernel_call(body, out_shape, scratch=(), smem=0, n_in=0, mib=16):
    specs = [pl.BlockSpec(memory_space=pltpu.SMEM)] * smem
    specs += [pl.BlockSpec(memory_space=pltpu.VMEM)] * (n_in - smem)
    many = isinstance(out_shape, (list, tuple))
    out_spec = pl.BlockSpec(memory_space=pltpu.VMEM)
    return pl.pallas_call(
        body,
        out_shape=out_shape,
        in_specs=specs,
        out_specs=[out_spec] * len(out_shape) if many else out_spec,
        scratch_shapes=list(scratch),
        compiler_params=pltpu.CompilerParams(vmem_limit_bytes=mib * 1024 * 1024),
    )


def pair_body(place, mine, theirs, out):
    last = place[1] == 1
    heads = (mine.shape[0] - 16) // HEAD
    logs = []
    for h in range(heads):
        rows = slice(h * HEAD, (h + 1) * HEAD)
        own_log, their_log = log_of(mine, heads, h), log_of(theirs, heads, h)
        own_state, their_state = mine[rows, :].astype(F32), theirs[rows, :].astype(F32)
        decay = as_column(jnp.exp(jnp.where(last, own_log, their_log)))
        early = jnp.where(last, their_state, own_state)
        late = jnp.where(last, own_state, their_state)
        out[rows, :] = (decay * early + late).astype(BF16)
        logs.append(own_log + their_log)
    out[heads * HEAD :, :] = pack_logs(logs)


def mix_body(n_cores, *refs):
    place = refs[0]
    query, cum, local, gate_logits, gain, weight, beside = refs[1:8]
    states = refs[8:-4]
    first, second, away, mixed = refs[-4:]
    rows, width = query.shape
    heads = width // HEAD
    last = place[1] == 1
    for h in range(heads):
        lanes = slice(h * HEAD, (h + 1) * HEAD)
        arrived = jnp.where(last, beside[lanes, :].astype(F32), 0.0)
        passed = jnp.where(last, log_of(beside, heads, h), 0.0)
        for s in states:
            arrived = arrived + as_column(jnp.exp(passed)) * s[lanes, :].astype(F32)
            passed = passed + log_of(s, heads, h)
        reach = query[:, lanes].astype(F32) * (HEAD**-0.5) * jnp.exp(cum[:, lanes])
        rec = local[:, lanes] + jnp.dot(reach, arrived, precision=HI, preferred_element_type=F32)
        scale = lax.rsqrt(jnp.mean(rec * rec, axis=-1, keepdims=True) + EPS)
        v = gate_logits[:, lanes].astype(F32)
        mixed[:, lanes] = rec * scale * gain[...] * (v / (1.0 + jnp.exp(-v)))
    y, c = place[2], place[3]
    n_y = 2
    own = rows // (n_y * n_cores)
    picked = []
    for e in range(n_cores):
        for k in range(n_y):
            t = lax.rem(y + k, n_y) * n_cores + lax.rem(c + e, n_cores)
            picked.append(mixed[pl.ds(pl.multiple_of(t * own, own), own), :])
    ordered = jnp.concatenate(picked, axis=0).astype(BF16)
    part = jnp.dot(ordered, weight[...], preferred_element_type=F32)
    first[...] = part[:own]
    second[...] = part[own : n_y * own]
    away[...] = part[n_y * own :].astype(BF16)


def norm_body(own, beside, arrived, residual, gain, stream_out, normed_out):
    rows = own.shape[0]
    stream = own[...] + beside[:rows, :].astype(F32) + arrived[...].astype(F32)
    stream = stream + residual[...].astype(F32)
    stream_out[...] = stream
    scale = lax.rsqrt(jnp.mean(stream * stream, axis=-1, keepdims=True) + EPS)
    normed = (stream * scale * gain[...]).astype(BF16)
    blocks, _, cols = normed_out.shape
    for i in range(blocks):
        normed_out[i] = normed[:, i * cols : (i + 1) * cols]


def lower_half(out_own, out_away, hidden, down, cut):
    acc = jnp.dot(hidden, down, preferred_element_type=F32)
    out_own[...] = acc[:cut]
    out_away[...] = acc[cut:].astype(BF16)


def mixer_body(n_a, n_cores, *refs):
    n_tok = n_a * n_cores
    n_b = 2
    place = refs[0]
    toks = refs[1 : 1 + n_tok]
    ups = refs[1 + n_tok : 1 + n_tok + 2 * n_b * n_a]
    downs = refs[1 + n_tok + 2 * n_b * n_a : -7]
    keep, away, hid_out, rows_x, up_all, hid, down_all = refs[-7:]
    a, b = place[0], place[1]
    _, own, cols = toks[0].shape
    for i in range(n_tok):
        for e in range(n_a):
            for x in range(n_b):
                k = lax.rem(a - e + n_a, n_a) * n_b + lax.rem(b + x, n_b)
                at = (e * n_b + x) * cols
                rows_x[i * own : (i + 1) * own, at : at + cols] = toks[i][k]
    for y in range(2):
        for e in range(n_a):
            for x in range(n_b):
                at = (e * n_b + x) * cols
                src, off = ups[(y * n_b + x) * n_a + e]
                up_all[at : at + cols, :] = src[off : off + cols, :]
        act = jnp.maximum(jnp.dot(rows_x[...], up_all[...], preferred_element_type=F32), 0.0)
        act = (act * act).astype(BF16)
        half = act.shape[1] // n_b
        for x in range(n_b):
            hid[y * n_b + x] = act[:, x * half : (x + 1) * half]
    width = keep.shape[1]
    at = 0
    for y in range(2):
        for x in range(n_b):
            h = hid[y * n_b + lax.rem(b + x, n_b)]
            step = h.shape[1]
            hid_out[:, at : at + step] = h
            for piece in downs[y * n_b + x :] if y * n_b + x == 3 else [downs[y * n_b + x]]:
                n = piece.shape[0]
                down_all[at : at + n, :] = piece[:, :width]
                at += n
    lower_half(keep, away, hid_out[...], down_all[...], n_a * own)


def mixer_rest_body(cut, hidden, *refs):
    downs, (keep, away, down_all) = refs[:-3], refs[-3:]
    width = keep.shape[1]
    at = 0
    for piece in downs:
        n = piece.shape[0]
        down_all[at : at + n, :] = piece[:, width:]
        at += n
    lower_half(keep, away, hidden[...], down_all[...], cut)


def fold_body(keep, got, *outs):
    rows = outs[0].shape[0]
    for d in range(len(outs)):
        at = (d + 1) * rows
        outs[d][...] = (keep[at : at + rows, :] + got[at : at + rows, :].astype(F32)).astype(BF16)


norm_eps = 1e-06
highest_precision = lax.Precision.HIGHEST


def carried_in(part, axis, combine, identity):
    place = lax.axis_index(axis)
    gathered = jax.tree.map(lambda a: lax.all_gather(a, axis), part)
    state = jax.tree.map(lambda a, e: jnp.zeros_like(a) + jnp.asarray(e, a.dtype), part, identity)

    def one(step, state):
        return combine(
            state, jax.tree.map(lambda a: lax.dynamic_index_in_dim(a, step, 0, False), gathered)
        )

    return lax.fori_loop(0, place, one, state)


def block_update(carry_forward_state, block_inputs):
    query_rows_block, gate_rows_block, value_rows_block, log_block = block_inputs
    cumulative_log = jnp.cumsum(log_block, axis=1)
    length = query_rows_block.shape[1]
    causal = jnp.arange(length)[:, None] >= jnp.arange(length)[None, :]
    across_blocks = jnp.einsum(
        "dcj,djw->dcw",
        query_rows_block * jnp.exp(cumulative_log),
        carry_forward_state,
        precision=highest_precision,
    )
    spread = cumulative_log[:, :, None, :] - cumulative_log[:, None, :, :]
    decay_table = jnp.exp(jnp.where(causal[None, :, :, None], spread, -jnp.inf))
    scores = jnp.einsum(
        "htk,hsk,htsk->hts",
        query_rows_block,
        gate_rows_block,
        decay_table,
        precision=highest_precision,
    )
    within = jnp.einsum("hts,hsv->htv", scores, value_rows_block, precision=highest_precision)
    final_log_total = cumulative_log[:, -1:, :]
    updated_state = jnp.exp(final_log_total[:, 0, :])[
        :, :, None
    ] * carry_forward_state + jnp.einsum(
        "tri,trw->tiw",
        gate_rows_block * jnp.exp(final_log_total - cumulative_log),
        value_rows_block,
        precision=highest_precision,
    )
    return (updated_state, across_blocks + within)


def to_blocks(array, inner):
    length = array.shape[0]
    split_up = array.reshape(length // BLOCK, BLOCK, array.shape[1] // inner, inner)
    return jnp.transpose(split_up, (0, 2, 1, 3))


def from_blocks(blocked):
    joined = jnp.transpose(blocked, (0, 2, 1, 3))
    return joined.reshape(joined.shape[0] * joined.shape[1], joined.shape[2], joined.shape[3])


def prepare_inputs(query, forget_logits, written_values, forget_floor_gap, extra_log_decay):
    input_gate_value = forget_floor_gap[None, :] * jax.nn.sigmoid(
        -forget_logits.astype(jnp.float32)
    )
    forget_log_rate = jnp.log1p(-input_gate_value) + extra_log_decay
    scaled_values = query.astype(jnp.float32) * HEAD_K ** (-0.5)
    return (scaled_values, input_gate_value, written_values.astype(jnp.float32), forget_log_rate)


def gate_out(recurrent, output_gate_logits, head_norm_gain):
    normal_part = recurrent * lax.rsqrt(
        jnp.mean(recurrent * recurrent, axis=-1, keepdims=True) + norm_eps
    )
    gating = jax.nn.silu(output_gate_logits.astype(jnp.float32)).reshape(recurrent.shape)
    mixed = normal_part * head_norm_gain * gating
    return mixed.reshape(recurrent.shape[0], -1).astype(jnp.bfloat16)


def normalize(stream, gain):
    scaled_rows = stream * lax.rsqrt(jnp.mean(stream * stream, axis=-1, keepdims=True) + norm_eps)
    return (scaled_rows * gain).astype(jnp.bfloat16)


def chain_states(earlier, later):
    return (earlier[0] + later[0], jnp.exp(later[0])[:, :, None] * earlier[1] + later[1])


def gathered_plan(
    query,
    forget_logits,
    written_values,
    output_gate_logits,
    forget_floor_gap,
    extra_log_decay,
    head_norm_gain,
    output_weight,
    residual,
    mixer_norm_gain,
    mixer_up_weight,
    mixer_down_weight,
):
    scaled_values, input_gate_value, value_rows, forget_log_rate = prepare_inputs(
        query, forget_logits, written_values, forget_floor_gap, extra_log_decay
    )
    row_count, local_width = query.shape
    head_count = local_width // HEAD_K
    start_state = jnp.zeros((head_count, HEAD_K, HEAD_V), jnp.float32)
    local_state, blocked = lax.scan(
        block_update,
        start_state,
        (
            to_blocks(scaled_values, HEAD_K),
            to_blocks(input_gate_value, HEAD_K),
            to_blocks(value_rows, HEAD_V),
            to_blocks(forget_log_rate, HEAD_K),
        ),
    )
    log_total = jnp.sum(forget_log_rate, axis=0).reshape(head_count, HEAD_K)
    arrived_state = carried_in(
        (log_total, local_state),
        "sp",
        chain_states,
        (jnp.zeros_like(log_total), jnp.zeros_like(local_state)),
    )
    running = jnp.cumsum(forget_log_rate, axis=0)
    reached_state = (scaled_values * jnp.exp(running)).reshape(row_count, head_count, HEAD_K)
    carried_over = jnp.einsum(
        "cja,jae->cje", reached_state, arrived_state[1], precision=highest_precision
    )
    mixed = gate_out(from_blocks(blocked) + carried_over, output_gate_logits, head_norm_gain)
    stream_own = lax.psum_scatter(
        jnp.dot(mixed, output_weight, preferred_element_type=jnp.float32).astype(jnp.bfloat16),
        "tp",
        scatter_dimension=0,
        tiled=True,
    ).astype(jnp.float32) + residual.astype(jnp.float32)
    normed = lax.all_gather(normalize(stream_own, mixer_norm_gain), "tp", axis=0, tiled=True)
    columns = normed
    lifted = jnp.dot(
        columns,
        lax.all_gather(mixer_up_weight, "sp", axis=0, tiled=True),
        preferred_element_type=jnp.float32,
    )
    hidden = jnp.square(jax.nn.relu(lifted)).astype(jnp.bfloat16)
    columns = hidden
    projected = jnp.dot(
        columns,
        lax.all_gather(mixer_down_weight, "sp", axis=0, tiled=True),
        preferred_element_type=jnp.float32,
    )
    mlp_own = lax.psum_scatter(
        projected.astype(jnp.bfloat16), "tp", scatter_dimension=0, tiled=True
    ).astype(jnp.float32)
    return (stream_own + mlp_own).astype(jnp.bfloat16)


def solution(mesh):
    specs = dict(
        mesh=mesh,
        in_specs=(
            P("sp", "tp"),
            P("sp", "tp"),
            P("sp", "tp"),
            P("sp", "tp"),
            P("tp"),
            P("sp", "tp"),
            P(),
            P("tp", None),
            P(("sp", "tp"), None),
            P(),
            P("sp", "tp"),
            P(("tp", "sp"), None),
        ),
        out_specs=P(("sp", "tp"), None),
        check_vma=False,
    )
    n_sp, n_tp = mesh.shape["sp"], mesh.shape["tp"]
    n_b, n_y = 2, 2
    n_a, n_c = n_sp // n_b, n_tp // n_y
    if n_sp % n_b or n_tp % n_y or n_a > 4 or n_c != 2:
        return jax.shard_map(gathered_plan, **specs)

    def flat(a, b, y, c):
        return (a % n_a * n_b + b % n_b) * n_tp + y % n_y * n_c + c % n_c

    def send(x, a=0, b=0, y=0, c=0, cyclic=True):
        pairs = [
            (flat(i, j, k, m), flat(i + a, j + b, k + y, m + c))
            for i in range(n_a)
            for j in range(n_b)
            for k in range(n_y)
            for m in range(n_c)
            if cyclic or i + a < n_a
        ]
        return lax.ppermute(x, AXES, pairs)

    def on_device(
        query,
        forget_logits,
        written_values,
        output_gate_logits,
        forget_floor_gap,
        extra_log_decay,
        head_norm_gain,
        output_weight,
        residual,
        mixer_norm_gain,
        mixer_up_weight,
        mixer_down_weight,
    ):
        sp, tp = lax.axis_index("sp"), lax.axis_index("tp")
        a, b, y, c = sp // n_b, sp % n_b, tp // n_c, tp % n_c
        place = jnp.stack([a, b, y, c]).astype(jnp.int32)
        rows, width = query.shape
        model = output_weight.shape[1]
        own = residual.shape[0]
        heads = width // HEAD

        packed_shape = jax.ShapeDtypeStruct((heads * HEAD + 16, HEAD), BF16)
        gate, cum, packed = kernel_call(
            gates_body,
            [
                jax.ShapeDtypeStruct((rows, width), F32),
                jax.ShapeDtypeStruct((rows, width), F32),
                packed_shape,
            ],
            n_in=4,
        )(forget_logits, written_values, forget_floor_gap[None, :], extra_log_decay)
        later_weight, packed = lax.optimization_barrier((mixer_up_weight, packed))

        up_rows, up_cols = mixer_up_weight.shape
        piece = up_cols // n_a
        mine = []
        for d in range(n_a):
            source = mixer_up_weight if d == n_a // 2 else later_weight
            cut = lax.dynamic_slice(source, (0, (a + d) % n_a * piece), (up_rows, piece))
            mine.append(cut if d == 0 else send(cut, a=d))
        groups = [mine[0::2], mine[1::2]]
        up_x, up_y, up_xy = [], [], []
        for g, members in enumerate(groups):
            joined = jnp.concatenate(members, axis=0)
            up_x.append(send(joined, b=1))
            up_y.append(send(joined, y=1))
            if g:
                up_xy.append(send(up_y[g], b=1))
            else:
                up_xy.append(send(up_x[g], y=1))
        up_arrays = mine + up_x + up_y + up_xy

        def up_places(refs):
            found = [(refs[e], 0) for e in range(n_a)]
            for k in range(3):
                found += [
                    (refs[n_a + 2 * k + e % 2], e // 2 * up_rows) for e in range(n_a)
                ]
            return found

        half = mixer_down_weight.shape[0] // 2
        down_x = send(mixer_down_weight, b=1)
        down_y = send(mixer_down_weight, y=1)
        down_xy = [send(down_x[:half], y=1), send(down_y[half:], b=1)]
        down_arrays = [mixer_down_weight, down_x, down_y] + down_xy

        beside = send(packed, b=1)
        pair = kernel_call(pair_body, packed_shape, smem=1, n_in=3)(place, packed, beside)
        states = [send(pair, a=d, cyclic=False) for d in range(1, n_a)]
        local = kernel_call(
            local_body, jax.ShapeDtypeStruct((rows, width), F32), n_in=4
        )(query, gate, cum, written_values)
        first, second, away = kernel_call(
            lambda *refs: mix_body(n_c, *refs),
            [
                jax.ShapeDtypeStruct((own, model), F32),
                jax.ShapeDtypeStruct((own, model), F32),
                jax.ShapeDtypeStruct((n_y * own, model), BF16),
            ],
            scratch=[pltpu.VMEM((rows, width), F32)],
            smem=1,
            n_in=8 + len(states),
        )(
            place,
            query,
            cum,
            local,
            output_gate_logits,
            head_norm_gain[None, :],
            output_weight,
            beside,
            *states,
        )
        got = send(away, c=1)
        other = send((second + got[own:].astype(F32)).astype(BF16), y=1)
        stream, normed = kernel_call(
            norm_body,
            [
                jax.ShapeDtypeStruct((own, model), F32),
                jax.ShapeDtypeStruct((n_sp, own, model // n_sp), BF16),
            ],
            n_in=5,
        )(first, got, other, residual, mixer_norm_gain[None, :])

        line = [normed] + [send(normed, a=d) for d in range(1, n_a)]
        toks = line + [send(u, c=1) for u in line]
        group = n_a * own
        part = model // 2
        sizes = [
            jax.ShapeDtypeStruct((group, part), F32),
            jax.ShapeDtypeStruct((group, part), BF16),
        ]
        units = n_y * piece

        def mixer(*refs):
            n_tok = len(toks)
            ups = up_places(refs[1 + n_tok : 1 + n_tok + len(up_arrays)])
            rest = refs[1 + n_tok + len(up_arrays) :]
            mixer_body(n_a, n_c, *refs[: 1 + n_tok], *ups, *rest)

        keep0, away0, hidden = kernel_call(
            mixer,
            sizes + [jax.ShapeDtypeStruct((n_c * group, units), BF16)],
            scratch=[
                pltpu.VMEM((n_c * group, model), BF16),
                pltpu.VMEM((model, piece), BF16),
                pltpu.VMEM((n_y * n_b, n_c * group, piece // n_b), BF16),
                pltpu.VMEM((units, part), BF16),
            ],
            smem=1,
            n_in=1 + len(toks) + len(up_arrays) + len(down_arrays),
            mib=34,
        )(place, *toks, *up_arrays, *down_arrays)
        got0 = send(away0, c=1)
        keep1, away1 = kernel_call(
            lambda *refs: mixer_rest_body(group, *refs),
            sizes,
            scratch=[pltpu.VMEM((units, part), BF16)],
            n_in=1 + len(down_arrays),
        )(hidden, *down_arrays)
        got1 = send(away1, c=1)
        halves = []
        for k, (keep, got) in enumerate([(keep0, got0), (keep1, got1)]):
            outs = kernel_call(
                fold_body, [jax.ShapeDtypeStruct((own, part), BF16)] * (n_a - 1), n_in=2
            )(keep, got)
            total = stream[:, k * part : (k + 1) * part] + keep[:own] + got[:own].astype(F32)
            for d in range(1, n_a):
                total = total + send(outs[d - 1], a=n_a - d).astype(F32)
            halves.append(total.astype(BF16))
        return jnp.concatenate(halves, axis=1)


    return jax.shard_map(on_device, **specs)
```

```python
import jax
import jax.numpy as jnp
from jax import lax
from jax.experimental import pallas as pl
from jax.experimental.pallas import tpu as pltpu
from jax.sharding import PartitionSpec as P


HEAD = 128
SUB = 64
EPS = 1e-06
HI = lax.Precision.HIGHEST
AXES = ("sp", "tp")
F32 = jnp.float32
BF16 = jnp.bfloat16


HEAD_K = 128
HEAD_V = 128
BLOCK = 64


def exact_parts(x):
    first = x.astype(BF16)
    rest = x - first.astype(F32)
    second = rest.astype(BF16)
    third = (rest - second.astype(F32)).astype(BF16)
    return first, second, third


def pack_logs(totals):
    lines = []
    for x in totals:
        lines += list(exact_parts(x))
    pad = 16 - len(lines)
    return jnp.concatenate(
        [x.astype(F32) for x in lines] + [jnp.zeros((pad, HEAD), F32)], axis=0
    ).astype(BF16)


def log_of(packed, heads, h):
    parts = packed[heads * HEAD :, :].astype(F32)
    return sum(parts[3 * h + k : 3 * h + k + 1, :] for k in range(3))


def as_column(row):
    return jnp.transpose(jnp.broadcast_to(row, (HEAD, HEAD)))


def gates_body(logits, values, gap, extra, gate_out, cum_out, packed):
    rows, width = logits.shape
    heads = width // HEAD
    z = logits[...].astype(F32)
    gate = gap[...] / (1.0 + jnp.exp(z))
    log_forget = jnp.log1p(-gate) + extra[...]
    r = lax.broadcasted_iota(jnp.int32, (rows, rows), 0)
    c = lax.broadcasted_iota(jnp.int32, (rows, rows), 1)
    lower = (r >= c).astype(F32)
    cum = jnp.dot(lower, log_forget, precision=HI, preferred_element_type=F32)
    gate_out[...] = gate
    cum_out[...] = cum
    total = cum[rows - 1 : rows, :]
    keys = gate * jnp.exp(total - cum)
    vals = values[...].astype(F32)
    for h in range(heads):
        ks = keys[:, h * HEAD : (h + 1) * HEAD]
        vs = vals[:, h * HEAD : (h + 1) * HEAD]
        state = lax.dot_general(
            ks, vs, (((0,), (0,)), ((), ())), precision=HI, preferred_element_type=F32
        )
        packed[h * HEAD : (h + 1) * HEAD, :] = state.astype(BF16)
    packed[heads * HEAD :, :] = pack_logs([total[:, h * HEAD : (h + 1) * HEAD] for h in range(heads)])


def local_body(query, gate, cum, values, out):
    rows, width = query.shape
    sub = min(SUB, rows)
    for h in range(width // HEAD):
        lanes = slice(h * HEAD, (h + 1) * HEAD)
        for i in range(rows // sub):
            lo, hi = i * sub, (i + 1) * sub
            mid = cum[lo + sub // 2 - 1 : lo + sub // 2, lanes]
            qs = query[lo:hi, lanes].astype(F32) * (HEAD**-0.5) * jnp.exp(cum[lo:hi, lanes] - mid)
            ks = gate[0:hi, lanes] * jnp.exp(mid - cum[0:hi, lanes])
            scores = lax.dot_general(
                qs, ks, (((1,), (1,)), ((), ())), precision=HI, preferred_element_type=F32
            )
            rr = lax.broadcasted_iota(jnp.int32, (sub, hi), 0) + lo
            cc = lax.broadcasted_iota(jnp.int32, (sub, hi), 1)
            scores = jnp.where(rr >= cc, scores, 0.0)
            out[lo:hi, lanes] = jnp.dot(
                scores, values[0:hi, lanes].astype(F32), precision=HI, preferred_element_type=F32
            )


def kernel_call(body, out_shape, scratch=(), smem=0, n_in=0, mib=16):
    specs = [pl.BlockSpec(memory_space=pltpu.SMEM)] * smem
    specs += [pl.BlockSpec(memory_space=pltpu.VMEM)] * (n_in - smem)
    many = isinstance(out_shape, (list, tuple))
    out_spec = pl.BlockSpec(memory_space=pltpu.VMEM)
    return pl.pallas_call(
        body,
        out_shape=out_shape,
        in_specs=specs,
        out_specs=[out_spec] * len(out_shape) if many else out_spec,
        scratch_shapes=list(scratch),
        compiler_params=pltpu.CompilerParams(vmem_limit_bytes=mib * 1024 * 1024),
    )


def pair_body(place, mine, theirs, out):
    last = place[1] == 1
    heads = (mine.shape[0] - 16) // HEAD
    logs = []
    for h in range(heads):
        rows = slice(h * HEAD, (h + 1) * HEAD)
        own_log, their_log = log_of(mine, heads, h), log_of(theirs, heads, h)
        own_state, their_state = mine[rows, :].astype(F32), theirs[rows, :].astype(F32)
        decay = as_column(jnp.exp(jnp.where(last, own_log, their_log)))
        early = jnp.where(last, their_state, own_state)
        late = jnp.where(last, own_state, their_state)
        out[rows, :] = (decay * early + late).astype(BF16)
        logs.append(own_log + their_log)
    out[heads * HEAD :, :] = pack_logs(logs)


def mix_body(n_cores, *refs):
    place = refs[0]
    query, cum, local, gate_logits, gain, weight, beside = refs[1:8]
    states = refs[8:-4]
    first, second, away, mixed = refs[-4:]
    rows, width = query.shape
    heads = width // HEAD
    last = place[1] == 1
    for h in range(heads):
        lanes = slice(h * HEAD, (h + 1) * HEAD)
        arrived = jnp.where(last, beside[lanes, :].astype(F32), 0.0)
        passed = jnp.where(last, log_of(beside, heads, h), 0.0)
        for s in states:
            arrived = arrived + as_column(jnp.exp(passed)) * s[lanes, :].astype(F32)
            passed = passed + log_of(s, heads, h)
        reach = query[:, lanes].astype(F32) * (HEAD**-0.5) * jnp.exp(cum[:, lanes])
        rec = local[:, lanes] + jnp.dot(reach, arrived, precision=HI, preferred_element_type=F32)
        scale = lax.rsqrt(jnp.mean(rec * rec, axis=-1, keepdims=True) + EPS)
        v = gate_logits[:, lanes].astype(F32)
        mixed[:, lanes] = rec * scale * gain[...] * (v / (1.0 + jnp.exp(-v)))
    y, c = place[2], place[3]
    n_y = 2
    own = rows // (n_y * n_cores)
    picked = []
    for e in range(n_cores):
        for k in range(n_y):
            t = lax.rem(y + k, n_y) * n_cores + lax.rem(c + e, n_cores)
            picked.append(mixed[pl.ds(pl.multiple_of(t * own, own), own), :])
    ordered = jnp.concatenate(picked, axis=0).astype(BF16)
    part = jnp.dot(ordered, weight[...], preferred_element_type=F32)
    first[...] = part[:own]
    second[...] = part[own : n_y * own]
    away[...] = part[n_y * own :].astype(BF16)


def norm_body(own, beside, arrived, residual, gain, stream_out, normed_out):
    rows = own.shape[0]
    stream = own[...] + beside[:rows, :].astype(F32) + arrived[...].astype(F32)
    stream = stream + residual[...].astype(F32)
    stream_out[...] = stream
    scale = lax.rsqrt(jnp.mean(stream * stream, axis=-1, keepdims=True) + EPS)
    normed = (stream * scale * gain[...]).astype(BF16)
    blocks, _, cols = normed_out.shape
    for i in range(blocks):
        normed_out[i] = normed[:, i * cols : (i + 1) * cols]


def hidden_half(rows_x, ups, up_all, cols, out):
    at = 0
    for src, off in ups:
        up_all[at : at + cols, :] = src[off : off + cols, :]
        at += cols
    act = jnp.maximum(jnp.dot(rows_x[...], up_all[...], preferred_element_type=F32), 0.0)
    out[...] = (act * act).astype(BF16)


def first_body(n_a, n_cores, place, toks, ups, rows_x, hidden, up_all):
    a, b = place[0], place[1]
    n_b = len(ups) // n_a
    _, own, cols = toks[0].shape
    for i in range(n_a * n_cores):
        for x in range(n_b):
            for e in range(n_a):
                k = lax.rem(a - e + n_a, n_a) * n_b + lax.rem(b + x, n_b)
                at = (x * n_a + e) * cols
                rows_x[i * own : (i + 1) * own, at : at + cols] = toks[i][k]
    hidden_half(rows_x, ups, up_all, cols, hidden)


def down_product(keep, away, units, pieces, down_all):
    at = 0
    for group in pieces:
        for piece in group:
            n = piece.shape[0]
            down_all[at : at + n, :] = piece[...]
            at += n
    acc = jnp.dot(units, down_all[...], preferred_element_type=F32)
    cut = keep.shape[0]
    keep[...] = acc[:cut]
    away[...] = acc[cut:].astype(BF16)


def lower_body(cols, place, rows_x, early, ups, pieces, keep, away, ordered, up_all, late, down_all):
    hidden_half(rows_x, ups, up_all, cols, late)
    n_b = 2
    b = place[1]
    half = late.shape[1] // n_b
    for y, src in enumerate((early, late)):
        for x in range(n_b):
            k = lax.rem(b + x, n_b)
            at = (y * n_b + x) * half
            ordered[:, at : at + half] = src[:, pl.ds(pl.multiple_of(k * half, half), half)]
    down_product(keep, away, ordered[...], pieces, down_all)


def fold_body(keep, got, *outs):
    rows = outs[0].shape[0]
    for d in range(len(outs)):
        at = (d + 1) * rows
        outs[d][...] = (keep[at : at + rows, :] + got[at : at + rows, :].astype(F32)).astype(BF16)


norm_eps = 1e-06
highest_precision = lax.Precision.HIGHEST


def carried_in(part, axis, combine, identity):
    place = lax.axis_index(axis)
    gathered = jax.tree.map(lambda a: lax.all_gather(a, axis), part)
    state = jax.tree.map(lambda a, e: jnp.zeros_like(a) + jnp.asarray(e, a.dtype), part, identity)

    def one(step, state):
        return combine(
            state, jax.tree.map(lambda a: lax.dynamic_index_in_dim(a, step, 0, False), gathered)
        )

    return lax.fori_loop(0, place, one, state)


def block_update(carry_forward_state, block_inputs):
    query_rows_block, gate_rows_block, value_rows_block, log_block = block_inputs
    cumulative_log = jnp.cumsum(log_block, axis=1)
    length = query_rows_block.shape[1]
    causal = jnp.arange(length)[:, None] >= jnp.arange(length)[None, :]
    across_blocks = jnp.einsum(
        "dcj,djw->dcw",
        query_rows_block * jnp.exp(cumulative_log),
        carry_forward_state,
        precision=highest_precision,
    )
    spread = cumulative_log[:, :, None, :] - cumulative_log[:, None, :, :]
    decay_table = jnp.exp(jnp.where(causal[None, :, :, None], spread, -jnp.inf))
    scores = jnp.einsum(
        "htk,hsk,htsk->hts",
        query_rows_block,
        gate_rows_block,
        decay_table,
        precision=highest_precision,
    )
    within = jnp.einsum("hts,hsv->htv", scores, value_rows_block, precision=highest_precision)
    final_log_total = cumulative_log[:, -1:, :]
    updated_state = jnp.exp(final_log_total[:, 0, :])[
        :, :, None
    ] * carry_forward_state + jnp.einsum(
        "tri,trw->tiw",
        gate_rows_block * jnp.exp(final_log_total - cumulative_log),
        value_rows_block,
        precision=highest_precision,
    )
    return (updated_state, across_blocks + within)


def to_blocks(array, inner):
    length = array.shape[0]
    split_up = array.reshape(length // BLOCK, BLOCK, array.shape[1] // inner, inner)
    return jnp.transpose(split_up, (0, 2, 1, 3))


def from_blocks(blocked):
    joined = jnp.transpose(blocked, (0, 2, 1, 3))
    return joined.reshape(joined.shape[0] * joined.shape[1], joined.shape[2], joined.shape[3])


def prepare_inputs(query, forget_logits, written_values, forget_floor_gap, extra_log_decay):
    input_gate_value = forget_floor_gap[None, :] * jax.nn.sigmoid(
        -forget_logits.astype(jnp.float32)
    )
    forget_log_rate = jnp.log1p(-input_gate_value) + extra_log_decay
    scaled_values = query.astype(jnp.float32) * HEAD_K ** (-0.5)
    return (scaled_values, input_gate_value, written_values.astype(jnp.float32), forget_log_rate)


def gate_out(recurrent, output_gate_logits, head_norm_gain):
    normal_part = recurrent * lax.rsqrt(
        jnp.mean(recurrent * recurrent, axis=-1, keepdims=True) + norm_eps
    )
    gating = jax.nn.silu(output_gate_logits.astype(jnp.float32)).reshape(recurrent.shape)
    mixed = normal_part * head_norm_gain * gating
    return mixed.reshape(recurrent.shape[0], -1).astype(jnp.bfloat16)


def normalize(stream, gain):
    scaled_rows = stream * lax.rsqrt(jnp.mean(stream * stream, axis=-1, keepdims=True) + norm_eps)
    return (scaled_rows * gain).astype(jnp.bfloat16)


def chain_states(earlier, later):
    return (earlier[0] + later[0], jnp.exp(later[0])[:, :, None] * earlier[1] + later[1])


def gathered_plan(
    query,
    forget_logits,
    written_values,
    output_gate_logits,
    forget_floor_gap,
    extra_log_decay,
    head_norm_gain,
    output_weight,
    residual,
    mixer_norm_gain,
    mixer_up_weight,
    mixer_down_weight,
):
    scaled_values, input_gate_value, value_rows, forget_log_rate = prepare_inputs(
        query, forget_logits, written_values, forget_floor_gap, extra_log_decay
    )
    row_count, local_width = query.shape
    head_count = local_width // HEAD_K
    start_state = jnp.zeros((head_count, HEAD_K, HEAD_V), jnp.float32)
    local_state, blocked = lax.scan(
        block_update,
        start_state,
        (
            to_blocks(scaled_values, HEAD_K),
            to_blocks(input_gate_value, HEAD_K),
            to_blocks(value_rows, HEAD_V),
            to_blocks(forget_log_rate, HEAD_K),
        ),
    )
    log_total = jnp.sum(forget_log_rate, axis=0).reshape(head_count, HEAD_K)
    arrived_state = carried_in(
        (log_total, local_state),
        "sp",
        chain_states,
        (jnp.zeros_like(log_total), jnp.zeros_like(local_state)),
    )
    running = jnp.cumsum(forget_log_rate, axis=0)
    reached_state = (scaled_values * jnp.exp(running)).reshape(row_count, head_count, HEAD_K)
    carried_over = jnp.einsum(
        "cja,jae->cje", reached_state, arrived_state[1], precision=highest_precision
    )
    mixed = gate_out(from_blocks(blocked) + carried_over, output_gate_logits, head_norm_gain)
    stream_own = lax.psum_scatter(
        jnp.dot(mixed, output_weight, preferred_element_type=jnp.float32).astype(jnp.bfloat16),
        "tp",
        scatter_dimension=0,
        tiled=True,
    ).astype(jnp.float32) + residual.astype(jnp.float32)
    normed = lax.all_gather(normalize(stream_own, mixer_norm_gain), "tp", axis=0, tiled=True)
    columns = normed
    lifted = jnp.dot(
        columns,
        lax.all_gather(mixer_up_weight, "sp", axis=0, tiled=True),
        preferred_element_type=jnp.float32,
    )
    hidden = jnp.square(jax.nn.relu(lifted)).astype(jnp.bfloat16)
    columns = hidden
    projected = jnp.dot(
        columns,
        lax.all_gather(mixer_down_weight, "sp", axis=0, tiled=True),
        preferred_element_type=jnp.float32,
    )
    mlp_own = lax.psum_scatter(
        projected.astype(jnp.bfloat16), "tp", scatter_dimension=0, tiled=True
    ).astype(jnp.float32)
    return (stream_own + mlp_own).astype(jnp.bfloat16)


def solution(mesh):
    specs = dict(
        mesh=mesh,
        in_specs=(
            P("sp", "tp"),
            P("sp", "tp"),
            P("sp", "tp"),
            P("sp", "tp"),
            P("tp"),
            P("sp", "tp"),
            P(),
            P("tp", None),
            P(("sp", "tp"), None),
            P(),
            P("sp", "tp"),
            P(("tp", "sp"), None),
        ),
        out_specs=P(("sp", "tp"), None),
        check_vma=False,
    )
    n_sp, n_tp = mesh.shape["sp"], mesh.shape["tp"]
    n_b, n_y = 2, 2
    n_a, n_c = n_sp // n_b, n_tp // n_y
    if n_sp % n_b or n_tp % n_y or n_a > 4 or n_c != 2:
        return jax.shard_map(gathered_plan, **specs)

    def flat(a, b, y, c):
        return (a % n_a * n_b + b % n_b) * n_tp + y % n_y * n_c + c % n_c

    def send(x, a=0, b=0, y=0, c=0, cyclic=True):
        pairs = [
            (flat(i, j, k, m), flat(i + a, j + b, k + y, m + c))
            for i in range(n_a)
            for j in range(n_b)
            for k in range(n_y)
            for m in range(n_c)
            if cyclic or i + a < n_a
        ]
        return lax.ppermute(x, AXES, pairs)

    def on_device(
        query,
        forget_logits,
        written_values,
        output_gate_logits,
        forget_floor_gap,
        extra_log_decay,
        head_norm_gain,
        output_weight,
        residual,
        mixer_norm_gain,
        mixer_up_weight,
        mixer_down_weight,
    ):
        sp, tp = lax.axis_index("sp"), lax.axis_index("tp")
        a, b, y, c = sp // n_b, sp % n_b, tp // n_c, tp % n_c
        place = jnp.stack([a, b, y, c]).astype(jnp.int32)
        rows, width = query.shape
        model = output_weight.shape[1]
        own = residual.shape[0]
        heads = width // HEAD

        packed_shape = jax.ShapeDtypeStruct((heads * HEAD + 16, HEAD), BF16)
        gate, cum, packed = kernel_call(
            gates_body,
            [
                jax.ShapeDtypeStruct((rows, width), F32),
                jax.ShapeDtypeStruct((rows, width), F32),
                packed_shape,
            ],
            n_in=4,
        )(forget_logits, written_values, forget_floor_gap[None, :], extra_log_decay)
        up_rows, up_cols = mixer_up_weight.shape
        piece = up_cols // n_a
        mine = []
        for d in range(n_a):
            cut = lax.dynamic_slice(mixer_up_weight, (0, (a + d) % n_a * piece), (up_rows, piece))
            mine.append(cut if d == 0 else send(cut, a=d))
        up_x, up_y = [], []
        for g in range(2):
            joined = jnp.concatenate(mine[g::2], axis=0)
            up_x.append(send(joined, b=1))
            up_y.append(send(joined, y=1))
        up_xy = [send(up_y[0], b=1), send(up_x[1], y=1)]

        def grouped(refs):
            return [(refs[e % 2], e // 2 * up_rows) for e in range(n_a)]

        part = model // 2
        half = mixer_down_weight.shape[0] // 2
        down = [mixer_down_weight[:, :part], mixer_down_weight[:, part:]]
        down_x = [send(u, b=1) for u in down]
        down_y = [send(u, y=1) for u in down]
        down_xy = [
            [send(down_y[0], b=1)], [send(down_x[1][:half], y=1), send(down_y[1][half:], b=1)]
        ]

        beside = send(packed, b=1)
        pair = kernel_call(pair_body, packed_shape, smem=1, n_in=3)(place, packed, beside)
        states = [send(pair, a=d, cyclic=False) for d in range(1, n_a)]
        local = kernel_call(
            local_body, jax.ShapeDtypeStruct((rows, width), F32), n_in=4
        )(query, gate, cum, written_values)
        first, second, away = kernel_call(
            lambda *refs: mix_body(n_c, *refs),
            [
                jax.ShapeDtypeStruct((own, model), F32),
                jax.ShapeDtypeStruct((own, model), F32),
                jax.ShapeDtypeStruct((n_y * own, model), BF16),
            ],
            scratch=[pltpu.VMEM((rows, width), F32)],
            smem=1,
            n_in=8 + len(states),
        )(
            place,
            query,
            cum,
            local,
            output_gate_logits,
            head_norm_gain[None, :],
            output_weight,
            beside,
            *states,
        )
        got = send(away, c=1)
        other = send((second + got[own:].astype(F32)).astype(BF16), y=1)
        stream, normed = kernel_call(
            norm_body,
            [
                jax.ShapeDtypeStruct((own, model), F32),
                jax.ShapeDtypeStruct((n_sp, own, model // n_sp), BF16),
            ],
            n_in=5,
        )(first, got, other, residual, mixer_norm_gain[None, :])

        line = [normed] + [send(normed, a=d) for d in range(1, n_a)]
        toks = line + [send(u, c=1) for u in line]
        group = n_a * own
        tokens = n_c * group
        units = n_y * piece
        cols = model // n_sp
        sizes = [
            jax.ShapeDtypeStruct((group, part), F32),
            jax.ShapeDtypeStruct((tokens - group, part), BF16),
        ]

        def first_half(*refs):
            t = 1 + len(toks)
            ups = [(refs[t + e], 0) for e in range(n_a)] + grouped(refs[t + n_a : t + n_a + 2])
            first_body(n_a, n_c, refs[0], refs[1:t], ups, *refs[-3:])

        rows_x, early = kernel_call(
            first_half,
            [
                jax.ShapeDtypeStruct((tokens, model), BF16),
                jax.ShapeDtypeStruct((tokens, piece), BF16),
            ],
            scratch=[pltpu.VMEM((model, piece), BF16)],
            smem=1,
            n_in=1 + len(toks) + n_a + 2,
            mib=24,
        )(place, *toks, *mine, *up_x)

        def second_half(*refs):
            ups = grouped(refs[3:5]) + grouped(refs[5:7])
            pieces = [[refs[7]], [refs[8]], [refs[9]], [refs[10]]]
            lower_body(cols, *refs[:3], ups, pieces, *refs[11:])

        keep0, away0, hidden = kernel_call(
            second_half,
            sizes + [jax.ShapeDtypeStruct((tokens, units), BF16)],
            scratch=[
                pltpu.VMEM((model, piece), BF16),
                pltpu.VMEM((tokens, piece), BF16),
                pltpu.VMEM((units, part), BF16),
            ],
            smem=1,
            n_in=11,
            mib=28,
        )(place, rows_x, early, *up_y, *up_xy, down[0], down_x[0], down_y[0], *down_xy[0])
        got0 = send(away0, c=1)

        def last_columns(hidden_ref, own_ref, x_ref, y_ref, r0_ref, r1_ref, keep, away, down_all):
            pieces = [[own_ref], [x_ref], [y_ref], [r0_ref, r1_ref]]
            down_product(keep, away, hidden_ref[...], pieces, down_all)

        keep1, away1 = kernel_call(
            last_columns, sizes, scratch=[pltpu.VMEM((units, part), BF16)], n_in=6
        )(hidden, down[1], down_x[1], down_y[1], *down_xy[1])
        got1 = send(away1, c=1)
        halves = []
        for k, (keep, got) in enumerate([(keep0, got0), (keep1, got1)]):
            outs = kernel_call(
                fold_body, [jax.ShapeDtypeStruct((own, part), BF16)] * (n_a - 1), n_in=2
            )(keep, got)
            total = stream[:, k * part : (k + 1) * part] + keep[:own] + got[:own].astype(F32)
            for d in range(1, n_a):
                total = total + send(outs[d - 1], a=n_a - d).astype(F32)
            halves.append(total.astype(BF16))
        return jnp.concatenate(halves, axis=1)


    return jax.shard_map(on_device, **specs)
```

```python
import jax
import jax.numpy as jnp
from jax import lax
from jax.experimental import pallas as pl
from jax.experimental.pallas import tpu as pltpu
from jax.sharding import PartitionSpec as P


HEAD = 128
SUB = 64
EPS = 1e-06
HI = lax.Precision.HIGHEST
AXES = ("sp", "tp")
F32 = jnp.float32
BF16 = jnp.bfloat16


HEAD_K = 128
HEAD_V = 128
BLOCK = 64


def exact_parts(x):
    first = x.astype(BF16)
    rest = x - first.astype(F32)
    second = rest.astype(BF16)
    third = (rest - second.astype(F32)).astype(BF16)
    return first, second, third


def pack_logs(totals):
    lines = []
    for x in totals:
        lines += list(exact_parts(x))
    pad = 16 - len(lines)
    return jnp.concatenate(
        [x.astype(F32) for x in lines] + [jnp.zeros((pad, HEAD), F32)], axis=0
    ).astype(BF16)


def log_of(packed, heads, h):
    parts = packed[heads * HEAD :, :].astype(F32)
    return sum(parts[3 * h + k : 3 * h + k + 1, :] for k in range(3))


def as_column(row):
    return jnp.transpose(jnp.broadcast_to(row, (HEAD, HEAD)))


def gates_body(logits, values, gap, extra, gate_out, cum_out, packed):
    rows, width = logits.shape
    heads = width // HEAD
    z = logits[...].astype(F32)
    gate = gap[...] / (1.0 + jnp.exp(z))
    log_forget = jnp.log1p(-gate) + extra[...]
    r = lax.broadcasted_iota(jnp.int32, (rows, rows), 0)
    c = lax.broadcasted_iota(jnp.int32, (rows, rows), 1)
    lower = (r >= c).astype(F32)
    cum = jnp.dot(lower, log_forget, precision=HI, preferred_element_type=F32)
    gate_out[...] = gate
    cum_out[...] = cum
    total = cum[rows - 1 : rows, :]
    keys = gate * jnp.exp(total - cum)
    vals = values[...].astype(F32)
    for h in range(heads):
        ks = keys[:, h * HEAD : (h + 1) * HEAD]
        vs = vals[:, h * HEAD : (h + 1) * HEAD]
        state = lax.dot_general(
            ks, vs, (((0,), (0,)), ((), ())), precision=HI, preferred_element_type=F32
        )
        packed[h * HEAD : (h + 1) * HEAD, :] = state.astype(BF16)
    packed[heads * HEAD :, :] = pack_logs([total[:, h * HEAD : (h + 1) * HEAD] for h in range(heads)])


def local_body(query, gate, cum, values, out):
    rows, width = query.shape
    sub = min(SUB, rows)
    for h in range(width // HEAD):
        lanes = slice(h * HEAD, (h + 1) * HEAD)
        for i in range(rows // sub):
            lo, hi = i * sub, (i + 1) * sub
            mid = cum[lo + sub // 2 - 1 : lo + sub // 2, lanes]
            qs = query[lo:hi, lanes].astype(F32) * (HEAD**-0.5) * jnp.exp(cum[lo:hi, lanes] - mid)
            ks = gate[0:hi, lanes] * jnp.exp(mid - cum[0:hi, lanes])
            scores = lax.dot_general(
                qs, ks, (((1,), (1,)), ((), ())), precision=HI, preferred_element_type=F32
            )
            rr = lax.broadcasted_iota(jnp.int32, (sub, hi), 0) + lo
            cc = lax.broadcasted_iota(jnp.int32, (sub, hi), 1)
            scores = jnp.where(rr >= cc, scores, 0.0)
            out[lo:hi, lanes] = jnp.dot(
                scores, values[0:hi, lanes].astype(F32), precision=HI, preferred_element_type=F32
            )


def kernel_call(body, out_shape, scratch=(), smem=0, n_in=0, mib=16, fetched=False):
    specs = [pl.BlockSpec(memory_space=pltpu.SMEM)] * smem
    space = pltpu.HBM if fetched else pltpu.VMEM
    specs += [pl.BlockSpec(memory_space=space)] * (n_in - smem)
    many = isinstance(out_shape, (list, tuple))
    out_spec = pl.BlockSpec(memory_space=pltpu.VMEM)
    return pl.pallas_call(
        body,
        out_shape=out_shape,
        in_specs=specs,
        out_specs=[out_spec] * len(out_shape) if many else out_spec,
        scratch_shapes=list(scratch),
        compiler_params=pltpu.CompilerParams(vmem_limit_bytes=mib * 1024 * 1024),
    )


def fetch_then(body, n):
    def run(*refs):
        sources, outs, held, sems = refs[:n], refs[n : -n - 1], refs[-n - 1 : -1], refs[-1]
        copies = [
            pltpu.make_async_copy(src, dst, sems.at[k])
            for k, (src, dst) in enumerate(zip(sources, held))
        ]
        for copy in copies:
            copy.start()
        for copy in copies:
            copy.wait()
        body(*held, *outs)

    return run


def pair_body(place, mine, theirs, out):
    last = place[1] == 1
    heads = (mine.shape[0] - 16) // HEAD
    logs = []
    for h in range(heads):
        rows = slice(h * HEAD, (h + 1) * HEAD)
        own_log, their_log = log_of(mine, heads, h), log_of(theirs, heads, h)
        own_state, their_state = mine[rows, :].astype(F32), theirs[rows, :].astype(F32)
        decay = as_column(jnp.exp(jnp.where(last, own_log, their_log)))
        early = jnp.where(last, their_state, own_state)
        late = jnp.where(last, own_state, their_state)
        out[rows, :] = (decay * early + late).astype(BF16)
        logs.append(own_log + their_log)
    out[heads * HEAD :, :] = pack_logs(logs)


def mix_body(n_cores, *refs):
    place = refs[0]
    query, cum, local, gate_logits, gain, weight, beside = refs[1:8]
    states = refs[8:-4]
    first, second, away, mixed = refs[-4:]
    rows, width = query.shape
    heads = width // HEAD
    last = place[1] == 1
    for h in range(heads):
        lanes = slice(h * HEAD, (h + 1) * HEAD)
        arrived = jnp.where(last, beside[lanes, :].astype(F32), 0.0)
        passed = jnp.where(last, log_of(beside, heads, h), 0.0)
        for s in states:
            arrived = arrived + as_column(jnp.exp(passed)) * s[lanes, :].astype(F32)
            passed = passed + log_of(s, heads, h)
        reach = query[:, lanes].astype(F32) * (HEAD**-0.5) * jnp.exp(cum[:, lanes])
        rec = local[:, lanes] + jnp.dot(reach, arrived, precision=HI, preferred_element_type=F32)
        scale = lax.rsqrt(jnp.mean(rec * rec, axis=-1, keepdims=True) + EPS)
        v = gate_logits[:, lanes].astype(F32)
        mixed[:, lanes] = rec * scale * gain[...] * (v / (1.0 + jnp.exp(-v)))
    y, c = place[2], place[3]
    n_y = 2
    own = rows // (n_y * n_cores)
    picked = []
    for e in range(n_cores):
        for k in range(n_y):
            t = lax.rem(y + k, n_y) * n_cores + lax.rem(c + e, n_cores)
            picked.append(mixed[pl.ds(pl.multiple_of(t * own, own), own), :])
    ordered = jnp.concatenate(picked, axis=0).astype(BF16)
    part = jnp.dot(ordered, weight[...], preferred_element_type=F32)
    first[...] = part[:own]
    second[...] = part[own : n_y * own]
    away[...] = part[n_y * own :].astype(BF16)


def norm_body(own, beside, arrived, residual, gain, stream_out, normed_out):
    rows = own.shape[0]
    stream = own[...] + beside[:rows, :].astype(F32) + arrived[...].astype(F32)
    stream = stream + residual[...].astype(F32)
    stream_out[...] = stream
    scale = lax.rsqrt(jnp.mean(stream * stream, axis=-1, keepdims=True) + EPS)
    normed = (stream * scale * gain[...]).astype(BF16)
    blocks, _, cols = normed_out.shape
    for i in range(blocks):
        normed_out[i] = normed[:, i * cols : (i + 1) * cols]


def hidden_half(rows_x, ups, up_all, cols, out):
    at = 0
    for src, off in ups:
        up_all[at : at + cols, :] = src[off : off + cols, :]
        at += cols
    act = jnp.maximum(jnp.dot(rows_x[...], up_all[...], preferred_element_type=F32), 0.0)
    out[...] = (act * act).astype(BF16)


def first_body(n_a, n_cores, place, toks, ups, rows_x, hidden, up_all):
    a, b = place[0], place[1]
    n_b = len(ups) // n_a
    _, own, cols = toks[0].shape
    for i in range(n_a * n_cores):
        for x in range(n_b):
            for e in range(n_a):
                k = lax.rem(a - e + n_a, n_a) * n_b + lax.rem(b + x, n_b)
                at = (x * n_a + e) * cols
                rows_x[i * own : (i + 1) * own, at : at + cols] = toks[i][k]
    hidden_half(rows_x, ups, up_all, cols, hidden)


def down_product(keep, away, units, pieces, down_all):
    at = 0
    for group in pieces:
        for piece in group:
            src, off = piece
            n = src.shape[0]
            down_all[at : at + n, :] = src[:, off : off + down_all.shape[1]]
            at += n
    acc = jnp.dot(units, down_all[...], preferred_element_type=F32)
    cut = keep.shape[0]
    keep[...] = acc[:cut]
    away[...] = acc[cut:].astype(BF16)


def lower_body(cols, place, rows_x, early, ups, pieces, keep, away, ordered, up_all, late, down_all):
    hidden_half(rows_x, ups, up_all, cols, late)
    n_b = 2
    b = place[1]
    half = late.shape[1] // n_b
    for y, src in enumerate((early, late)):
        for x in range(n_b):
            k = lax.rem(b + x, n_b)
            at = (y * n_b + x) * half
            ordered[:, at : at + half] = src[:, pl.ds(pl.multiple_of(k * half, half), half)]
    down_product(keep, away, ordered[...], pieces, down_all)


def fold_body(keep, got, *outs):
    rows = outs[0].shape[0]
    for d in range(len(outs)):
        at = (d + 1) * rows
        outs[d][...] = (keep[at : at + rows, :] + got[at : at + rows, :].astype(F32)).astype(BF16)


norm_eps = 1e-06
highest_precision = lax.Precision.HIGHEST


def carried_in(part, axis, combine, identity):
    place = lax.axis_index(axis)
    gathered = jax.tree.map(lambda a: lax.all_gather(a, axis), part)
    state = jax.tree.map(lambda a, e: jnp.zeros_like(a) + jnp.asarray(e, a.dtype), part, identity)

    def one(step, state):
        return combine(
            state, jax.tree.map(lambda a: lax.dynamic_index_in_dim(a, step, 0, False), gathered)
        )

    return lax.fori_loop(0, place, one, state)


def block_update(carry_forward_state, block_inputs):
    query_rows_block, gate_rows_block, value_rows_block, log_block = block_inputs
    cumulative_log = jnp.cumsum(log_block, axis=1)
    length = query_rows_block.shape[1]
    causal = jnp.arange(length)[:, None] >= jnp.arange(length)[None, :]
    across_blocks = jnp.einsum(
        "dcj,djw->dcw",
        query_rows_block * jnp.exp(cumulative_log),
        carry_forward_state,
        precision=highest_precision,
    )
    spread = cumulative_log[:, :, None, :] - cumulative_log[:, None, :, :]
    decay_table = jnp.exp(jnp.where(causal[None, :, :, None], spread, -jnp.inf))
    scores = jnp.einsum(
        "htk,hsk,htsk->hts",
        query_rows_block,
        gate_rows_block,
        decay_table,
        precision=highest_precision,
    )
    within = jnp.einsum("hts,hsv->htv", scores, value_rows_block, precision=highest_precision)
    final_log_total = cumulative_log[:, -1:, :]
    updated_state = jnp.exp(final_log_total[:, 0, :])[
        :, :, None
    ] * carry_forward_state + jnp.einsum(
        "tri,trw->tiw",
        gate_rows_block * jnp.exp(final_log_total - cumulative_log),
        value_rows_block,
        precision=highest_precision,
    )
    return (updated_state, across_blocks + within)


def to_blocks(array, inner):
    length = array.shape[0]
    split_up = array.reshape(length // BLOCK, BLOCK, array.shape[1] // inner, inner)
    return jnp.transpose(split_up, (0, 2, 1, 3))


def from_blocks(blocked):
    joined = jnp.transpose(blocked, (0, 2, 1, 3))
    return joined.reshape(joined.shape[0] * joined.shape[1], joined.shape[2], joined.shape[3])


def prepare_inputs(query, forget_logits, written_values, forget_floor_gap, extra_log_decay):
    input_gate_value = forget_floor_gap[None, :] * jax.nn.sigmoid(
        -forget_logits.astype(jnp.float32)
    )
    forget_log_rate = jnp.log1p(-input_gate_value) + extra_log_decay
    scaled_values = query.astype(jnp.float32) * HEAD_K ** (-0.5)
    return (scaled_values, input_gate_value, written_values.astype(jnp.float32), forget_log_rate)


def gate_out(recurrent, output_gate_logits, head_norm_gain):
    normal_part = recurrent * lax.rsqrt(
        jnp.mean(recurrent * recurrent, axis=-1, keepdims=True) + norm_eps
    )
    gating = jax.nn.silu(output_gate_logits.astype(jnp.float32)).reshape(recurrent.shape)
    mixed = normal_part * head_norm_gain * gating
    return mixed.reshape(recurrent.shape[0], -1).astype(jnp.bfloat16)


def normalize(stream, gain):
    scaled_rows = stream * lax.rsqrt(jnp.mean(stream * stream, axis=-1, keepdims=True) + norm_eps)
    return (scaled_rows * gain).astype(jnp.bfloat16)


def chain_states(earlier, later):
    return (earlier[0] + later[0], jnp.exp(later[0])[:, :, None] * earlier[1] + later[1])


def gathered_plan(
    query,
    forget_logits,
    written_values,
    output_gate_logits,
    forget_floor_gap,
    extra_log_decay,
    head_norm_gain,
    output_weight,
    residual,
    mixer_norm_gain,
    mixer_up_weight,
    mixer_down_weight,
):
    scaled_values, input_gate_value, value_rows, forget_log_rate = prepare_inputs(
        query, forget_logits, written_values, forget_floor_gap, extra_log_decay
    )
    row_count, local_width = query.shape
    head_count = local_width // HEAD_K
    start_state = jnp.zeros((head_count, HEAD_K, HEAD_V), jnp.float32)
    local_state, blocked = lax.scan(
        block_update,
        start_state,
        (
            to_blocks(scaled_values, HEAD_K),
            to_blocks(input_gate_value, HEAD_K),
            to_blocks(value_rows, HEAD_V),
            to_blocks(forget_log_rate, HEAD_K),
        ),
    )
    log_total = jnp.sum(forget_log_rate, axis=0).reshape(head_count, HEAD_K)
    arrived_state = carried_in(
        (log_total, local_state),
        "sp",
        chain_states,
        (jnp.zeros_like(log_total), jnp.zeros_like(local_state)),
    )
    running = jnp.cumsum(forget_log_rate, axis=0)
    reached_state = (scaled_values * jnp.exp(running)).reshape(row_count, head_count, HEAD_K)
    carried_over = jnp.einsum(
        "cja,jae->cje", reached_state, arrived_state[1], precision=highest_precision
    )
    mixed = gate_out(from_blocks(blocked) + carried_over, output_gate_logits, head_norm_gain)
    stream_own = lax.psum_scatter(
        jnp.dot(mixed, output_weight, preferred_element_type=jnp.float32).astype(jnp.bfloat16),
        "tp",
        scatter_dimension=0,
        tiled=True,
    ).astype(jnp.float32) + residual.astype(jnp.float32)
    normed = lax.all_gather(normalize(stream_own, mixer_norm_gain), "tp", axis=0, tiled=True)
    columns = normed
    lifted = jnp.dot(
        columns,
        lax.all_gather(mixer_up_weight, "sp", axis=0, tiled=True),
        preferred_element_type=jnp.float32,
    )
    hidden = jnp.square(jax.nn.relu(lifted)).astype(jnp.bfloat16)
    columns = hidden
    projected = jnp.dot(
        columns,
        lax.all_gather(mixer_down_weight, "sp", axis=0, tiled=True),
        preferred_element_type=jnp.float32,
    )
    mlp_own = lax.psum_scatter(
        projected.astype(jnp.bfloat16), "tp", scatter_dimension=0, tiled=True
    ).astype(jnp.float32)
    return (stream_own + mlp_own).astype(jnp.bfloat16)


def solution(mesh):
    specs = dict(
        mesh=mesh,
        in_specs=(
            P("sp", "tp"),
            P("sp", "tp"),
            P("sp", "tp"),
            P("sp", "tp"),
            P("tp"),
            P("sp", "tp"),
            P(),
            P("tp", None),
            P(("sp", "tp"), None),
            P(),
            P("sp", "tp"),
            P(("tp", "sp"), None),
        ),
        out_specs=P(("sp", "tp"), None),
        check_vma=False,
    )
    n_sp, n_tp = mesh.shape["sp"], mesh.shape["tp"]
    n_b, n_y = 2, 2
    n_a, n_c = n_sp // n_b, n_tp // n_y
    if n_sp % n_b or n_tp % n_y or n_a > 4 or n_c != 2:
        return jax.shard_map(gathered_plan, **specs)

    def flat(a, b, y, c):
        return (a % n_a * n_b + b % n_b) * n_tp + y % n_y * n_c + c % n_c

    def send(x, a=0, b=0, y=0, c=0, cyclic=True):
        pairs = [
            (flat(i, j, k, m), flat(i + a, j + b, k + y, m + c))
            for i in range(n_a)
            for j in range(n_b)
            for k in range(n_y)
            for m in range(n_c)
            if cyclic or i + a < n_a
        ]
        return lax.ppermute(x, AXES, pairs)

    def on_device(
        query,
        forget_logits,
        written_values,
        output_gate_logits,
        forget_floor_gap,
        extra_log_decay,
        head_norm_gain,
        output_weight,
        residual,
        mixer_norm_gain,
        mixer_up_weight,
        mixer_down_weight,
    ):
        sp, tp = lax.axis_index("sp"), lax.axis_index("tp")
        a, b, y, c = sp // n_b, sp % n_b, tp // n_c, tp % n_c
        place = jnp.stack([a, b, y, c]).astype(jnp.int32)
        rows, width = query.shape
        model = output_weight.shape[1]
        own = residual.shape[0]
        heads = width // HEAD

        packed_shape = jax.ShapeDtypeStruct((heads * HEAD + 16, HEAD), BF16)
        gate, cum, packed = kernel_call(
            fetch_then(gates_body, 4),
            [
                jax.ShapeDtypeStruct((rows, width), F32),
                jax.ShapeDtypeStruct((rows, width), F32),
                packed_shape,
            ],
            scratch=[
                pltpu.VMEM((rows, width), BF16),
                pltpu.VMEM((rows, width), BF16),
                pltpu.VMEM((1, width), F32),
                pltpu.VMEM((rows, width), F32),
                pltpu.SemaphoreType.DMA((4,)),
            ],
            n_in=4,
            fetched=True,
        )(forget_logits, written_values, forget_floor_gap[None, :], extra_log_decay)
        up_rows, up_cols = mixer_up_weight.shape
        piece = up_cols // n_a
        mine = []
        for d in range(n_a):
            cut = lax.dynamic_slice(mixer_up_weight, (0, (a + d) % n_a * piece), (up_rows, piece))
            mine.append(cut if d == 0 else send(cut, a=d))
        up_x, up_y = [], []
        for g in range(2):
            joined = jnp.concatenate(mine[g::2], axis=0)
            up_x.append(send(joined, b=1))
            up_y.append(send(joined, y=1))
        up_xy = [send(up_x[0], y=1), send(up_y[1], b=1)]

        def grouped(refs):
            return [(refs[e % 2], e // 2 * up_rows) for e in range(n_a)]

        part = model // 2
        half = mixer_down_weight.shape[0] // 2
        down_x = send(mixer_down_weight, b=1)
        down_y = send(mixer_down_weight, y=1)
        down_xy = []
        for k in range(2):
            lanes = slice(k * part, (k + 1) * part)
            down_xy.append([send(down_x[:half, lanes], y=1), send(down_y[half:, lanes], b=1)])
        whole = [mixer_down_weight, down_x, down_y]

        beside = send(packed, b=1)
        pair = kernel_call(pair_body, packed_shape, smem=1, n_in=3)(place, packed, beside)
        states = [send(pair, a=d, cyclic=False) for d in range(1, n_a)]
        local = kernel_call(
            local_body, jax.ShapeDtypeStruct((rows, width), F32), n_in=4
        )(query, gate, cum, written_values)
        first, second, away = kernel_call(
            lambda *refs: mix_body(n_c, *refs),
            [
                jax.ShapeDtypeStruct((own, model), F32),
                jax.ShapeDtypeStruct((own, model), F32),
                jax.ShapeDtypeStruct((n_y * own, model), BF16),
            ],
            scratch=[pltpu.VMEM((rows, width), F32)],
            smem=1,
            n_in=8 + len(states),
        )(
            place,
            query,
            cum,
            local,
            output_gate_logits,
            head_norm_gain[None, :],
            output_weight,
            beside,
            *states,
        )
        got = send(away, c=1)
        other = send((second + got[own:].astype(F32)).astype(BF16), y=1)
        stream, normed = kernel_call(
            norm_body,
            [
                jax.ShapeDtypeStruct((own, model), F32),
                jax.ShapeDtypeStruct((n_sp, own, model // n_sp), BF16),
            ],
            n_in=5,
        )(first, got, other, residual, mixer_norm_gain[None, :])

        line = [normed] + [send(normed, a=d) for d in range(1, n_a)]
        toks = line + [send(u, c=1) for u in line]
        group = n_a * own
        tokens = n_c * group
        units = n_y * piece
        cols = model // n_sp
        sizes = [
            jax.ShapeDtypeStruct((group, part), F32),
            jax.ShapeDtypeStruct((tokens - group, part), BF16),
        ]

        def first_half(*refs):
            t = 1 + len(toks)
            ups = [(refs[t + e], 0) for e in range(n_a)] + grouped(refs[t + n_a : t + n_a + 2])
            first_body(n_a, n_c, refs[0], refs[1:t], ups, *refs[-3:])

        rows_x, early = kernel_call(
            first_half,
            [
                jax.ShapeDtypeStruct((tokens, model), BF16),
                jax.ShapeDtypeStruct((tokens, piece), BF16),
            ],
            scratch=[pltpu.VMEM((model, piece), BF16)],
            smem=1,
            n_in=1 + len(toks) + n_a + 2,
            mib=24,
        )(place, *toks, *mine, *up_x)

        def second_half(*refs):
            ups = grouped(refs[3:5]) + grouped(refs[5:7])
            pieces = [[(r, 0)] for r in refs[7:10]] + [[(refs[10], 0), (refs[11], 0)]]
            lower_body(cols, *refs[:3], ups, pieces, *refs[12:])

        keep0, away0, hidden = kernel_call(
            second_half,
            sizes + [jax.ShapeDtypeStruct((tokens, units), BF16)],
            scratch=[
                pltpu.VMEM((model, piece), BF16),
                pltpu.VMEM((tokens, piece), BF16),
                pltpu.VMEM((units, part), BF16),
            ],
            smem=1,
            n_in=12,
            mib=30,
        )(place, rows_x, early, *up_y, *up_xy, *whole, *down_xy[0])
        got0 = send(away0, c=1)

        def last_columns(hidden_ref, own_ref, x_ref, y_ref, r0_ref, r1_ref, keep, away, down_all):
            pieces = [[(r, part)] for r in (own_ref, x_ref, y_ref)]
            pieces.append([(r0_ref, 0), (r1_ref, 0)])
            down_product(keep, away, hidden_ref[...], pieces, down_all)

        keep1, away1 = kernel_call(
            last_columns, sizes, scratch=[pltpu.VMEM((units, part), BF16)], n_in=6
        )(hidden, *whole, *down_xy[1])
        got1 = send(away1, c=1)
        halves = []
        for k, (keep, got) in enumerate([(keep0, got0), (keep1, got1)]):
            outs = kernel_call(
                fold_body, [jax.ShapeDtypeStruct((own, part), BF16)] * (n_a - 1), n_in=2
            )(keep, got)
            total = stream[:, k * part : (k + 1) * part] + keep[:own] + got[:own].astype(F32)
            for d in range(1, n_a):
                total = total + send(outs[d - 1], a=n_a - d).astype(F32)
            halves.append(total.astype(BF16))
        return jnp.concatenate(halves, axis=1)


    return jax.shard_map(on_device, **specs)
```

```python
import jax
import jax.numpy as jnp
from jax import lax
from jax.experimental import pallas as pl
from jax.experimental.pallas import tpu as pltpu
from jax.sharding import PartitionSpec as P


HEAD = 128
SUB = 64
EPS = 1e-06
HI = lax.Precision.HIGHEST
AXES = ("sp", "tp")
F32 = jnp.float32
BF16 = jnp.bfloat16


HEAD_K = 128
HEAD_V = 128
BLOCK = 64


def exact_parts(x):
    first = x.astype(BF16)
    rest = x - first.astype(F32)
    second = rest.astype(BF16)
    third = (rest - second.astype(F32)).astype(BF16)
    return first, second, third


def pack_logs(totals):
    lines = []
    for x in totals:
        lines += list(exact_parts(x))
    pad = 16 - len(lines)
    return jnp.concatenate(
        [x.astype(F32) for x in lines] + [jnp.zeros((pad, HEAD), F32)], axis=0
    ).astype(BF16)


def log_of(packed, heads, h):
    parts = packed[heads * HEAD :, :].astype(F32)
    return sum(parts[3 * h + k : 3 * h + k + 1, :] for k in range(3))


def as_column(row):
    return jnp.transpose(jnp.broadcast_to(row, (HEAD, HEAD)))


def gates_body(logits, values, gap, extra, gate_out, cum_out, packed):
    rows, width = logits.shape
    heads = width // HEAD
    z = logits[...].astype(F32)
    gate = gap[...] / (1.0 + jnp.exp(z))
    log_forget = jnp.log1p(-gate) + extra[...]
    r = lax.broadcasted_iota(jnp.int32, (rows, rows), 0)
    c = lax.broadcasted_iota(jnp.int32, (rows, rows), 1)
    lower = (r >= c).astype(F32)
    cum = jnp.dot(lower, log_forget, precision=HI, preferred_element_type=F32)
    gate_out[...] = gate
    cum_out[...] = cum
    total = cum[rows - 1 : rows, :]
    keys = gate * jnp.exp(total - cum)
    vals = values[...].astype(F32)
    for h in range(heads):
        ks = keys[:, h * HEAD : (h + 1) * HEAD]
        vs = vals[:, h * HEAD : (h + 1) * HEAD]
        state = lax.dot_general(
            ks, vs, (((0,), (0,)), ((), ())), precision=HI, preferred_element_type=F32
        )
        packed[h * HEAD : (h + 1) * HEAD, :] = state.astype(BF16)
    packed[heads * HEAD :, :] = pack_logs([total[:, h * HEAD : (h + 1) * HEAD] for h in range(heads)])


def local_body(query, gate, cum, values, out):
    rows, width = query.shape
    sub = min(SUB, rows)
    for h in range(width // HEAD):
        lanes = slice(h * HEAD, (h + 1) * HEAD)
        for i in range(rows // sub):
            lo, hi = i * sub, (i + 1) * sub
            mid = cum[lo + sub // 2 - 1 : lo + sub // 2, lanes]
            qs = query[lo:hi, lanes].astype(F32) * (HEAD**-0.5) * jnp.exp(cum[lo:hi, lanes] - mid)
            ks = gate[0:hi, lanes] * jnp.exp(mid - cum[0:hi, lanes])
            scores = lax.dot_general(
                qs, ks, (((1,), (1,)), ((), ())), precision=HI, preferred_element_type=F32
            )
            rr = lax.broadcasted_iota(jnp.int32, (sub, hi), 0) + lo
            cc = lax.broadcasted_iota(jnp.int32, (sub, hi), 1)
            scores = jnp.where(rr >= cc, scores, 0.0)
            out[lo:hi, lanes] = jnp.dot(
                scores, values[0:hi, lanes].astype(F32), precision=HI, preferred_element_type=F32
            )


def kernel_call(body, out_shape, scratch=(), smem=0, n_in=0, mib=16, fetched=False):
    specs = [pl.BlockSpec(memory_space=pltpu.SMEM)] * smem
    space = pltpu.HBM if fetched else pltpu.VMEM
    specs += [pl.BlockSpec(memory_space=space)] * (n_in - smem)
    many = isinstance(out_shape, (list, tuple))
    out_spec = pl.BlockSpec(memory_space=pltpu.VMEM)
    return pl.pallas_call(
        body,
        out_shape=out_shape,
        in_specs=specs,
        out_specs=[out_spec] * len(out_shape) if many else out_spec,
        scratch_shapes=list(scratch),
        compiler_params=pltpu.CompilerParams(vmem_limit_bytes=mib * 1024 * 1024),
    )


def fetch_then(body, n):
    def run(*refs):
        sources, outs, held, sems = refs[:n], refs[n : -n - 1], refs[-n - 1 : -1], refs[-1]
        copies = [
            pltpu.make_async_copy(src, dst, sems.at[k])
            for k, (src, dst) in enumerate(zip(sources, held))
        ]
        for copy in copies:
            copy.start()
        for copy in copies:
            copy.wait()
        body(*held, *outs)

    return run


def pair_body(place, mine, theirs, out):
    last = place[1] == 1
    heads = (mine.shape[0] - 16) // HEAD
    logs = []
    for h in range(heads):
        rows = slice(h * HEAD, (h + 1) * HEAD)
        own_log, their_log = log_of(mine, heads, h), log_of(theirs, heads, h)
        own_state, their_state = mine[rows, :].astype(F32), theirs[rows, :].astype(F32)
        decay = as_column(jnp.exp(jnp.where(last, own_log, their_log)))
        early = jnp.where(last, their_state, own_state)
        late = jnp.where(last, own_state, their_state)
        out[rows, :] = (decay * early + late).astype(BF16)
        logs.append(own_log + their_log)
    out[heads * HEAD :, :] = pack_logs(logs)


def mix_body(n_cores, *refs):
    place = refs[0]
    query, cum, local, gate_logits, gain, weight, beside = refs[1:8]
    states = refs[8:-4]
    first, second, away, mixed = refs[-4:]
    rows, width = query.shape
    heads = width // HEAD
    last = place[1] == 1
    for h in range(heads):
        lanes = slice(h * HEAD, (h + 1) * HEAD)
        arrived = jnp.where(last, beside[lanes, :].astype(F32), 0.0)
        passed = jnp.where(last, log_of(beside, heads, h), 0.0)
        for s in states:
            arrived = arrived + as_column(jnp.exp(passed)) * s[lanes, :].astype(F32)
            passed = passed + log_of(s, heads, h)
        reach = query[:, lanes].astype(F32) * (HEAD**-0.5) * jnp.exp(cum[:, lanes])
        rec = local[:, lanes] + jnp.dot(reach, arrived, precision=HI, preferred_element_type=F32)
        scale = lax.rsqrt(jnp.mean(rec * rec, axis=-1, keepdims=True) + EPS)
        v = gate_logits[:, lanes].astype(F32)
        mixed[:, lanes] = rec * scale * gain[...] * (v / (1.0 + jnp.exp(-v)))
    y, c = place[2], place[3]
    n_y = 2
    own = rows // (n_y * n_cores)
    picked = []
    for e in range(n_cores):
        for k in range(n_y):
            t = lax.rem(y + k, n_y) * n_cores + lax.rem(c + e, n_cores)
            picked.append(mixed[pl.ds(pl.multiple_of(t * own, own), own), :])
    ordered = jnp.concatenate(picked, axis=0).astype(BF16)
    part = jnp.dot(ordered, weight[...], preferred_element_type=F32)
    first[...] = part[:own]
    second[...] = part[own : n_y * own]
    away[...] = part[n_y * own :].astype(BF16)


def norm_body(own, beside, arrived, residual, gain, stream_out, normed_out):
    rows = own.shape[0]
    stream = own[...] + beside[:rows, :].astype(F32) + arrived[...].astype(F32)
    stream = stream + residual[...].astype(F32)
    stream_out[...] = stream
    scale = lax.rsqrt(jnp.mean(stream * stream, axis=-1, keepdims=True) + EPS)
    normed = (stream * scale * gain[...]).astype(BF16)
    blocks, _, cols = normed_out.shape
    for i in range(blocks):
        normed_out[i] = normed[:, i * cols : (i + 1) * cols]


def hidden_half(rows_x, ups, up_all, cols, out):
    at = 0
    for src, off in ups:
        up_all[at : at + cols, :] = src[off : off + cols, :]
        at += cols
    act = jnp.maximum(jnp.dot(rows_x[...], up_all[...], preferred_element_type=F32), 0.0)
    out[...] = (act * act).astype(BF16)


def first_body(n_a, n_cores, place, toks, ups, rows_x, hidden, up_all):
    a, b = place[0], place[1]
    n_b = len(ups) // n_a
    _, own, cols = toks[0].shape
    for i in range(n_a * n_cores):
        for x in range(n_b):
            for e in range(n_a):
                k = lax.rem(a - e + n_a, n_a) * n_b + lax.rem(b + x, n_b)
                at = (x * n_a + e) * cols
                rows_x[i * own : (i + 1) * own, at : at + cols] = toks[i][k]
    hidden_half(rows_x, ups, up_all, cols, hidden)


def down_product(keep, away, units, pieces, down_all):
    at = 0
    for group in pieces:
        for piece in group:
            src, off = piece
            n = src.shape[0]
            down_all[at : at + n, :] = src[:, off : off + down_all.shape[1]]
            at += n
    acc = jnp.dot(units, down_all[...], preferred_element_type=F32)
    cut = keep.shape[0]
    keep[...] = acc[:cut]
    away[...] = acc[cut:].astype(BF16)


def lower_body(cols, place, rows_x, early, ups, pieces, keep, away, ordered, up_all, late, down_all):
    hidden_half(rows_x, ups, up_all, cols, late)
    n_b = 2
    b = place[1]
    half = late.shape[1] // n_b
    for y, src in enumerate((early, late)):
        for x in range(n_b):
            k = lax.rem(b + x, n_b)
            at = (y * n_b + x) * half
            ordered[:, at : at + half] = src[:, pl.ds(pl.multiple_of(k * half, half), half)]
    down_product(keep, away, ordered[...], pieces, down_all)


def fold_body(keep, got, near, held):
    rows = near.shape[0] // 2
    for k in range(2):
        for out, block in ((held, 2 * k), (near, 2 * k + 1)):
            src = slice(block * rows, (block + 1) * rows)
            both = keep[src, :] + got[src, :].astype(F32)
            out[k * rows : (k + 1) * rows, :] = both.astype(out.dtype)


norm_eps = 1e-06
highest_precision = lax.Precision.HIGHEST


def carried_in(part, axis, combine, identity):
    place = lax.axis_index(axis)
    gathered = jax.tree.map(lambda a: lax.all_gather(a, axis), part)
    state = jax.tree.map(lambda a, e: jnp.zeros_like(a) + jnp.asarray(e, a.dtype), part, identity)

    def one(step, state):
        return combine(
            state, jax.tree.map(lambda a: lax.dynamic_index_in_dim(a, step, 0, False), gathered)
        )

    return lax.fori_loop(0, place, one, state)


def block_update(carry_forward_state, block_inputs):
    query_rows_block, gate_rows_block, value_rows_block, log_block = block_inputs
    cumulative_log = jnp.cumsum(log_block, axis=1)
    length = query_rows_block.shape[1]
    causal = jnp.arange(length)[:, None] >= jnp.arange(length)[None, :]
    across_blocks = jnp.einsum(
        "dcj,djw->dcw",
        query_rows_block * jnp.exp(cumulative_log),
        carry_forward_state,
        precision=highest_precision,
    )
    spread = cumulative_log[:, :, None, :] - cumulative_log[:, None, :, :]
    decay_table = jnp.exp(jnp.where(causal[None, :, :, None], spread, -jnp.inf))
    scores = jnp.einsum(
        "htk,hsk,htsk->hts",
        query_rows_block,
        gate_rows_block,
        decay_table,
        precision=highest_precision,
    )
    within = jnp.einsum("hts,hsv->htv", scores, value_rows_block, precision=highest_precision)
    final_log_total = cumulative_log[:, -1:, :]
    updated_state = jnp.exp(final_log_total[:, 0, :])[
        :, :, None
    ] * carry_forward_state + jnp.einsum(
        "tri,trw->tiw",
        gate_rows_block * jnp.exp(final_log_total - cumulative_log),
        value_rows_block,
        precision=highest_precision,
    )
    return (updated_state, across_blocks + within)


def to_blocks(array, inner):
    length = array.shape[0]
    split_up = array.reshape(length // BLOCK, BLOCK, array.shape[1] // inner, inner)
    return jnp.transpose(split_up, (0, 2, 1, 3))


def from_blocks(blocked):
    joined = jnp.transpose(blocked, (0, 2, 1, 3))
    return joined.reshape(joined.shape[0] * joined.shape[1], joined.shape[2], joined.shape[3])


def prepare_inputs(query, forget_logits, written_values, forget_floor_gap, extra_log_decay):
    input_gate_value = forget_floor_gap[None, :] * jax.nn.sigmoid(
        -forget_logits.astype(jnp.float32)
    )
    forget_log_rate = jnp.log1p(-input_gate_value) + extra_log_decay
    scaled_values = query.astype(jnp.float32) * HEAD_K ** (-0.5)
    return (scaled_values, input_gate_value, written_values.astype(jnp.float32), forget_log_rate)


def gate_out(recurrent, output_gate_logits, head_norm_gain):
    normal_part = recurrent * lax.rsqrt(
        jnp.mean(recurrent * recurrent, axis=-1, keepdims=True) + norm_eps
    )
    gating = jax.nn.silu(output_gate_logits.astype(jnp.float32)).reshape(recurrent.shape)
    mixed = normal_part * head_norm_gain * gating
    return mixed.reshape(recurrent.shape[0], -1).astype(jnp.bfloat16)


def normalize(stream, gain):
    scaled_rows = stream * lax.rsqrt(jnp.mean(stream * stream, axis=-1, keepdims=True) + norm_eps)
    return (scaled_rows * gain).astype(jnp.bfloat16)


def chain_states(earlier, later):
    return (earlier[0] + later[0], jnp.exp(later[0])[:, :, None] * earlier[1] + later[1])


def gathered_plan(
    query,
    forget_logits,
    written_values,
    output_gate_logits,
    forget_floor_gap,
    extra_log_decay,
    head_norm_gain,
    output_weight,
    residual,
    mixer_norm_gain,
    mixer_up_weight,
    mixer_down_weight,
):
    scaled_values, input_gate_value, value_rows, forget_log_rate = prepare_inputs(
        query, forget_logits, written_values, forget_floor_gap, extra_log_decay
    )
    row_count, local_width = query.shape
    head_count = local_width // HEAD_K
    start_state = jnp.zeros((head_count, HEAD_K, HEAD_V), jnp.float32)
    local_state, blocked = lax.scan(
        block_update,
        start_state,
        (
            to_blocks(scaled_values, HEAD_K),
            to_blocks(input_gate_value, HEAD_K),
            to_blocks(value_rows, HEAD_V),
            to_blocks(forget_log_rate, HEAD_K),
        ),
    )
    log_total = jnp.sum(forget_log_rate, axis=0).reshape(head_count, HEAD_K)
    arrived_state = carried_in(
        (log_total, local_state),
        "sp",
        chain_states,
        (jnp.zeros_like(log_total), jnp.zeros_like(local_state)),
    )
    running = jnp.cumsum(forget_log_rate, axis=0)
    reached_state = (scaled_values * jnp.exp(running)).reshape(row_count, head_count, HEAD_K)
    carried_over = jnp.einsum(
        "cja,jae->cje", reached_state, arrived_state[1], precision=highest_precision
    )
    mixed = gate_out(from_blocks(blocked) + carried_over, output_gate_logits, head_norm_gain)
    stream_own = lax.psum_scatter(
        jnp.dot(mixed, output_weight, preferred_element_type=jnp.float32).astype(jnp.bfloat16),
        "tp",
        scatter_dimension=0,
        tiled=True,
    ).astype(jnp.float32) + residual.astype(jnp.float32)
    normed = lax.all_gather(normalize(stream_own, mixer_norm_gain), "tp", axis=0, tiled=True)
    columns = normed
    lifted = jnp.dot(
        columns,
        lax.all_gather(mixer_up_weight, "sp", axis=0, tiled=True),
        preferred_element_type=jnp.float32,
    )
    hidden = jnp.square(jax.nn.relu(lifted)).astype(jnp.bfloat16)
    columns = hidden
    projected = jnp.dot(
        columns,
        lax.all_gather(mixer_down_weight, "sp", axis=0, tiled=True),
        preferred_element_type=jnp.float32,
    )
    mlp_own = lax.psum_scatter(
        projected.astype(jnp.bfloat16), "tp", scatter_dimension=0, tiled=True
    ).astype(jnp.float32)
    return (stream_own + mlp_own).astype(jnp.bfloat16)


def solution(mesh):
    specs = dict(
        mesh=mesh,
        in_specs=(
            P("sp", "tp"),
            P("sp", "tp"),
            P("sp", "tp"),
            P("sp", "tp"),
            P("tp"),
            P("sp", "tp"),
            P(),
            P("tp", None),
            P(("sp", "tp"), None),
            P(),
            P("sp", "tp"),
            P(("tp", "sp"), None),
        ),
        out_specs=P(("sp", "tp"), None),
        check_vma=False,
    )
    n_sp, n_tp = mesh.shape["sp"], mesh.shape["tp"]
    n_b, n_y = 2, 2
    n_a, n_c = n_sp // n_b, n_tp // n_y
    if n_sp % n_b or n_tp % n_y or n_a != 4 or n_c != 2:
        return jax.shard_map(gathered_plan, **specs)

    def flat(a, b, y, c):
        return (a % n_a * n_b + b % n_b) * n_tp + y % n_y * n_c + c % n_c

    def send(x, a=0, b=0, y=0, c=0, flip=0, cyclic=True):
        pairs = [
            (flat(i, j, k, m), flat((i ^ flip) + a, j + b, k + y, m + c))
            for i in range(n_a)
            for j in range(n_b)
            for k in range(n_y)
            for m in range(n_c)
            if cyclic or i + a < n_a
        ]
        return lax.ppermute(x, AXES, pairs)

    def on_device(
        query,
        forget_logits,
        written_values,
        output_gate_logits,
        forget_floor_gap,
        extra_log_decay,
        head_norm_gain,
        output_weight,
        residual,
        mixer_norm_gain,
        mixer_up_weight,
        mixer_down_weight,
    ):
        sp, tp = lax.axis_index("sp"), lax.axis_index("tp")
        a, b, y, c = sp // n_b, sp % n_b, tp // n_c, tp % n_c
        place = jnp.stack([a, b, y, c]).astype(jnp.int32)
        rows, width = query.shape
        model = output_weight.shape[1]
        own = residual.shape[0]
        heads = width // HEAD

        packed_shape = jax.ShapeDtypeStruct((heads * HEAD + 16, HEAD), BF16)
        gate, cum, packed = kernel_call(
            fetch_then(gates_body, 4),
            [
                jax.ShapeDtypeStruct((rows, width), F32),
                jax.ShapeDtypeStruct((rows, width), F32),
                packed_shape,
            ],
            scratch=[
                pltpu.VMEM((rows, width), BF16),
                pltpu.VMEM((rows, width), BF16),
                pltpu.VMEM((1, width), F32),
                pltpu.VMEM((rows, width), F32),
                pltpu.SemaphoreType.DMA((4,)),
            ],
            n_in=4,
            fetched=True,
            mib=60,
        )(forget_logits, written_values, forget_floor_gap[None, :], extra_log_decay)
        up_rows, up_cols = mixer_up_weight.shape
        piece = up_cols // n_a
        mine = []
        for d in range(n_a):
            cut = lax.dynamic_slice(mixer_up_weight, (0, (a + d) % n_a * piece), (up_rows, piece))
            mine.append(cut if d == 0 else send(cut, a=d))

        def grouped(refs):
            return [(refs[0], 0), (refs[2], 0), (refs[1], 0), (refs[2], up_rows)]

        part = model // 2
        half = mixer_down_weight.shape[0] // 2
        down_x = send(mixer_down_weight, b=1)
        down_y = send(mixer_down_weight, y=1)
        down_xy = []
        for k in range(2):
            lanes = slice(k * part, (k + 1) * part)
            down_xy.append([send(down_x[:half, lanes], y=1), send(down_y[half:, lanes], b=1)])
        whole = [mixer_down_weight, down_x, down_y]

        beside = send(packed, b=1)
        pair = kernel_call(pair_body, packed_shape, smem=1, n_in=3)(place, packed, beside)
        states = [send(pair, a=d, cyclic=False) for d in range(1, n_a)]
        local = kernel_call(
            local_body, jax.ShapeDtypeStruct((rows, width), F32), n_in=4
        )(query, gate, cum, written_values)
        first, second, away = kernel_call(
            lambda *refs: mix_body(n_c, *refs),
            [
                jax.ShapeDtypeStruct((own, model), F32),
                jax.ShapeDtypeStruct((own, model), F32),
                jax.ShapeDtypeStruct((n_y * own, model), BF16),
            ],
            scratch=[pltpu.VMEM((rows, width), F32)],
            smem=1,
            n_in=8 + len(states),
        )(
            place,
            query,
            cum,
            local,
            output_gate_logits,
            head_norm_gain[None, :],
            output_weight,
            beside,
            *states,
        )
        got = send(away, c=1)
        second = (second + got[own:].astype(F32)).astype(BF16)
        other = send(second, y=1)
        late = lax.optimization_barrier((mine[1], mine[3], second))[:2]
        up_x, up_y = [], []
        for members in [mine[0], mine[2], jnp.concatenate(late, axis=0)]:
            up_x.append(send(members, b=1))
            up_y.append(send(members, y=1))
        up_xy = [send(up_x[0], y=1), send(up_x[1], y=1), send(up_y[2], b=1)]
        stream, normed = kernel_call(
            norm_body,
            [
                jax.ShapeDtypeStruct((own, model), F32),
                jax.ShapeDtypeStruct((n_sp, own, model // n_sp), BF16),
            ],
            n_in=5,
        )(first, got, other, residual, mixer_norm_gain[None, :])

        line = [normed] + [send(normed, flip=d) for d in range(1, n_a)]
        toks = line + [send(u, c=1) for u in line]
        group = n_a * own
        tokens = n_c * group
        units = n_y * piece
        cols = model // n_sp
        sizes = [
            jax.ShapeDtypeStruct((group, part), F32),
            jax.ShapeDtypeStruct((tokens - group, part), BF16),
        ]

        def first_half(*refs):
            t = 1 + len(toks)
            ups = [(refs[t + e], 0) for e in range(n_a)] + grouped(refs[t + n_a : t + n_a + 3])
            first_body(n_a, n_c, refs[0], refs[1:t], ups, *refs[-3:])

        rows_x, early = kernel_call(
            first_half,
            [
                jax.ShapeDtypeStruct((tokens, model), BF16),
                jax.ShapeDtypeStruct((tokens, piece), BF16),
            ],
            scratch=[pltpu.VMEM((model, piece), BF16)],
            smem=1,
            n_in=1 + len(toks) + n_a + 3,
            mib=24,
        )(place, *toks, *mine, *up_x)

        def second_half(*refs):
            ups = grouped(refs[3:6]) + grouped(refs[6:9])
            pieces = [[(r, 0)] for r in refs[9:12]] + [[(refs[12], 0), (refs[13], 0)]]
            lower_body(cols, *refs[:3], ups, pieces, *refs[14:])

        keep0, away0, hidden = kernel_call(
            second_half,
            sizes + [jax.ShapeDtypeStruct((tokens, units), BF16)],
            scratch=[
                pltpu.VMEM((model, piece), BF16),
                pltpu.VMEM((tokens, piece), BF16),
                pltpu.VMEM((units, part), BF16),
            ],
            smem=1,
            n_in=14,
            mib=30,
        )(place, rows_x, early, *up_y, *up_xy, *whole, *down_xy[0])
        got0 = send(away0, c=1)

        def last_columns(hidden_ref, own_ref, x_ref, y_ref, r0_ref, r1_ref, keep, away, down_all):
            pieces = [[(r, part)] for r in (own_ref, x_ref, y_ref)]
            pieces.append([(r0_ref, 0), (r1_ref, 0)])
            down_product(keep, away, hidden_ref[...], pieces, down_all)

        keep1, away1 = kernel_call(
            last_columns, sizes, scratch=[pltpu.VMEM((units, part), BF16)], n_in=6
        )(hidden, *whole, *down_xy[1])
        got1 = send(away1, c=1)
        halves = []
        for k, (keep, got) in enumerate([(keep0, got0), (keep1, got1)]):
            near, held = kernel_call(
                fold_body,
                [
                    jax.ShapeDtypeStruct((n_b * own, part), BF16),
                    jax.ShapeDtypeStruct((n_b * own, part), F32),
                ],
                n_in=2,
            )(keep, got)
            near = send(near, flip=1)
            far = (held[own:] + near[own:].astype(F32)).astype(BF16)
            far = send(far, flip=2)
            total = stream[:, k * part : (k + 1) * part] + held[:own] + near[:own].astype(F32)
            total = total + far.astype(F32)
            halves.append(total.astype(BF16))
        return jnp.concatenate(halves, axis=1)


    return jax.shard_map(on_device, **specs)
```

```python
import jax
import jax.numpy as jnp
from jax import lax
from jax.experimental import pallas as pl
from jax.experimental.pallas import tpu as pltpu
from jax.sharding import PartitionSpec as P


HEAD = 128
SUB = 64
EPS = 1e-06
HI = lax.Precision.HIGHEST
AXES = ("sp", "tp")
F32 = jnp.float32
BF16 = jnp.bfloat16


HEAD_K = 128
HEAD_V = 128
BLOCK = 64


def exact_parts(x):
    first = x.astype(BF16)
    rest = x - first.astype(F32)
    second = rest.astype(BF16)
    third = (rest - second.astype(F32)).astype(BF16)
    return first, second, third


def pack_logs(totals):
    lines = []
    for x in totals:
        lines += list(exact_parts(x))
    pad = 16 - len(lines)
    return jnp.concatenate(
        [x.astype(F32) for x in lines] + [jnp.zeros((pad, HEAD), F32)], axis=0
    ).astype(BF16)


def log_of(packed, heads, h):
    parts = packed[heads * HEAD :, :].astype(F32)
    return sum(parts[3 * h + k : 3 * h + k + 1, :] for k in range(3))


def as_column(row):
    return jnp.transpose(jnp.broadcast_to(row, (HEAD, HEAD)))


def gates_body(values, gates, logs, cum_out, packed):
    rows, width = gates.shape
    heads = width // HEAD
    gate, log_forget = gates[...], logs[...]
    r = lax.broadcasted_iota(jnp.int32, (rows, rows), 0)
    c = lax.broadcasted_iota(jnp.int32, (rows, rows), 1)
    lower = (r >= c).astype(F32)
    cum = jnp.dot(lower, log_forget, precision=HI, preferred_element_type=F32)
    cum_out[...] = cum
    total = cum[rows - 1 : rows, :]
    keys = gate * jnp.exp(total - cum)
    vals = values[...].astype(F32)
    for h in range(heads):
        ks = keys[:, h * HEAD : (h + 1) * HEAD]
        vs = vals[:, h * HEAD : (h + 1) * HEAD]
        state = lax.dot_general(
            ks, vs, (((0,), (0,)), ((), ())), precision=HI, preferred_element_type=F32
        )
        packed[h * HEAD : (h + 1) * HEAD, :] = state.astype(BF16)
    packed[heads * HEAD :, :] = pack_logs([total[:, h * HEAD : (h + 1) * HEAD] for h in range(heads)])


def local_body(query, gate, cum, values, out):
    rows, width = query.shape
    sub = min(SUB, rows)
    for h in range(width // HEAD):
        lanes = slice(h * HEAD, (h + 1) * HEAD)
        for i in range(rows // sub):
            lo, hi = i * sub, (i + 1) * sub
            mid = cum[lo + sub // 2 - 1 : lo + sub // 2, lanes]
            qs = query[lo:hi, lanes].astype(F32) * (HEAD**-0.5) * jnp.exp(cum[lo:hi, lanes] - mid)
            ks = gate[0:hi, lanes] * jnp.exp(mid - cum[0:hi, lanes])
            scores = lax.dot_general(
                qs, ks, (((1,), (1,)), ((), ())), precision=HI, preferred_element_type=F32
            )
            rr = lax.broadcasted_iota(jnp.int32, (sub, hi), 0) + lo
            cc = lax.broadcasted_iota(jnp.int32, (sub, hi), 1)
            scores = jnp.where(rr >= cc, scores, 0.0)
            out[lo:hi, lanes] = jnp.dot(
                scores, values[0:hi, lanes].astype(F32), precision=HI, preferred_element_type=F32
            )


def kernel_call(body, out_shape, scratch=(), smem=0, n_in=0, mib=16):
    specs = [pl.BlockSpec(memory_space=pltpu.SMEM)] * smem
    specs += [pl.BlockSpec(memory_space=pltpu.VMEM)] * (n_in - smem)
    many = isinstance(out_shape, (list, tuple))
    out_spec = pl.BlockSpec(memory_space=pltpu.VMEM)
    return pl.pallas_call(
        body,
        out_shape=out_shape,
        in_specs=specs,
        out_specs=[out_spec] * len(out_shape) if many else out_spec,
        scratch_shapes=list(scratch),
        compiler_params=pltpu.CompilerParams(vmem_limit_bytes=mib * 1024 * 1024),
    )


def pair_body(place, mine, theirs, out):
    last = place[1] == 1
    heads = (mine.shape[0] - 16) // HEAD
    logs = []
    for h in range(heads):
        rows = slice(h * HEAD, (h + 1) * HEAD)
        own_log, their_log = log_of(mine, heads, h), log_of(theirs, heads, h)
        own_state, their_state = mine[rows, :].astype(F32), theirs[rows, :].astype(F32)
        decay = as_column(jnp.exp(jnp.where(last, own_log, their_log)))
        early = jnp.where(last, their_state, own_state)
        late = jnp.where(last, own_state, their_state)
        out[rows, :] = (decay * early + late).astype(BF16)
        logs.append(own_log + their_log)
    out[heads * HEAD :, :] = pack_logs(logs)


def mix_body(n_cores, *refs):
    place = refs[0]
    query, cum, local, gate_logits, gain, weight, beside = refs[1:8]
    states = refs[8:-4]
    first, second, away, mixed = refs[-4:]
    rows, width = query.shape
    heads = width // HEAD
    last = place[1] == 1
    for h in range(heads):
        lanes = slice(h * HEAD, (h + 1) * HEAD)
        arrived = jnp.where(last, beside[lanes, :].astype(F32), 0.0)
        passed = jnp.where(last, log_of(beside, heads, h), 0.0)
        for s in states:
            arrived = arrived + as_column(jnp.exp(passed)) * s[lanes, :].astype(F32)
            passed = passed + log_of(s, heads, h)
        reach = query[:, lanes].astype(F32) * (HEAD**-0.5) * jnp.exp(cum[:, lanes])
        rec = local[:, lanes] + jnp.dot(reach, arrived, precision=HI, preferred_element_type=F32)
        scale = lax.rsqrt(jnp.mean(rec * rec, axis=-1, keepdims=True) + EPS)
        v = gate_logits[:, lanes].astype(F32)
        mixed[:, lanes] = rec * scale * gain[...] * (v / (1.0 + jnp.exp(-v)))
    y, c = place[2], place[3]
    n_y = 2
    own = rows // (n_y * n_cores)
    picked = []
    for e in range(n_cores):
        for k in range(n_y):
            t = lax.rem(y + k, n_y) * n_cores + lax.rem(c + e, n_cores)
            picked.append(mixed[pl.ds(pl.multiple_of(t * own, own), own), :])
    ordered = jnp.concatenate(picked, axis=0).astype(BF16)
    part = jnp.dot(ordered, weight[...], preferred_element_type=F32)
    first[...] = part[:own]
    second[...] = part[own : n_y * own]
    away[...] = part[n_y * own :].astype(BF16)


def norm_body(own, beside, arrived, residual, gain, stream_out, normed_out):
    rows = own.shape[0]
    stream = own[...] + beside[:rows, :].astype(F32) + arrived[...].astype(F32)
    stream = stream + residual[...].astype(F32)
    stream_out[...] = stream
    scale = lax.rsqrt(jnp.mean(stream * stream, axis=-1, keepdims=True) + EPS)
    normed = (stream * scale * gain[...]).astype(BF16)
    blocks, _, cols = normed_out.shape
    for i in range(blocks):
        normed_out[i] = normed[:, i * cols : (i + 1) * cols]


def hidden_half(rows_x, ups, up_all, cols, out):
    at = 0
    for src, off in ups:
        up_all[at : at + cols, :] = src[off : off + cols, :]
        at += cols
    act = jnp.maximum(jnp.dot(rows_x[...], up_all[...], preferred_element_type=F32), 0.0)
    out[...] = (act * act).astype(BF16)


def first_body(n_a, n_cores, place, toks, ups, rows_x, hidden, up_all):
    a, b = place[0], place[1]
    n_b = len(ups) // n_a
    _, own, cols = toks[0].shape
    for i in range(n_a * n_cores):
        for x in range(n_b):
            for e in range(n_a):
                k = lax.rem(a - e + n_a, n_a) * n_b + lax.rem(b + x, n_b)
                at = (x * n_a + e) * cols
                rows_x[i * own : (i + 1) * own, at : at + cols] = toks[i][k]
    hidden_half(rows_x, ups, up_all, cols, hidden)


def down_product(keep, away, units, pieces, down_all):
    at = 0
    for group in pieces:
        for piece in group:
            src, off = piece
            n = src.shape[0]
            down_all[at : at + n, :] = src[:, off : off + down_all.shape[1]]
            at += n
    acc = jnp.dot(units, down_all[...], preferred_element_type=F32)
    cut = keep.shape[0]
    keep[...] = acc[:cut]
    away[...] = acc[cut:].astype(BF16)


def lower_body(cols, place, rows_x, early, ups, pieces, keep, away, ordered, up_all, late, down_all):
    hidden_half(rows_x, ups, up_all, cols, late)
    n_b = 2
    b = place[1]
    half = late.shape[1] // n_b
    for y, src in enumerate((early, late)):
        for x in range(n_b):
            k = lax.rem(b + x, n_b)
            at = (y * n_b + x) * half
            ordered[:, at : at + half] = src[:, pl.ds(pl.multiple_of(k * half, half), half)]
    down_product(keep, away, ordered[...], pieces, down_all)


def fold_body(keep, got, near, held):
    rows = near.shape[0] // 2
    for k in range(2):
        for out, block in ((held, 2 * k), (near, 2 * k + 1)):
            src = slice(block * rows, (block + 1) * rows)
            both = keep[src, :] + got[src, :].astype(F32)
            out[k * rows : (k + 1) * rows, :] = both.astype(out.dtype)


norm_eps = 1e-06
highest_precision = lax.Precision.HIGHEST


def carried_in(part, axis, combine, identity):
    place = lax.axis_index(axis)
    gathered = jax.tree.map(lambda a: lax.all_gather(a, axis), part)
    state = jax.tree.map(lambda a, e: jnp.zeros_like(a) + jnp.asarray(e, a.dtype), part, identity)

    def one(step, state):
        return combine(
            state, jax.tree.map(lambda a: lax.dynamic_index_in_dim(a, step, 0, False), gathered)
        )

    return lax.fori_loop(0, place, one, state)


def block_update(carry_forward_state, block_inputs):
    query_rows_block, gate_rows_block, value_rows_block, log_block = block_inputs
    cumulative_log = jnp.cumsum(log_block, axis=1)
    length = query_rows_block.shape[1]
    causal = jnp.arange(length)[:, None] >= jnp.arange(length)[None, :]
    across_blocks = jnp.einsum(
        "dcj,djw->dcw",
        query_rows_block * jnp.exp(cumulative_log),
        carry_forward_state,
        precision=highest_precision,
    )
    spread = cumulative_log[:, :, None, :] - cumulative_log[:, None, :, :]
    decay_table = jnp.exp(jnp.where(causal[None, :, :, None], spread, -jnp.inf))
    scores = jnp.einsum(
        "htk,hsk,htsk->hts",
        query_rows_block,
        gate_rows_block,
        decay_table,
        precision=highest_precision,
    )
    within = jnp.einsum("hts,hsv->htv", scores, value_rows_block, precision=highest_precision)
    final_log_total = cumulative_log[:, -1:, :]
    updated_state = jnp.exp(final_log_total[:, 0, :])[
        :, :, None
    ] * carry_forward_state + jnp.einsum(
        "tri,trw->tiw",
        gate_rows_block * jnp.exp(final_log_total - cumulative_log),
        value_rows_block,
        precision=highest_precision,
    )
    return (updated_state, across_blocks + within)


def to_blocks(array, inner):
    length = array.shape[0]
    split_up = array.reshape(length // BLOCK, BLOCK, array.shape[1] // inner, inner)
    return jnp.transpose(split_up, (0, 2, 1, 3))


def from_blocks(blocked):
    joined = jnp.transpose(blocked, (0, 2, 1, 3))
    return joined.reshape(joined.shape[0] * joined.shape[1], joined.shape[2], joined.shape[3])


def prepare_inputs(query, forget_logits, written_values, forget_floor_gap, extra_log_decay):
    input_gate_value = forget_floor_gap[None, :] * jax.nn.sigmoid(
        -forget_logits.astype(jnp.float32)
    )
    forget_log_rate = jnp.log1p(-input_gate_value) + extra_log_decay
    scaled_values = query.astype(jnp.float32) * HEAD_K ** (-0.5)
    return (scaled_values, input_gate_value, written_values.astype(jnp.float32), forget_log_rate)


def gate_out(recurrent, output_gate_logits, head_norm_gain):
    normal_part = recurrent * lax.rsqrt(
        jnp.mean(recurrent * recurrent, axis=-1, keepdims=True) + norm_eps
    )
    gating = jax.nn.silu(output_gate_logits.astype(jnp.float32)).reshape(recurrent.shape)
    mixed = normal_part * head_norm_gain * gating
    return mixed.reshape(recurrent.shape[0], -1).astype(jnp.bfloat16)


def normalize(stream, gain):
    scaled_rows = stream * lax.rsqrt(jnp.mean(stream * stream, axis=-1, keepdims=True) + norm_eps)
    return (scaled_rows * gain).astype(jnp.bfloat16)


def chain_states(earlier, later):
    return (earlier[0] + later[0], jnp.exp(later[0])[:, :, None] * earlier[1] + later[1])


def gathered_plan(
    query,
    forget_logits,
    written_values,
    output_gate_logits,
    forget_floor_gap,
    extra_log_decay,
    head_norm_gain,
    output_weight,
    residual,
    mixer_norm_gain,
    mixer_up_weight,
    mixer_down_weight,
):
    scaled_values, input_gate_value, value_rows, forget_log_rate = prepare_inputs(
        query, forget_logits, written_values, forget_floor_gap, extra_log_decay
    )
    row_count, local_width = query.shape
    head_count = local_width // HEAD_K
    start_state = jnp.zeros((head_count, HEAD_K, HEAD_V), jnp.float32)
    local_state, blocked = lax.scan(
        block_update,
        start_state,
        (
            to_blocks(scaled_values, HEAD_K),
            to_blocks(input_gate_value, HEAD_K),
            to_blocks(value_rows, HEAD_V),
            to_blocks(forget_log_rate, HEAD_K),
        ),
    )
    log_total = jnp.sum(forget_log_rate, axis=0).reshape(head_count, HEAD_K)
    arrived_state = carried_in(
        (log_total, local_state),
        "sp",
        chain_states,
        (jnp.zeros_like(log_total), jnp.zeros_like(local_state)),
    )
    running = jnp.cumsum(forget_log_rate, axis=0)
    reached_state = (scaled_values * jnp.exp(running)).reshape(row_count, head_count, HEAD_K)
    carried_over = jnp.einsum(
        "cja,jae->cje", reached_state, arrived_state[1], precision=highest_precision
    )
    mixed = gate_out(from_blocks(blocked) + carried_over, output_gate_logits, head_norm_gain)
    stream_own = lax.psum_scatter(
        jnp.dot(mixed, output_weight, preferred_element_type=jnp.float32).astype(jnp.bfloat16),
        "tp",
        scatter_dimension=0,
        tiled=True,
    ).astype(jnp.float32) + residual.astype(jnp.float32)
    normed = lax.all_gather(normalize(stream_own, mixer_norm_gain), "tp", axis=0, tiled=True)
    columns = normed
    lifted = jnp.dot(
        columns,
        lax.all_gather(mixer_up_weight, "sp", axis=0, tiled=True),
        preferred_element_type=jnp.float32,
    )
    hidden = jnp.square(jax.nn.relu(lifted)).astype(jnp.bfloat16)
    columns = hidden
    projected = jnp.dot(
        columns,
        lax.all_gather(mixer_down_weight, "sp", axis=0, tiled=True),
        preferred_element_type=jnp.float32,
    )
    mlp_own = lax.psum_scatter(
        projected.astype(jnp.bfloat16), "tp", scatter_dimension=0, tiled=True
    ).astype(jnp.float32)
    return (stream_own + mlp_own).astype(jnp.bfloat16)


def solution(mesh):
    specs = dict(
        mesh=mesh,
        in_specs=(
            P("sp", "tp"),
            P("sp", "tp"),
            P("sp", "tp"),
            P("sp", "tp"),
            P("tp"),
            P("sp", "tp"),
            P(),
            P("tp", None),
            P(("sp", "tp"), None),
            P(),
            P("sp", "tp"),
            P(("tp", "sp"), None),
        ),
        out_specs=P(("sp", "tp"), None),
        check_vma=False,
    )
    n_sp, n_tp = mesh.shape["sp"], mesh.shape["tp"]
    n_b, n_y = 2, 2
    n_a, n_c = n_sp // n_b, n_tp // n_y
    if n_sp % n_b or n_tp % n_y or n_a != 4 or n_c != 2:
        return jax.shard_map(gathered_plan, **specs)

    def flat(a, b, y, c):
        return (a % n_a * n_b + b % n_b) * n_tp + y % n_y * n_c + c % n_c

    def send(x, a=0, b=0, y=0, c=0, flip=0, cyclic=True):
        pairs = [
            (flat(i, j, k, m), flat((i ^ flip) + a, j + b, k + y, m + c))
            for i in range(n_a)
            for j in range(n_b)
            for k in range(n_y)
            for m in range(n_c)
            if cyclic or i + a < n_a
        ]
        return lax.ppermute(x, AXES, pairs)

    def on_device(
        query,
        forget_logits,
        written_values,
        output_gate_logits,
        forget_floor_gap,
        extra_log_decay,
        head_norm_gain,
        output_weight,
        residual,
        mixer_norm_gain,
        mixer_up_weight,
        mixer_down_weight,
    ):
        sp, tp = lax.axis_index("sp"), lax.axis_index("tp")
        a, b, y, c = sp // n_b, sp % n_b, tp // n_c, tp % n_c
        place = jnp.stack([a, b, y, c]).astype(jnp.int32)
        rows, width = query.shape
        model = output_weight.shape[1]
        own = residual.shape[0]
        heads = width // HEAD

        packed_shape = jax.ShapeDtypeStruct((heads * HEAD + 16, HEAD), BF16)
        gate = forget_floor_gap[None, :] * jax.nn.sigmoid(-forget_logits.astype(F32))
        log_forget = jnp.log1p(-gate) + extra_log_decay
        cum, packed = kernel_call(
            gates_body, [jax.ShapeDtypeStruct((rows, width), F32), packed_shape], n_in=3
        )(written_values, gate, log_forget)

        up_rows, up_cols = mixer_up_weight.shape
        piece = up_cols // n_a
        mine = []
        for d in range(n_a):
            cut = lax.dynamic_slice(mixer_up_weight, (0, (a + d) % n_a * piece), (up_rows, piece))
            mine.append(cut if d == 0 else send(cut, a=d))

        def grouped(refs):
            return [(refs[0], 0), (refs[2], 0), (refs[1], 0), (refs[2], up_rows)]

        part = model // 2
        half = mixer_down_weight.shape[0] // 2
        down_x = send(mixer_down_weight, b=1)
        down_y = send(mixer_down_weight, y=1)
        down_xy = []
        for k in range(2):
            lanes = slice(k * part, (k + 1) * part)
            cut = half if k else half // 2
            down_xy.append([send(down_x[:cut, lanes], y=1), send(down_y[cut:, lanes], b=1)])
        whole = [mixer_down_weight, down_x, down_y]

        beside = send(packed, b=1)
        pair = kernel_call(pair_body, packed_shape, smem=1, n_in=3)(place, packed, beside)
        states = [send(pair, a=d, cyclic=False) for d in range(1, n_a)]
        local = kernel_call(
            local_body, jax.ShapeDtypeStruct((rows, width), F32), n_in=4
        )(query, gate, cum, written_values)
        first, second, away = kernel_call(
            lambda *refs: mix_body(n_c, *refs),
            [
                jax.ShapeDtypeStruct((own, model), F32),
                jax.ShapeDtypeStruct((own, model), F32),
                jax.ShapeDtypeStruct((n_y * own, model), BF16),
            ],
            scratch=[pltpu.VMEM((rows, width), F32)],
            smem=1,
            n_in=8 + len(states),
        )(
            place,
            query,
            cum,
            local,
            output_gate_logits,
            head_norm_gain[None, :],
            output_weight,
            beside,
            *states,
        )
        got = send(away, c=1)
        second = (second + got[own:].astype(F32)).astype(BF16)
        other = send(second, y=1)
        late = lax.optimization_barrier((mine[1], mine[3], second))[:2]
        up_x, up_y = [], []
        for members in [mine[0], mine[2], jnp.concatenate(late, axis=0)]:
            up_x.append(send(members, b=1))
            up_y.append(send(members, y=1))
        up_xy = [send(up_x[0], y=1), send(up_x[1], y=1), send(up_y[2], b=1)]
        stream, normed = kernel_call(
            norm_body,
            [
                jax.ShapeDtypeStruct((own, model), F32),
                jax.ShapeDtypeStruct((n_sp, own, model // n_sp), BF16),
            ],
            n_in=5,
        )(first, got, other, residual, mixer_norm_gain[None, :])

        line = [normed] + [send(normed, flip=d) for d in range(1, n_a)]
        toks = line + [send(u, c=1) for u in line]
        group = n_a * own
        tokens = n_c * group
        units = n_y * piece
        cols = model // n_sp
        sizes = [
            jax.ShapeDtypeStruct((group, part), F32),
            jax.ShapeDtypeStruct((tokens - group, part), BF16),
        ]

        def first_half(*refs):
            t = 1 + len(toks)
            ups = [(refs[t + e], 0) for e in range(n_a)] + grouped(refs[t + n_a : t + n_a + 3])
            first_body(n_a, n_c, refs[0], refs[1:t], ups, *refs[-3:])

        rows_x, early = kernel_call(
            first_half,
            [
                jax.ShapeDtypeStruct((tokens, model), BF16),
                jax.ShapeDtypeStruct((tokens, piece), BF16),
            ],
            scratch=[pltpu.VMEM((model, piece), BF16)],
            smem=1,
            n_in=1 + len(toks) + n_a + 3,
            mib=24,
        )(place, *toks, *mine, *up_x)

        def second_half(*refs):
            ups = grouped(refs[3:6]) + grouped(refs[6:9])
            pieces = [[(r, 0)] for r in refs[9:12]] + [[(refs[12], 0), (refs[13], 0)]]
            lower_body(cols, *refs[:3], ups, pieces, *refs[14:])

        keep0, away0, hidden = kernel_call(
            second_half,
            sizes + [jax.ShapeDtypeStruct((tokens, units), BF16)],
            scratch=[
                pltpu.VMEM((model, piece), BF16),
                pltpu.VMEM((tokens, piece), BF16),
                pltpu.VMEM((units, part), BF16),
            ],
            smem=1,
            n_in=14,
            mib=30,
        )(place, rows_x, early, *up_y, *up_xy, *whole, *down_xy[0])
        got0 = send(away0, c=1)

        def last_columns(hidden_ref, own_ref, x_ref, y_ref, r0_ref, r1_ref, keep, away, down_all):
            pieces = [[(r, part)] for r in (own_ref, x_ref, y_ref)]
            pieces.append([(r0_ref, 0), (r1_ref, 0)])
            down_product(keep, away, hidden_ref[...], pieces, down_all)

        keep1, away1 = kernel_call(
            last_columns, sizes, scratch=[pltpu.VMEM((units, part), BF16)], n_in=6
        )(hidden, *whole, *down_xy[1])
        got1 = send(away1, c=1)
        halves = []
        for k, (keep, got) in enumerate([(keep0, got0), (keep1, got1)]):
            near, held = kernel_call(
                fold_body,
                [
                    jax.ShapeDtypeStruct((n_b * own, part), BF16),
                    jax.ShapeDtypeStruct((n_b * own, part), F32),
                ],
                n_in=2,
            )(keep, got)
            near = send(near, flip=1)
            far = (held[own:] + near[own:].astype(F32)).astype(BF16)
            far = send(far, flip=2)
            total = stream[:, k * part : (k + 1) * part] + held[:own] + near[:own].astype(F32)
            total = total + far.astype(F32)
            halves.append(total.astype(BF16))
        return jnp.concatenate(halves, axis=1)


    return jax.shard_map(on_device, **specs)
```

```python
import jax
import jax.numpy as jnp
from jax import lax
from jax.experimental import pallas as pl
from jax.experimental.pallas import tpu as pltpu
from jax.sharding import PartitionSpec as P


HEAD = 128
SUB = 64
EPS = 1e-06
HI = lax.Precision.HIGHEST
AXES = ("sp", "tp")
F32 = jnp.float32
BF16 = jnp.bfloat16


HEAD_K = 128
HEAD_V = 128
BLOCK = 64


def exact_parts(x):
    first = x.astype(BF16)
    rest = x - first.astype(F32)
    second = rest.astype(BF16)
    third = (rest - second.astype(F32)).astype(BF16)
    return first, second, third


def pack_logs(totals):
    lines = []
    for x in totals:
        lines += list(exact_parts(x))
    pad = 16 - len(lines)
    return jnp.concatenate(
        [x.astype(F32) for x in lines] + [jnp.zeros((pad, HEAD), F32)], axis=0
    ).astype(BF16)


def log_of(packed, heads, h):
    parts = packed[heads * HEAD :, :].astype(F32)
    return sum(parts[3 * h + k : 3 * h + k + 1, :] for k in range(3))


def as_column(row):
    return jnp.transpose(jnp.broadcast_to(row, (HEAD, HEAD)))


def gates_body(values, gates, logs, cum_out, packed):
    rows, width = gates.shape
    heads = width // HEAD
    gate, log_forget = gates[...], logs[...]
    r = lax.broadcasted_iota(jnp.int32, (rows, rows), 0)
    c = lax.broadcasted_iota(jnp.int32, (rows, rows), 1)
    lower = (r >= c).astype(F32)
    cum = jnp.dot(lower, log_forget, precision=HI, preferred_element_type=F32)
    cum_out[...] = cum
    total = cum[rows - 1 : rows, :]
    keys = gate * jnp.exp(total - cum)
    vals = values[...].astype(F32)
    for h in range(heads):
        ks = keys[:, h * HEAD : (h + 1) * HEAD]
        vs = vals[:, h * HEAD : (h + 1) * HEAD]
        state = lax.dot_general(
            ks, vs, (((0,), (0,)), ((), ())), precision=HI, preferred_element_type=F32
        )
        packed[h * HEAD : (h + 1) * HEAD, :] = state.astype(BF16)
    packed[heads * HEAD :, :] = pack_logs([total[:, h * HEAD : (h + 1) * HEAD] for h in range(heads)])


def local_body(query, gate, cum, values, out):
    rows, width = query.shape
    sub = min(SUB, rows)
    for h in range(width // HEAD):
        lanes = slice(h * HEAD, (h + 1) * HEAD)
        for i in range(rows // sub):
            lo, hi = i * sub, (i + 1) * sub
            mid = cum[lo + sub // 2 - 1 : lo + sub // 2, lanes]
            qs = query[lo:hi, lanes].astype(F32) * (HEAD**-0.5) * jnp.exp(cum[lo:hi, lanes] - mid)
            ks = gate[0:hi, lanes] * jnp.exp(mid - cum[0:hi, lanes])
            scores = lax.dot_general(
                qs, ks, (((1,), (1,)), ((), ())), precision=HI, preferred_element_type=F32
            )
            rr = lax.broadcasted_iota(jnp.int32, (sub, hi), 0) + lo
            cc = lax.broadcasted_iota(jnp.int32, (sub, hi), 1)
            scores = jnp.where(rr >= cc, scores, 0.0)
            out[lo:hi, lanes] = jnp.dot(
                scores, values[0:hi, lanes].astype(F32), precision=HI, preferred_element_type=F32
            )


def kernel_call(body, out_shape, scratch=(), smem=0, n_in=0, mib=16):
    specs = [pl.BlockSpec(memory_space=pltpu.SMEM)] * smem
    specs += [pl.BlockSpec(memory_space=pltpu.VMEM)] * (n_in - smem)
    many = isinstance(out_shape, (list, tuple))
    out_spec = pl.BlockSpec(memory_space=pltpu.VMEM)
    return pl.pallas_call(
        body,
        out_shape=out_shape,
        in_specs=specs,
        out_specs=[out_spec] * len(out_shape) if many else out_spec,
        scratch_shapes=list(scratch),
        compiler_params=pltpu.CompilerParams(vmem_limit_bytes=mib * 1024 * 1024),
    )


def pair_body(place, mine, theirs, out):
    last = place[1] == 1
    heads = (mine.shape[0] - 16) // HEAD
    logs = []
    for h in range(heads):
        rows = slice(h * HEAD, (h + 1) * HEAD)
        own_log, their_log = log_of(mine, heads, h), log_of(theirs, heads, h)
        own_state, their_state = mine[rows, :].astype(F32), theirs[rows, :].astype(F32)
        decay = as_column(jnp.exp(jnp.where(last, own_log, their_log)))
        early = jnp.where(last, their_state, own_state)
        late = jnp.where(last, own_state, their_state)
        out[rows, :] = (decay * early + late).astype(BF16)
        logs.append(own_log + their_log)
    out[heads * HEAD :, :] = pack_logs(logs)


def mix_body(n_cores, *refs):
    place = refs[0]
    query, cum, local, gate_logits, gain, weight, beside = refs[1:8]
    states = refs[8:-4]
    first, second, away, mixed = refs[-4:]
    rows, width = query.shape
    heads = width // HEAD
    last = place[1] == 1
    for h in range(heads):
        lanes = slice(h * HEAD, (h + 1) * HEAD)
        arrived = jnp.where(last, beside[lanes, :].astype(F32), 0.0)
        passed = jnp.where(last, log_of(beside, heads, h), 0.0)
        for s in states:
            arrived = arrived + as_column(jnp.exp(passed)) * s[lanes, :].astype(F32)
            passed = passed + log_of(s, heads, h)
        reach = query[:, lanes].astype(F32) * (HEAD**-0.5) * jnp.exp(cum[:, lanes])
        rec = local[:, lanes] + jnp.dot(reach, arrived, precision=HI, preferred_element_type=F32)
        scale = lax.rsqrt(jnp.mean(rec * rec, axis=-1, keepdims=True) + EPS)
        v = gate_logits[:, lanes].astype(F32)
        mixed[:, lanes] = rec * scale * gain[...] * (v / (1.0 + jnp.exp(-v)))
    y, c = place[2], place[3]
    n_y = 2
    own = rows // (n_y * n_cores)
    picked = []
    for e in range(n_cores):
        for k in range(n_y):
            t = lax.rem(y + k, n_y) * n_cores + lax.rem(c + e, n_cores)
            picked.append(mixed[pl.ds(pl.multiple_of(t * own, own), own), :])
    ordered = jnp.concatenate(picked, axis=0).astype(BF16)
    part = jnp.dot(ordered, weight[...], preferred_element_type=F32)
    first[...] = part[:own]
    second[...] = part[own : n_y * own]
    away[...] = part[n_y * own :].astype(BF16)


def norm_body(own, beside, arrived, residual, gain, stream_out, normed_out):
    rows = own.shape[0]
    stream = own[...] + beside[:rows, :].astype(F32) + arrived[...].astype(F32)
    stream = stream + residual[...].astype(F32)
    stream_out[...] = stream
    scale = lax.rsqrt(jnp.mean(stream * stream, axis=-1, keepdims=True) + EPS)
    normed = (stream * scale * gain[...]).astype(BF16)
    blocks, _, cols = normed_out.shape
    for i in range(blocks):
        normed_out[i] = normed[:, i * cols : (i + 1) * cols]


def hidden_half(rows_x, ups, up_all, cols, out):
    at = 0
    for src, off in ups:
        up_all[at : at + cols, :] = src[off : off + cols, :]
        at += cols
    act = jnp.maximum(jnp.dot(rows_x[...], up_all[...], preferred_element_type=F32), 0.0)
    out[...] = (act * act).astype(BF16)


def first_body(n_a, n_cores, place, toks, ups, rows_x, hidden, up_all):
    a, b = place[0], place[1]
    n_b = len(ups) // n_a
    _, own, cols = toks[0].shape
    for i in range(n_a * n_cores):
        for x in range(n_b):
            for e in range(n_a):
                k = lax.rem(a - e + n_a, n_a) * n_b + lax.rem(b + x, n_b)
                at = (x * n_a + e) * cols
                rows_x[i * own : (i + 1) * own, at : at + cols] = toks[i][k]
    hidden_half(rows_x, ups, up_all, cols, hidden)


def down_product(keep, away, units, pieces, down_all):
    at = 0
    for group in pieces:
        for piece in group:
            src, off = piece
            n = src.shape[0]
            down_all[at : at + n, :] = src[:, off : off + down_all.shape[1]]
            at += n
    acc = jnp.dot(units, down_all[...], preferred_element_type=F32)
    cut = keep.shape[0]
    keep[...] = acc[:cut]
    away[...] = acc[cut:].astype(BF16)


def lower_body(cols, place, rows_x, early, ups, pieces, keep, away, ordered, up_all, late, down_all):
    hidden_half(rows_x, ups, up_all, cols, late)
    n_b = 2
    b = place[1]
    half = late.shape[1] // n_b
    for y, src in enumerate((early, late)):
        for x in range(n_b):
            k = lax.rem(b + x, n_b)
            at = (y * n_b + x) * half
            ordered[:, at : at + half] = src[:, pl.ds(pl.multiple_of(k * half, half), half)]
    down_product(keep, away, ordered[...], pieces, down_all)


def fold_body(keep, got, near, held):
    rows = near.shape[0] // 2
    for k in range(2):
        for out, block in ((held, 2 * k), (near, 2 * k + 1)):
            src = slice(block * rows, (block + 1) * rows)
            both = keep[src, :] + got[src, :].astype(F32)
            out[k * rows : (k + 1) * rows, :] = both.astype(out.dtype)


norm_eps = 1e-06
highest_precision = lax.Precision.HIGHEST


def carried_in(part, axis, combine, identity):
    place = lax.axis_index(axis)
    gathered = jax.tree.map(lambda a: lax.all_gather(a, axis), part)
    state = jax.tree.map(lambda a, e: jnp.zeros_like(a) + jnp.asarray(e, a.dtype), part, identity)

    def one(step, state):
        return combine(
            state, jax.tree.map(lambda a: lax.dynamic_index_in_dim(a, step, 0, False), gathered)
        )

    return lax.fori_loop(0, place, one, state)


def block_update(carry_forward_state, block_inputs):
    query_rows_block, gate_rows_block, value_rows_block, log_block = block_inputs
    cumulative_log = jnp.cumsum(log_block, axis=1)
    length = query_rows_block.shape[1]
    causal = jnp.arange(length)[:, None] >= jnp.arange(length)[None, :]
    across_blocks = jnp.einsum(
        "dcj,djw->dcw",
        query_rows_block * jnp.exp(cumulative_log),
        carry_forward_state,
        precision=highest_precision,
    )
    spread = cumulative_log[:, :, None, :] - cumulative_log[:, None, :, :]
    decay_table = jnp.exp(jnp.where(causal[None, :, :, None], spread, -jnp.inf))
    scores = jnp.einsum(
        "htk,hsk,htsk->hts",
        query_rows_block,
        gate_rows_block,
        decay_table,
        precision=highest_precision,
    )
    within = jnp.einsum("hts,hsv->htv", scores, value_rows_block, precision=highest_precision)
    final_log_total = cumulative_log[:, -1:, :]
    updated_state = jnp.exp(final_log_total[:, 0, :])[
        :, :, None
    ] * carry_forward_state + jnp.einsum(
        "tri,trw->tiw",
        gate_rows_block * jnp.exp(final_log_total - cumulative_log),
        value_rows_block,
        precision=highest_precision,
    )
    return (updated_state, across_blocks + within)


def to_blocks(array, inner):
    length = array.shape[0]
    split_up = array.reshape(length // BLOCK, BLOCK, array.shape[1] // inner, inner)
    return jnp.transpose(split_up, (0, 2, 1, 3))


def from_blocks(blocked):
    joined = jnp.transpose(blocked, (0, 2, 1, 3))
    return joined.reshape(joined.shape[0] * joined.shape[1], joined.shape[2], joined.shape[3])


def prepare_inputs(query, forget_logits, written_values, forget_floor_gap, extra_log_decay):
    input_gate_value = forget_floor_gap[None, :] * jax.nn.sigmoid(
        -forget_logits.astype(jnp.float32)
    )
    forget_log_rate = jnp.log1p(-input_gate_value) + extra_log_decay
    scaled_values = query.astype(jnp.float32) * HEAD_K ** (-0.5)
    return (scaled_values, input_gate_value, written_values.astype(jnp.float32), forget_log_rate)


def gate_out(recurrent, output_gate_logits, head_norm_gain):
    normal_part = recurrent * lax.rsqrt(
        jnp.mean(recurrent * recurrent, axis=-1, keepdims=True) + norm_eps
    )
    gating = jax.nn.silu(output_gate_logits.astype(jnp.float32)).reshape(recurrent.shape)
    mixed = normal_part * head_norm_gain * gating
    return mixed.reshape(recurrent.shape[0], -1).astype(jnp.bfloat16)


def normalize(stream, gain):
    scaled_rows = stream * lax.rsqrt(jnp.mean(stream * stream, axis=-1, keepdims=True) + norm_eps)
    return (scaled_rows * gain).astype(jnp.bfloat16)


def chain_states(earlier, later):
    return (earlier[0] + later[0], jnp.exp(later[0])[:, :, None] * earlier[1] + later[1])


def gathered_plan(
    query,
    forget_logits,
    written_values,
    output_gate_logits,
    forget_floor_gap,
    extra_log_decay,
    head_norm_gain,
    output_weight,
    residual,
    mixer_norm_gain,
    mixer_up_weight,
    mixer_down_weight,
):
    scaled_values, input_gate_value, value_rows, forget_log_rate = prepare_inputs(
        query, forget_logits, written_values, forget_floor_gap, extra_log_decay
    )
    row_count, local_width = query.shape
    head_count = local_width // HEAD_K
    start_state = jnp.zeros((head_count, HEAD_K, HEAD_V), jnp.float32)
    local_state, blocked = lax.scan(
        block_update,
        start_state,
        (
            to_blocks(scaled_values, HEAD_K),
            to_blocks(input_gate_value, HEAD_K),
            to_blocks(value_rows, HEAD_V),
            to_blocks(forget_log_rate, HEAD_K),
        ),
    )
    log_total = jnp.sum(forget_log_rate, axis=0).reshape(head_count, HEAD_K)
    arrived_state = carried_in(
        (log_total, local_state),
        "sp",
        chain_states,
        (jnp.zeros_like(log_total), jnp.zeros_like(local_state)),
    )
    running = jnp.cumsum(forget_log_rate, axis=0)
    reached_state = (scaled_values * jnp.exp(running)).reshape(row_count, head_count, HEAD_K)
    carried_over = jnp.einsum(
        "cja,jae->cje", reached_state, arrived_state[1], precision=highest_precision
    )
    mixed = gate_out(from_blocks(blocked) + carried_over, output_gate_logits, head_norm_gain)
    stream_own = lax.psum_scatter(
        jnp.dot(mixed, output_weight, preferred_element_type=jnp.float32).astype(jnp.bfloat16),
        "tp",
        scatter_dimension=0,
        tiled=True,
    ).astype(jnp.float32) + residual.astype(jnp.float32)
    normed = lax.all_gather(normalize(stream_own, mixer_norm_gain), "tp", axis=0, tiled=True)
    columns = normed
    lifted = jnp.dot(
        columns,
        lax.all_gather(mixer_up_weight, "sp", axis=0, tiled=True),
        preferred_element_type=jnp.float32,
    )
    hidden = jnp.square(jax.nn.relu(lifted)).astype(jnp.bfloat16)
    columns = hidden
    projected = jnp.dot(
        columns,
        lax.all_gather(mixer_down_weight, "sp", axis=0, tiled=True),
        preferred_element_type=jnp.float32,
    )
    mlp_own = lax.psum_scatter(
        projected.astype(jnp.bfloat16), "tp", scatter_dimension=0, tiled=True
    ).astype(jnp.float32)
    return (stream_own + mlp_own).astype(jnp.bfloat16)


def solution(mesh):
    specs = dict(
        mesh=mesh,
        in_specs=(
            P("sp", "tp"),
            P("sp", "tp"),
            P("sp", "tp"),
            P("sp", "tp"),
            P("tp"),
            P("sp", "tp"),
            P(),
            P("tp", None),
            P(("sp", "tp"), None),
            P(),
            P("sp", "tp"),
            P(("tp", "sp"), None),
        ),
        out_specs=P(("sp", "tp"), None),
        check_vma=False,
    )
    n_sp, n_tp = mesh.shape["sp"], mesh.shape["tp"]
    n_b, n_y = 2, 2
    n_a, n_c = n_sp // n_b, n_tp // n_y
    if n_sp % n_b or n_tp % n_y or n_a != 4 or n_c != 2:
        return jax.shard_map(gathered_plan, **specs)

    def flat(a, b, y, c):
        return (a % n_a * n_b + b % n_b) * n_tp + y % n_y * n_c + c % n_c

    def send(x, a=0, b=0, y=0, c=0, flip=0, cyclic=True):
        pairs = [
            (flat(i, j, k, m), flat((i ^ flip) + a, j + b, k + y, m + c))
            for i in range(n_a)
            for j in range(n_b)
            for k in range(n_y)
            for m in range(n_c)
            if cyclic or i + a < n_a
        ]
        return lax.ppermute(x, AXES, pairs)

    def on_device(
        query,
        forget_logits,
        written_values,
        output_gate_logits,
        forget_floor_gap,
        extra_log_decay,
        head_norm_gain,
        output_weight,
        residual,
        mixer_norm_gain,
        mixer_up_weight,
        mixer_down_weight,
    ):
        sp, tp = lax.axis_index("sp"), lax.axis_index("tp")
        a, b, y, c = sp // n_b, sp % n_b, tp // n_c, tp % n_c
        place = jnp.stack([a, b, y, c]).astype(jnp.int32)
        rows, width = query.shape
        model = output_weight.shape[1]
        own = residual.shape[0]
        heads = width // HEAD

        packed_shape = jax.ShapeDtypeStruct((heads * HEAD + 16, HEAD), BF16)
        gate = forget_floor_gap[None, :] * jax.nn.sigmoid(-forget_logits.astype(F32))
        log_forget = jnp.log1p(-gate) + extra_log_decay
        cum, packed = kernel_call(
            gates_body, [jax.ShapeDtypeStruct((rows, width), F32), packed_shape], n_in=3
        )(written_values, gate, log_forget)

        up_rows, up_cols = mixer_up_weight.shape
        piece = up_cols // n_a
        mine = []
        for d in range(n_a):
            start = (0, (a + d) % n_a * piece)
            cut = lax.dynamic_slice(mixer_up_weight, start, (up_rows, piece))
            mine.append(cut if d == 0 else send(cut, a=d))

        def grouped(refs):
            return [(refs[0], 0), (refs[2], 0), (refs[1], 0), (refs[2], up_rows)]

        part = model // 2
        half = mixer_down_weight.shape[0] // 2
        down_x = send(mixer_down_weight, b=1)
        down_y = send(mixer_down_weight, y=1)
        down_xy = []
        for k in range(2):
            lanes = slice(k * part, (k + 1) * part)
            cut = half if k else half // 2
            down_xy.append([send(down_x[:cut, lanes], y=1), send(down_y[cut:, lanes], b=1)])
        whole = [mixer_down_weight, down_x, down_y]

        beside = send(packed, b=1)
        pair = kernel_call(pair_body, packed_shape, smem=1, n_in=3)(place, packed, beside)
        states = [send(pair, a=d, cyclic=False) for d in range(1, n_a)]
        local = kernel_call(
            local_body, jax.ShapeDtypeStruct((rows, width), F32), n_in=4
        )(query, gate, cum, written_values)
        first, second, away = kernel_call(
            lambda *refs: mix_body(n_c, *refs),
            [
                jax.ShapeDtypeStruct((own, model), F32),
                jax.ShapeDtypeStruct((own, model), F32),
                jax.ShapeDtypeStruct((n_y * own, model), BF16),
            ],
            scratch=[pltpu.VMEM((rows, width), F32)],
            smem=1,
            n_in=8 + len(states),
        )(
            place,
            query,
            cum,
            local,
            output_gate_logits,
            head_norm_gain[None, :],
            output_weight,
            beside,
            *states,
        )
        got = send(away, c=1)
        second = (second + got[own:].astype(F32)).astype(BF16)
        other = send(second, y=1)
        stream, normed = kernel_call(
            norm_body,
            [
                jax.ShapeDtypeStruct((own, model), F32),
                jax.ShapeDtypeStruct((n_sp, own, model // n_sp), BF16),
            ],
            n_in=5,
        )(first, got, other, residual, mixer_norm_gain[None, :])

        late = lax.optimization_barrier((mine[1], mine[3], normed))[:2]
        up_x, up_y = [], []
        for members in [mine[0], mine[2], jnp.concatenate(late, axis=0)]:
            up_x.append(send(members, b=1))
            up_y.append(send(members, y=1))
        up_xy = [send(up_x[0], y=1), send(up_x[1], y=1), send(up_y[2], b=1)]

        line = [normed] + [send(normed, flip=d) for d in range(1, n_a)]
        toks = line + [send(u, c=1) for u in line]
        group = n_a * own
        tokens = n_c * group
        units = n_y * piece
        cols = model // n_sp
        sizes = [
            jax.ShapeDtypeStruct((group, part), F32),
            jax.ShapeDtypeStruct((tokens - group, part), BF16),
        ]

        def first_half(*refs):
            t = 1 + len(toks)
            ups = [(refs[t + e], 0) for e in range(n_a)] + grouped(refs[t + n_a : t + n_a + 3])
            first_body(n_a, n_c, refs[0], refs[1:t], ups, *refs[-3:])

        rows_x, early = kernel_call(
            first_half,
            [
                jax.ShapeDtypeStruct((tokens, model), BF16),
                jax.ShapeDtypeStruct((tokens, piece), BF16),
            ],
            scratch=[pltpu.VMEM((model, piece), BF16)],
            smem=1,
            n_in=1 + len(toks) + n_a + 3,
            mib=24,
        )(place, *toks, *mine, *up_x)

        def second_half(*refs):
            ups = grouped(refs[3:6]) + grouped(refs[6:9])
            pieces = [[(r, 0)] for r in refs[9:12]] + [[(refs[12], 0), (refs[13], 0)]]
            lower_body(cols, *refs[:3], ups, pieces, *refs[14:])

        keep0, away0, hidden = kernel_call(
            second_half,
            sizes + [jax.ShapeDtypeStruct((tokens, units), BF16)],
            scratch=[
                pltpu.VMEM((model, piece), BF16),
                pltpu.VMEM((tokens, piece), BF16),
                pltpu.VMEM((units, part), BF16),
            ],
            smem=1,
            n_in=14,
            mib=30,
        )(place, rows_x, early, *up_y, *up_xy, *whole, *down_xy[0])
        got0 = send(away0, c=1)

        def last_columns(hidden_ref, own_ref, x_ref, y_ref, r0_ref, r1_ref, keep, away, down_all):
            pieces = [[(r, part)] for r in (own_ref, x_ref, y_ref)]
            pieces.append([(r0_ref, 0), (r1_ref, 0)])
            down_product(keep, away, hidden_ref[...], pieces, down_all)

        keep1, away1 = kernel_call(
            last_columns, sizes, scratch=[pltpu.VMEM((units, part), BF16)], n_in=6
        )(hidden, *whole, *down_xy[1])
        got1 = send(away1, c=1)
        halves = []
        for k, (keep, got) in enumerate([(keep0, got0), (keep1, got1)]):
            near, held = kernel_call(
                fold_body,
                [
                    jax.ShapeDtypeStruct((n_b * own, part), BF16),
                    jax.ShapeDtypeStruct((n_b * own, part), F32),
                ],
                n_in=2,
            )(keep, got)
            near = send(near, flip=1)
            far = (held[own:] + near[own:].astype(F32)).astype(BF16)
            far = send(far, flip=2)
            total = stream[:, k * part : (k + 1) * part] + held[:own] + near[:own].astype(F32)
            total = total + far.astype(F32)
            halves.append(total.astype(BF16))
        return jnp.concatenate(halves, axis=1)


    return jax.shard_map(on_device, **specs)
```

```python
import jax
import jax.numpy as jnp
from jax import lax
from jax.experimental import pallas as pl
from jax.experimental.pallas import tpu as pltpu
from jax.sharding import PartitionSpec as P


HEAD = 128
SUB = 64
EPS = 1e-06
HI = lax.Precision.HIGHEST
AXES = ("sp", "tp")
F32 = jnp.float32
BF16 = jnp.bfloat16


HEAD_K = 128
HEAD_V = 128
BLOCK = 64


def exact_parts(x):
    first = x.astype(BF16)
    rest = x - first.astype(F32)
    second = rest.astype(BF16)
    third = (rest - second.astype(F32)).astype(BF16)
    return first, second, third


def pack_logs(totals):
    lines = []
    for x in totals:
        lines += list(exact_parts(x))
    pad = 16 - len(lines)
    return jnp.concatenate(
        [x.astype(F32) for x in lines] + [jnp.zeros((pad, HEAD), F32)], axis=0
    ).astype(BF16)


def log_of(packed, heads, h):
    parts = packed[heads * HEAD :, :].astype(F32)
    return sum(parts[3 * h + k : 3 * h + k + 1, :] for k in range(3))


def as_column(row):
    return jnp.transpose(jnp.broadcast_to(row, (HEAD, HEAD)))


def gates_body(values, gates, logs, cum_out, packed):
    rows, width = gates.shape
    heads = width // HEAD
    gate, log_forget = gates[...], logs[...]
    r = lax.broadcasted_iota(jnp.int32, (rows, rows), 0)
    c = lax.broadcasted_iota(jnp.int32, (rows, rows), 1)
    lower = (r >= c).astype(F32)
    cum = jnp.dot(lower, log_forget, precision=HI, preferred_element_type=F32)
    cum_out[...] = cum
    total = cum[rows - 1 : rows, :]
    keys = gate * jnp.exp(total - cum)
    vals = values[...].astype(F32)
    for h in range(heads):
        ks = keys[:, h * HEAD : (h + 1) * HEAD]
        vs = vals[:, h * HEAD : (h + 1) * HEAD]
        state = lax.dot_general(
            ks, vs, (((0,), (0,)), ((), ())), precision=HI, preferred_element_type=F32
        )
        packed[h * HEAD : (h + 1) * HEAD, :] = state.astype(BF16)
    packed[heads * HEAD :, :] = pack_logs([total[:, h * HEAD : (h + 1) * HEAD] for h in range(heads)])


def local_body(query, gate, cum, values, out):
    rows, width = query.shape
    sub = min(SUB, rows)
    for h in range(width // HEAD):
        lanes = slice(h * HEAD, (h + 1) * HEAD)
        for i in range(rows // sub):
            lo, hi = i * sub, (i + 1) * sub
            mid = cum[lo + sub // 2 - 1 : lo + sub // 2, lanes]
            qs = query[lo:hi, lanes].astype(F32) * (HEAD**-0.5) * jnp.exp(cum[lo:hi, lanes] - mid)
            ks = gate[0:hi, lanes] * jnp.exp(mid - cum[0:hi, lanes])
            scores = lax.dot_general(
                qs, ks, (((1,), (1,)), ((), ())), precision=HI, preferred_element_type=F32
            )
            rr = lax.broadcasted_iota(jnp.int32, (sub, hi), 0) + lo
            cc = lax.broadcasted_iota(jnp.int32, (sub, hi), 1)
            scores = jnp.where(rr >= cc, scores, 0.0)
            out[lo:hi, lanes] = jnp.dot(
                scores, values[0:hi, lanes].astype(F32), precision=HI, preferred_element_type=F32
            )


def kernel_call(body, out_shape, scratch=(), smem=0, n_in=0, mib=16):
    specs = [pl.BlockSpec(memory_space=pltpu.SMEM)] * smem
    specs += [pl.BlockSpec(memory_space=pltpu.VMEM)] * (n_in - smem)
    many = isinstance(out_shape, (list, tuple))
    out_spec = pl.BlockSpec(memory_space=pltpu.VMEM)
    return pl.pallas_call(
        body,
        out_shape=out_shape,
        in_specs=specs,
        out_specs=[out_spec] * len(out_shape) if many else out_spec,
        scratch_shapes=list(scratch),
        compiler_params=pltpu.CompilerParams(vmem_limit_bytes=mib * 1024 * 1024),
    )


def pair_body(place, mine, theirs, out):
    last = place[1] == 1
    heads = (mine.shape[0] - 16) // HEAD
    logs = []
    for h in range(heads):
        rows = slice(h * HEAD, (h + 1) * HEAD)
        own_log, their_log = log_of(mine, heads, h), log_of(theirs, heads, h)
        own_state, their_state = mine[rows, :].astype(F32), theirs[rows, :].astype(F32)
        decay = as_column(jnp.exp(jnp.where(last, own_log, their_log)))
        early = jnp.where(last, their_state, own_state)
        late = jnp.where(last, own_state, their_state)
        out[rows, :] = (decay * early + late).astype(BF16)
        logs.append(own_log + their_log)
    out[heads * HEAD :, :] = pack_logs(logs)


def mix_body(n_cores, *refs):
    place = refs[0]
    query, cum, local, gate_logits, gain, weight, beside = refs[1:8]
    states = refs[8:-4]
    first, second, away, mixed = refs[-4:]
    rows, width = query.shape
    heads = width // HEAD
    last = place[1] == 1
    for h in range(heads):
        lanes = slice(h * HEAD, (h + 1) * HEAD)
        arrived = jnp.where(last, beside[lanes, :].astype(F32), 0.0)
        passed = jnp.where(last, log_of(beside, heads, h), 0.0)
        for s in states:
            arrived = arrived + as_column(jnp.exp(passed)) * s[lanes, :].astype(F32)
            passed = passed + log_of(s, heads, h)
        reach = query[:, lanes].astype(F32) * (HEAD**-0.5) * jnp.exp(cum[:, lanes])
        rec = local[:, lanes] + jnp.dot(reach, arrived, precision=HI, preferred_element_type=F32)
        scale = lax.rsqrt(jnp.mean(rec * rec, axis=-1, keepdims=True) + EPS)
        v = gate_logits[:, lanes].astype(F32)
        mixed[:, lanes] = rec * scale * gain[...] * (v / (1.0 + jnp.exp(-v)))
    y, c = place[2], place[3]
    n_y = 2
    own = rows // (n_y * n_cores)
    picked = []
    for e in range(n_cores):
        for k in range(n_y):
            t = lax.rem(y + k, n_y) * n_cores + lax.rem(c + e, n_cores)
            picked.append(mixed[pl.ds(pl.multiple_of(t * own, own), own), :])
    ordered = jnp.concatenate(picked, axis=0).astype(BF16)
    part = jnp.dot(ordered, weight[...], preferred_element_type=F32)
    first[...] = part[:own]
    second[...] = part[own : n_y * own]
    away[...] = part[n_y * own :].astype(BF16)


def norm_body(own, beside, arrived, residual, gain, stream_out, normed_out):
    rows = own.shape[0]
    stream = own[...] + beside[:rows, :].astype(F32) + arrived[...].astype(F32)
    stream = stream + residual[...].astype(F32)
    stream_out[...] = stream
    scale = lax.rsqrt(jnp.mean(stream * stream, axis=-1, keepdims=True) + EPS)
    normed = (stream * scale * gain[...]).astype(BF16)
    blocks, _, cols = normed_out.shape
    for i in range(blocks):
        normed_out[i] = normed[:, i * cols : (i + 1) * cols]


def hidden_half(rows_x, ups, up_all, cols, out):
    at = 0
    for src, off in ups:
        up_all[at : at + cols, :] = src[off : off + cols, :]
        at += cols
    act = jnp.maximum(jnp.dot(rows_x[...], up_all[...], preferred_element_type=F32), 0.0)
    out[...] = (act * act).astype(BF16)


def first_body(n_a, n_cores, place, toks, ups, rows_x, hidden, up_all):
    a, b = place[0], place[1]
    n_b = len(ups) // n_a
    _, own, cols = toks[0].shape
    for i in range(n_a * n_cores):
        for x in range(n_b):
            for e in range(n_a):
                k = lax.rem(a - e + n_a, n_a) * n_b + lax.rem(b + x, n_b)
                at = (x * n_a + e) * cols
                rows_x[i * own : (i + 1) * own, at : at + cols] = toks[i][k]
    hidden_half(rows_x, ups, up_all, cols, hidden)


def down_product(keep, away, units, pieces, down_all):
    at = 0
    for group in pieces:
        for piece in group:
            src, off = piece
            n = src.shape[0]
            down_all[at : at + n, :] = src[:, off : off + down_all.shape[1]]
            at += n
    acc = jnp.dot(units, down_all[...], preferred_element_type=F32)
    cut = keep.shape[0]
    keep[...] = acc[:cut]
    away[...] = acc[cut:].astype(BF16)


def lower_body(cols, place, rows_x, early, ups, pieces, keep, away, ordered, up_all, late, down_all):
    hidden_half(rows_x, ups, up_all, cols, late)
    n_b = 2
    b = place[1]
    half = late.shape[1] // n_b
    for y, src in enumerate((early, late)):
        for x in range(n_b):
            k = lax.rem(b + x, n_b)
            at = (y * n_b + x) * half
            ordered[:, at : at + half] = src[:, pl.ds(pl.multiple_of(k * half, half), half)]
    down_product(keep, away, ordered[...], pieces, down_all)


def fold_body(keep, got, near, held):
    rows = near.shape[0] // 2
    for k in range(2):
        for out, block in ((held, 2 * k), (near, 2 * k + 1)):
            src = slice(block * rows, (block + 1) * rows)
            both = keep[src, :] + got[src, :].astype(F32)
            out[k * rows : (k + 1) * rows, :] = both.astype(out.dtype)


norm_eps = 1e-06
highest_precision = lax.Precision.HIGHEST


def carried_in(part, axis, combine, identity):
    place = lax.axis_index(axis)
    gathered = jax.tree.map(lambda a: lax.all_gather(a, axis), part)
    state = jax.tree.map(lambda a, e: jnp.zeros_like(a) + jnp.asarray(e, a.dtype), part, identity)

    def one(step, state):
        return combine(
            state, jax.tree.map(lambda a: lax.dynamic_index_in_dim(a, step, 0, False), gathered)
        )

    return lax.fori_loop(0, place, one, state)


def block_update(carry_forward_state, block_inputs):
    query_rows_block, gate_rows_block, value_rows_block, log_block = block_inputs
    cumulative_log = jnp.cumsum(log_block, axis=1)
    length = query_rows_block.shape[1]
    causal = jnp.arange(length)[:, None] >= jnp.arange(length)[None, :]
    across_blocks = jnp.einsum(
        "dcj,djw->dcw",
        query_rows_block * jnp.exp(cumulative_log),
        carry_forward_state,
        precision=highest_precision,
    )
    spread = cumulative_log[:, :, None, :] - cumulative_log[:, None, :, :]
    decay_table = jnp.exp(jnp.where(causal[None, :, :, None], spread, -jnp.inf))
    scores = jnp.einsum(
        "htk,hsk,htsk->hts",
        query_rows_block,
        gate_rows_block,
        decay_table,
        precision=highest_precision,
    )
    within = jnp.einsum("hts,hsv->htv", scores, value_rows_block, precision=highest_precision)
    final_log_total = cumulative_log[:, -1:, :]
    updated_state = jnp.exp(final_log_total[:, 0, :])[
        :, :, None
    ] * carry_forward_state + jnp.einsum(
        "tri,trw->tiw",
        gate_rows_block * jnp.exp(final_log_total - cumulative_log),
        value_rows_block,
        precision=highest_precision,
    )
    return (updated_state, across_blocks + within)


def to_blocks(array, inner):
    length = array.shape[0]
    split_up = array.reshape(length // BLOCK, BLOCK, array.shape[1] // inner, inner)
    return jnp.transpose(split_up, (0, 2, 1, 3))


def from_blocks(blocked):
    joined = jnp.transpose(blocked, (0, 2, 1, 3))
    return joined.reshape(joined.shape[0] * joined.shape[1], joined.shape[2], joined.shape[3])


def prepare_inputs(query, forget_logits, written_values, forget_floor_gap, extra_log_decay):
    input_gate_value = forget_floor_gap[None, :] * jax.nn.sigmoid(
        -forget_logits.astype(jnp.float32)
    )
    forget_log_rate = jnp.log1p(-input_gate_value) + extra_log_decay
    scaled_values = query.astype(jnp.float32) * HEAD_K ** (-0.5)
    return (scaled_values, input_gate_value, written_values.astype(jnp.float32), forget_log_rate)


def gate_out(recurrent, output_gate_logits, head_norm_gain):
    normal_part = recurrent * lax.rsqrt(
        jnp.mean(recurrent * recurrent, axis=-1, keepdims=True) + norm_eps
    )
    gating = jax.nn.silu(output_gate_logits.astype(jnp.float32)).reshape(recurrent.shape)
    mixed = normal_part * head_norm_gain * gating
    return mixed.reshape(recurrent.shape[0], -1).astype(jnp.bfloat16)


def normalize(stream, gain):
    scaled_rows = stream * lax.rsqrt(jnp.mean(stream * stream, axis=-1, keepdims=True) + norm_eps)
    return (scaled_rows * gain).astype(jnp.bfloat16)


def chain_states(earlier, later):
    return (earlier[0] + later[0], jnp.exp(later[0])[:, :, None] * earlier[1] + later[1])


def gathered_plan(
    query,
    forget_logits,
    written_values,
    output_gate_logits,
    forget_floor_gap,
    extra_log_decay,
    head_norm_gain,
    output_weight,
    residual,
    mixer_norm_gain,
    mixer_up_weight,
    mixer_down_weight,
):
    scaled_values, input_gate_value, value_rows, forget_log_rate = prepare_inputs(
        query, forget_logits, written_values, forget_floor_gap, extra_log_decay
    )
    row_count, local_width = query.shape
    head_count = local_width // HEAD_K
    start_state = jnp.zeros((head_count, HEAD_K, HEAD_V), jnp.float32)
    local_state, blocked = lax.scan(
        block_update,
        start_state,
        (
            to_blocks(scaled_values, HEAD_K),
            to_blocks(input_gate_value, HEAD_K),
            to_blocks(value_rows, HEAD_V),
            to_blocks(forget_log_rate, HEAD_K),
        ),
    )
    log_total = jnp.sum(forget_log_rate, axis=0).reshape(head_count, HEAD_K)
    arrived_state = carried_in(
        (log_total, local_state),
        "sp",
        chain_states,
        (jnp.zeros_like(log_total), jnp.zeros_like(local_state)),
    )
    running = jnp.cumsum(forget_log_rate, axis=0)
    reached_state = (scaled_values * jnp.exp(running)).reshape(row_count, head_count, HEAD_K)
    carried_over = jnp.einsum(
        "cja,jae->cje", reached_state, arrived_state[1], precision=highest_precision
    )
    mixed = gate_out(from_blocks(blocked) + carried_over, output_gate_logits, head_norm_gain)
    stream_own = lax.psum_scatter(
        jnp.dot(mixed, output_weight, preferred_element_type=jnp.float32).astype(jnp.bfloat16),
        "tp",
        scatter_dimension=0,
        tiled=True,
    ).astype(jnp.float32) + residual.astype(jnp.float32)
    normed = lax.all_gather(normalize(stream_own, mixer_norm_gain), "tp", axis=0, tiled=True)
    columns = normed
    lifted = jnp.dot(
        columns,
        lax.all_gather(mixer_up_weight, "sp", axis=0, tiled=True),
        preferred_element_type=jnp.float32,
    )
    hidden = jnp.square(jax.nn.relu(lifted)).astype(jnp.bfloat16)
    columns = hidden
    projected = jnp.dot(
        columns,
        lax.all_gather(mixer_down_weight, "sp", axis=0, tiled=True),
        preferred_element_type=jnp.float32,
    )
    mlp_own = lax.psum_scatter(
        projected.astype(jnp.bfloat16), "tp", scatter_dimension=0, tiled=True
    ).astype(jnp.float32)
    return (stream_own + mlp_own).astype(jnp.bfloat16)


def solution(mesh):
    specs = dict(
        mesh=mesh,
        in_specs=(
            P("sp", "tp"),
            P("sp", "tp"),
            P("sp", "tp"),
            P("sp", "tp"),
            P("tp"),
            P("sp", "tp"),
            P(),
            P("tp", None),
            P(("sp", "tp"), None),
            P(),
            P("sp", "tp"),
            P(("tp", "sp"), None),
        ),
        out_specs=P(("sp", "tp"), None),
        check_vma=False,
    )
    n_sp, n_tp = mesh.shape["sp"], mesh.shape["tp"]
    n_b, n_y = 2, 2
    n_a, n_c = n_sp // n_b, n_tp // n_y
    if n_sp % n_b or n_tp % n_y or n_a != 4 or n_c != 2:
        return jax.shard_map(gathered_plan, **specs)

    def flat(a, b, y, c):
        return (a % n_a * n_b + b % n_b) * n_tp + y % n_y * n_c + c % n_c

    def send(x, a=0, b=0, y=0, c=0, flip=0, cyclic=True):
        pairs = [
            (flat(i, j, k, m), flat((i ^ flip) + a, j + b, k + y, m + c))
            for i in range(n_a)
            for j in range(n_b)
            for k in range(n_y)
            for m in range(n_c)
            if cyclic or i + a < n_a
        ]
        return lax.ppermute(x, AXES, pairs)

    def on_device(
        query,
        forget_logits,
        written_values,
        output_gate_logits,
        forget_floor_gap,
        extra_log_decay,
        head_norm_gain,
        output_weight,
        residual,
        mixer_norm_gain,
        mixer_up_weight,
        mixer_down_weight,
    ):
        sp, tp = lax.axis_index("sp"), lax.axis_index("tp")
        a, b, y, c = sp // n_b, sp % n_b, tp // n_c, tp % n_c
        place = jnp.stack([a, b, y, c]).astype(jnp.int32)
        rows, width = query.shape
        model = output_weight.shape[1]
        own = residual.shape[0]
        heads = width // HEAD

        packed_shape = jax.ShapeDtypeStruct((heads * HEAD + 16, HEAD), BF16)
        gate = forget_floor_gap[None, :] * jax.nn.sigmoid(-forget_logits.astype(F32))
        log_forget = jnp.log1p(-gate) + extra_log_decay
        cum, packed = kernel_call(
            gates_body, [jax.ShapeDtypeStruct((rows, width), F32), packed_shape], n_in=3
        )(written_values, gate, log_forget)

        up_rows, up_cols = mixer_up_weight.shape
        piece = up_cols // n_a
        mine = []
        for d in range(n_a):
            start = (0, (a + d) % n_a * piece)
            cut = lax.dynamic_slice(mixer_up_weight, start, (up_rows, piece))
            mine.append(cut if d == 0 else send(cut, a=d))

        def grouped(refs):
            return [(refs[0], 0), (refs[2], 0), (refs[1], 0), (refs[2], up_rows)]

        part = model // 2
        half = mixer_down_weight.shape[0] // 2
        down_x = send(mixer_down_weight, b=1)
        down_y = send(mixer_down_weight, y=1)
        down_xy = []
        for k in range(2):
            lanes = slice(k * part, (k + 1) * part)
            cut = half if k else half // 2
            down_xy.append([send(down_x[:cut, lanes], y=1), send(down_y[cut:, lanes], b=1)])
        whole = [mixer_down_weight, down_x, down_y]

        beside = send(packed, b=1)
        pair = kernel_call(pair_body, packed_shape, smem=1, n_in=3)(place, packed, beside)
        states = [send(pair, a=d, cyclic=False) for d in range(1, n_a)]
        local = kernel_call(
            local_body, jax.ShapeDtypeStruct((rows, width), F32), n_in=4
        )(query, gate, cum, written_values)
        first, second, away = kernel_call(
            lambda *refs: mix_body(n_c, *refs),
            [
                jax.ShapeDtypeStruct((own, model), F32),
                jax.ShapeDtypeStruct((own, model), F32),
                jax.ShapeDtypeStruct((n_y * own, model), BF16),
            ],
            scratch=[pltpu.VMEM((rows, width), F32)],
            smem=1,
            n_in=8 + len(states),
        )(
            place,
            query,
            cum,
            local,
            output_gate_logits,
            head_norm_gain[None, :],
            output_weight,
            beside,
            *states,
        )
        got = send(away, c=1)
        second = (second + got[own:].astype(F32)).astype(BF16)
        other = send(second, y=1)
        stream, normed = kernel_call(
            norm_body,
            [
                jax.ShapeDtypeStruct((own, model), F32),
                jax.ShapeDtypeStruct((n_sp, own, model // n_sp), BF16),
            ],
            n_in=5,
        )(first, got, other, residual, mixer_norm_gain[None, :])

        late = lax.optimization_barrier((mine[1], mine[3], normed))[:2]
        up_x, up_y = [], []
        for members in [mine[0], mine[2], jnp.concatenate(late, axis=0)]:
            up_x.append(send(members, b=1))
            up_y.append(send(members, y=1))
        up_xy = [
            send(up_y[0], b=1),
            send(up_x[1], y=1),
            send(up_y[2][:up_rows], b=1),
            send(up_x[2][up_rows:], y=1),
        ]

        line = [normed] + [send(normed, flip=d) for d in range(1, n_a)]
        toks = line + [send(u, c=1) for u in line]
        group = n_a * own
        tokens = n_c * group
        units = n_y * piece
        cols = model // n_sp
        sizes = [
            jax.ShapeDtypeStruct((group, part), F32),
            jax.ShapeDtypeStruct((tokens - group, part), BF16),
        ]

        def first_half(*refs):
            t = 1 + len(toks)
            ups = [(refs[t + e], 0) for e in range(n_a)] + grouped(refs[t + n_a : t + n_a + 3])
            first_body(n_a, n_c, refs[0], refs[1:t], ups, *refs[-3:])

        rows_x, early = kernel_call(
            first_half,
            [
                jax.ShapeDtypeStruct((tokens, model), BF16),
                jax.ShapeDtypeStruct((tokens, piece), BF16),
            ],
            scratch=[pltpu.VMEM((model, piece), BF16)],
            smem=1,
            n_in=1 + len(toks) + n_a + 3,
            mib=24,
        )(place, *toks, *mine, *up_x)

        def second_half(*refs):
            ups = grouped(refs[3:6]) + [(refs[6 + k], 0) for k in (0, 2, 1, 3)]
            pieces = [[(r, 0)] for r in refs[10:13]] + [[(refs[13], 0), (refs[14], 0)]]
            lower_body(cols, *refs[:3], ups, pieces, *refs[15:])

        keep0, away0, hidden = kernel_call(
            second_half,
            sizes + [jax.ShapeDtypeStruct((tokens, units), BF16)],
            scratch=[
                pltpu.VMEM((model, piece), BF16),
                pltpu.VMEM((tokens, piece), BF16),
                pltpu.VMEM((units, part), BF16),
            ],
            smem=1,
            n_in=15,
            mib=30,
        )(place, rows_x, early, *up_y, *up_xy, *whole, *down_xy[0])
        got0 = send(away0, c=1)

        def last_columns(hidden_ref, own_ref, x_ref, y_ref, r0_ref, r1_ref, keep, away, down_all):
            pieces = [[(r, part)] for r in (own_ref, x_ref, y_ref)]
            pieces.append([(r0_ref, 0), (r1_ref, 0)])
            down_product(keep, away, hidden_ref[...], pieces, down_all)

        keep1, away1 = kernel_call(
            last_columns, sizes, scratch=[pltpu.VMEM((units, part), BF16)], n_in=6
        )(hidden, *whole, *down_xy[1])
        got1 = send(away1, c=1)
        halves = []
        for k, (keep, got) in enumerate([(keep0, got0), (keep1, got1)]):
            near, held = kernel_call(
                fold_body,
                [
                    jax.ShapeDtypeStruct((n_b * own, part), BF16),
                    jax.ShapeDtypeStruct((n_b * own, part), F32),
                ],
                n_in=2,
            )(keep, got)
            near = send(near, flip=1)
            far = (held[own:] + near[own:].astype(F32)).astype(BF16)
            far = send(far, flip=2)
            total = stream[:, k * part : (k + 1) * part] + held[:own] + near[:own].astype(F32)
            total = total + far.astype(F32)
            halves.append(total.astype(BF16))
        return jnp.concatenate(halves, axis=1)


    return jax.shard_map(on_device, **specs)
```

```python
import jax
import jax.numpy as jnp
from jax import lax
from jax.experimental import pallas as pl
from jax.experimental.pallas import tpu as pltpu
from jax.sharding import PartitionSpec as P


HEAD = 128
SUB = 64
EPS = 1e-06
HI = lax.Precision.HIGHEST
AXES = ("sp", "tp")
F32 = jnp.float32
BF16 = jnp.bfloat16


HEAD_K = 128
HEAD_V = 128
BLOCK = 64


def exact_parts(x):
    first = x.astype(BF16)
    rest = x - first.astype(F32)
    second = rest.astype(BF16)
    third = (rest - second.astype(F32)).astype(BF16)
    return first, second, third


def pack_logs(totals):
    lines = []
    for x in totals:
        lines += list(exact_parts(x))
    pad = 16 - len(lines)
    return jnp.concatenate(
        [x.astype(F32) for x in lines] + [jnp.zeros((pad, HEAD), F32)], axis=0
    ).astype(BF16)


def log_of(packed, heads, h):
    parts = packed[heads * HEAD :, :].astype(F32)
    return sum(parts[3 * h + k : 3 * h + k + 1, :] for k in range(3))


def as_column(row):
    return jnp.transpose(jnp.broadcast_to(row, (HEAD, HEAD)))


def gates_body(values, gates, logs, cum_out, packed):
    rows, width = gates.shape
    heads = width // HEAD
    gate, log_forget = gates[...], logs[...]
    r = lax.broadcasted_iota(jnp.int32, (rows, rows), 0)
    c = lax.broadcasted_iota(jnp.int32, (rows, rows), 1)
    lower = (r >= c).astype(F32)
    cum = jnp.dot(lower, log_forget, precision=HI, preferred_element_type=F32)
    cum_out[...] = cum
    total = cum[rows - 1 : rows, :]
    keys = gate * jnp.exp(total - cum)
    vals = values[...].astype(F32)
    for h in range(heads):
        ks = keys[:, h * HEAD : (h + 1) * HEAD]
        vs = vals[:, h * HEAD : (h + 1) * HEAD]
        state = lax.dot_general(
            ks, vs, (((0,), (0,)), ((), ())), precision=HI, preferred_element_type=F32
        )
        packed[h * HEAD : (h + 1) * HEAD, :] = state.astype(BF16)
    packed[heads * HEAD :, :] = pack_logs([total[:, h * HEAD : (h + 1) * HEAD] for h in range(heads)])


def local_body(query, gate, cum, values, out):
    rows, width = query.shape
    sub = min(SUB, rows)
    for h in range(width // HEAD):
        lanes = slice(h * HEAD, (h + 1) * HEAD)
        for i in range(rows // sub):
            lo, hi = i * sub, (i + 1) * sub
            mid = cum[lo + sub // 2 - 1 : lo + sub // 2, lanes]
            qs = query[lo:hi, lanes].astype(F32) * (HEAD**-0.5) * jnp.exp(cum[lo:hi, lanes] - mid)
            ks = gate[0:hi, lanes] * jnp.exp(mid - cum[0:hi, lanes])
            scores = lax.dot_general(
                qs, ks, (((1,), (1,)), ((), ())), precision=HI, preferred_element_type=F32
            )
            rr = lax.broadcasted_iota(jnp.int32, (sub, hi), 0) + lo
            cc = lax.broadcasted_iota(jnp.int32, (sub, hi), 1)
            scores = jnp.where(rr >= cc, scores, 0.0)
            out[lo:hi, lanes] = jnp.dot(
                scores, values[0:hi, lanes].astype(F32), precision=HI, preferred_element_type=F32
            )


def kernel_call(body, out_shape, scratch=(), smem=0, n_in=0, mib=16):
    specs = [pl.BlockSpec(memory_space=pltpu.SMEM)] * smem
    specs += [pl.BlockSpec(memory_space=pltpu.VMEM)] * (n_in - smem)
    many = isinstance(out_shape, (list, tuple))
    out_spec = pl.BlockSpec(memory_space=pltpu.VMEM)
    return pl.pallas_call(
        body,
        out_shape=out_shape,
        in_specs=specs,
        out_specs=[out_spec] * len(out_shape) if many else out_spec,
        scratch_shapes=list(scratch),
        compiler_params=pltpu.CompilerParams(vmem_limit_bytes=mib * 1024 * 1024),
    )


def pair_body(place, mine, theirs, out):
    last = place[1] == 1
    heads = (mine.shape[0] - 16) // HEAD
    logs = []
    for h in range(heads):
        rows = slice(h * HEAD, (h + 1) * HEAD)
        own_log, their_log = log_of(mine, heads, h), log_of(theirs, heads, h)
        own_state, their_state = mine[rows, :].astype(F32), theirs[rows, :].astype(F32)
        decay = as_column(jnp.exp(jnp.where(last, own_log, their_log)))
        early = jnp.where(last, their_state, own_state)
        late = jnp.where(last, own_state, their_state)
        out[rows, :] = (decay * early + late).astype(BF16)
        logs.append(own_log + their_log)
    out[heads * HEAD :, :] = pack_logs(logs)


def mix_body(n_cores, *refs):
    place = refs[0]
    query, cum, local, gate_logits, gain, weight, beside = refs[1:8]
    states = refs[8:-4]
    first, second, away, mixed = refs[-4:]
    rows, width = query.shape
    heads = width // HEAD
    last = place[1] == 1
    for h in range(heads):
        lanes = slice(h * HEAD, (h + 1) * HEAD)
        arrived = jnp.where(last, beside[lanes, :].astype(F32), 0.0)
        passed = jnp.where(last, log_of(beside, heads, h), 0.0)
        for s in states:
            arrived = arrived + as_column(jnp.exp(passed)) * s[lanes, :].astype(F32)
            passed = passed + log_of(s, heads, h)
        reach = query[:, lanes].astype(F32) * (HEAD**-0.5) * jnp.exp(cum[:, lanes])
        rec = local[:, lanes] + jnp.dot(reach, arrived, precision=HI, preferred_element_type=F32)
        scale = lax.rsqrt(jnp.mean(rec * rec, axis=-1, keepdims=True) + EPS)
        v = gate_logits[:, lanes].astype(F32)
        mixed[:, lanes] = rec * scale * gain[...] * (v / (1.0 + jnp.exp(-v)))
    y, c = place[2], place[3]
    n_y = 2
    own = rows // (n_y * n_cores)
    picked = []
    for e in range(n_cores):
        for k in range(n_y):
            t = lax.rem(y + k, n_y) * n_cores + lax.rem(c + e, n_cores)
            picked.append(mixed[pl.ds(pl.multiple_of(t * own, own), own), :])
    ordered = jnp.concatenate(picked, axis=0).astype(BF16)
    part = jnp.dot(ordered, weight[...], preferred_element_type=F32)
    first[...] = part[:own]
    second[...] = part[own : n_y * own]
    away[...] = part[n_y * own :].astype(BF16)


def norm_body(own, beside, arrived, residual, gain, stream_out, normed_out):
    rows = own.shape[0]
    stream = own[...] + beside[:rows, :].astype(F32) + arrived[...].astype(F32)
    stream = stream + residual[...].astype(F32)
    stream_out[...] = stream
    scale = lax.rsqrt(jnp.mean(stream * stream, axis=-1, keepdims=True) + EPS)
    normed = (stream * scale * gain[...]).astype(BF16)
    blocks, _, cols = normed_out.shape
    for i in range(blocks):
        normed_out[i] = normed[:, i * cols : (i + 1) * cols]


def hidden_half(rows_x, ups, up_all, cols, out):
    at = 0
    for src, off in ups:
        up_all[at : at + cols, :] = src[off : off + cols, :]
        at += cols
    act = jnp.maximum(jnp.dot(rows_x[...], up_all[...], preferred_element_type=F32), 0.0)
    out[...] = (act * act).astype(BF16)


def first_body(n_a, n_cores, place, toks, ups, rows_x, hidden, up_all):
    a, b = place[0], place[1]
    n_b = len(ups) // n_a
    _, own, cols = toks[0].shape
    for i in range(n_a * n_cores):
        for x in range(n_b):
            for e in range(n_a):
                k = lax.rem(a - e + n_a, n_a) * n_b + lax.rem(b + x, n_b)
                at = (x * n_a + e) * cols
                rows_x[i * own : (i + 1) * own, at : at + cols] = toks[i][k]
    hidden_half(rows_x, ups, up_all, cols, hidden)


def down_product(keep, away, units, pieces, down_all):
    at = 0
    for group in pieces:
        for piece in group:
            src, off = piece
            n = src.shape[0]
            down_all[at : at + n, :] = src[:, off : off + down_all.shape[1]]
            at += n
    acc = jnp.dot(units, down_all[...], preferred_element_type=F32)
    cut = keep.shape[0]
    keep[...] = acc[:cut]
    away[...] = acc[cut:].astype(BF16)


def lower_body(cols, place, rows_x, early, ups, pieces, keep, away, ordered, up_all, late, down_all):
    hidden_half(rows_x, ups, up_all, cols, late)
    n_b = 2
    b = place[1]
    half = late.shape[1] // n_b
    for y, src in enumerate((early, late)):
        for x in range(n_b):
            k = lax.rem(b + x, n_b)
            at = (y * n_b + x) * half
            ordered[:, at : at + half] = src[:, pl.ds(pl.multiple_of(k * half, half), half)]
    down_product(keep, away, ordered[...], pieces, down_all)


def fold_body(keep, got, near, held):
    rows = near.shape[0] // 2
    for k in range(2):
        for out, block in ((held, 2 * k), (near, 2 * k + 1)):
            src = slice(block * rows, (block + 1) * rows)
            both = keep[src, :] + got[src, :].astype(F32)
            out[k * rows : (k + 1) * rows, :] = both.astype(out.dtype)


norm_eps = 1e-06
highest_precision = lax.Precision.HIGHEST


def carried_in(part, axis, combine, identity):
    place = lax.axis_index(axis)
    gathered = jax.tree.map(lambda a: lax.all_gather(a, axis), part)
    state = jax.tree.map(lambda a, e: jnp.zeros_like(a) + jnp.asarray(e, a.dtype), part, identity)

    def one(step, state):
        return combine(
            state, jax.tree.map(lambda a: lax.dynamic_index_in_dim(a, step, 0, False), gathered)
        )

    return lax.fori_loop(0, place, one, state)


def block_update(carry_forward_state, block_inputs):
    query_rows_block, gate_rows_block, value_rows_block, log_block = block_inputs
    cumulative_log = jnp.cumsum(log_block, axis=1)
    length = query_rows_block.shape[1]
    causal = jnp.arange(length)[:, None] >= jnp.arange(length)[None, :]
    across_blocks = jnp.einsum(
        "dcj,djw->dcw",
        query_rows_block * jnp.exp(cumulative_log),
        carry_forward_state,
        precision=highest_precision,
    )
    spread = cumulative_log[:, :, None, :] - cumulative_log[:, None, :, :]
    decay_table = jnp.exp(jnp.where(causal[None, :, :, None], spread, -jnp.inf))
    scores = jnp.einsum(
        "htk,hsk,htsk->hts",
        query_rows_block,
        gate_rows_block,
        decay_table,
        precision=highest_precision,
    )
    within = jnp.einsum("hts,hsv->htv", scores, value_rows_block, precision=highest_precision)
    final_log_total = cumulative_log[:, -1:, :]
    updated_state = jnp.exp(final_log_total[:, 0, :])[
        :, :, None
    ] * carry_forward_state + jnp.einsum(
        "tri,trw->tiw",
        gate_rows_block * jnp.exp(final_log_total - cumulative_log),
        value_rows_block,
        precision=highest_precision,
    )
    return (updated_state, across_blocks + within)


def to_blocks(array, inner):
    length = array.shape[0]
    split_up = array.reshape(length // BLOCK, BLOCK, array.shape[1] // inner, inner)
    return jnp.transpose(split_up, (0, 2, 1, 3))


def from_blocks(blocked):
    joined = jnp.transpose(blocked, (0, 2, 1, 3))
    return joined.reshape(joined.shape[0] * joined.shape[1], joined.shape[2], joined.shape[3])


def prepare_inputs(query, forget_logits, written_values, forget_floor_gap, extra_log_decay):
    input_gate_value = forget_floor_gap[None, :] * jax.nn.sigmoid(
        -forget_logits.astype(jnp.float32)
    )
    forget_log_rate = jnp.log1p(-input_gate_value) + extra_log_decay
    scaled_values = query.astype(jnp.float32) * HEAD_K ** (-0.5)
    return (scaled_values, input_gate_value, written_values.astype(jnp.float32), forget_log_rate)


def gate_out(recurrent, output_gate_logits, head_norm_gain):
    normal_part = recurrent * lax.rsqrt(
        jnp.mean(recurrent * recurrent, axis=-1, keepdims=True) + norm_eps
    )
    gating = jax.nn.silu(output_gate_logits.astype(jnp.float32)).reshape(recurrent.shape)
    mixed = normal_part * head_norm_gain * gating
    return mixed.reshape(recurrent.shape[0], -1).astype(jnp.bfloat16)


def normalize(stream, gain):
    scaled_rows = stream * lax.rsqrt(jnp.mean(stream * stream, axis=-1, keepdims=True) + norm_eps)
    return (scaled_rows * gain).astype(jnp.bfloat16)


def chain_states(earlier, later):
    return (earlier[0] + later[0], jnp.exp(later[0])[:, :, None] * earlier[1] + later[1])


def gathered_plan(
    query,
    forget_logits,
    written_values,
    output_gate_logits,
    forget_floor_gap,
    extra_log_decay,
    head_norm_gain,
    output_weight,
    residual,
    mixer_norm_gain,
    mixer_up_weight,
    mixer_down_weight,
):
    scaled_values, input_gate_value, value_rows, forget_log_rate = prepare_inputs(
        query, forget_logits, written_values, forget_floor_gap, extra_log_decay
    )
    row_count, local_width = query.shape
    head_count = local_width // HEAD_K
    start_state = jnp.zeros((head_count, HEAD_K, HEAD_V), jnp.float32)
    local_state, blocked = lax.scan(
        block_update,
        start_state,
        (
            to_blocks(scaled_values, HEAD_K),
            to_blocks(input_gate_value, HEAD_K),
            to_blocks(value_rows, HEAD_V),
            to_blocks(forget_log_rate, HEAD_K),
        ),
    )
    log_total = jnp.sum(forget_log_rate, axis=0).reshape(head_count, HEAD_K)
    arrived_state = carried_in(
        (log_total, local_state),
        "sp",
        chain_states,
        (jnp.zeros_like(log_total), jnp.zeros_like(local_state)),
    )
    running = jnp.cumsum(forget_log_rate, axis=0)
    reached_state = (scaled_values * jnp.exp(running)).reshape(row_count, head_count, HEAD_K)
    carried_over = jnp.einsum(
        "cja,jae->cje", reached_state, arrived_state[1], precision=highest_precision
    )
    mixed = gate_out(from_blocks(blocked) + carried_over, output_gate_logits, head_norm_gain)
    stream_own = lax.psum_scatter(
        jnp.dot(mixed, output_weight, preferred_element_type=jnp.float32).astype(jnp.bfloat16),
        "tp",
        scatter_dimension=0,
        tiled=True,
    ).astype(jnp.float32) + residual.astype(jnp.float32)
    normed = lax.all_gather(normalize(stream_own, mixer_norm_gain), "tp", axis=0, tiled=True)
    columns = normed
    lifted = jnp.dot(
        columns,
        lax.all_gather(mixer_up_weight, "sp", axis=0, tiled=True),
        preferred_element_type=jnp.float32,
    )
    hidden = jnp.square(jax.nn.relu(lifted)).astype(jnp.bfloat16)
    columns = hidden
    projected = jnp.dot(
        columns,
        lax.all_gather(mixer_down_weight, "sp", axis=0, tiled=True),
        preferred_element_type=jnp.float32,
    )
    mlp_own = lax.psum_scatter(
        projected.astype(jnp.bfloat16), "tp", scatter_dimension=0, tiled=True
    ).astype(jnp.float32)
    return (stream_own + mlp_own).astype(jnp.bfloat16)


def solution(mesh):
    specs = dict(
        mesh=mesh,
        in_specs=(
            P("sp", "tp"),
            P("sp", "tp"),
            P("sp", "tp"),
            P("sp", "tp"),
            P("tp"),
            P("sp", "tp"),
            P(),
            P("tp", None),
            P(("sp", "tp"), None),
            P(),
            P("sp", "tp"),
            P(("tp", "sp"), None),
        ),
        out_specs=P(("sp", "tp"), None),
        check_vma=False,
    )
    n_sp, n_tp = mesh.shape["sp"], mesh.shape["tp"]
    n_b, n_y = 2, 2
    n_a, n_c = n_sp // n_b, n_tp // n_y
    if n_sp % n_b or n_tp % n_y or n_a != 4 or n_c != 2:
        return jax.shard_map(gathered_plan, **specs)

    def flat(a, b, y, c):
        return (a % n_a * n_b + b % n_b) * n_tp + y % n_y * n_c + c % n_c

    def send(x, a=0, b=0, y=0, c=0, flip=0, cyclic=True):
        pairs = [
            (flat(i, j, k, m), flat((i ^ flip) + a, j + b, k + y, m + c))
            for i in range(n_a)
            for j in range(n_b)
            for k in range(n_y)
            for m in range(n_c)
            if cyclic or i + a < n_a
        ]
        return lax.ppermute(x, AXES, pairs)

    def on_device(
        query,
        forget_logits,
        written_values,
        output_gate_logits,
        forget_floor_gap,
        extra_log_decay,
        head_norm_gain,
        output_weight,
        residual,
        mixer_norm_gain,
        mixer_up_weight,
        mixer_down_weight,
    ):
        sp, tp = lax.axis_index("sp"), lax.axis_index("tp")
        a, b, y, c = sp // n_b, sp % n_b, tp // n_c, tp % n_c
        place = jnp.stack([a, b, y, c]).astype(jnp.int32)
        rows, width = query.shape
        model = output_weight.shape[1]
        own = residual.shape[0]
        heads = width // HEAD

        packed_shape = jax.ShapeDtypeStruct((heads * HEAD + 16, HEAD), BF16)
        gate = forget_floor_gap[None, :] * jax.nn.sigmoid(-forget_logits.astype(F32))
        log_forget = jnp.log1p(-gate) + extra_log_decay
        cum, packed = kernel_call(
            gates_body, [jax.ShapeDtypeStruct((rows, width), F32), packed_shape], n_in=3
        )(written_values, gate, log_forget)

        up_rows, up_cols = mixer_up_weight.shape
        piece = up_cols // n_a
        mine = []
        for d in range(n_a):
            start = (0, (a + d) % n_a * piece)
            cut = lax.dynamic_slice(mixer_up_weight, start, (up_rows, piece))
            mine.append(cut if d == 0 else send(cut, a=d))

        def grouped(refs):
            return [(refs[0], 0), (refs[1], 0), (refs[2], 0), (refs[2], up_rows)]

        part = model // 2
        half = mixer_down_weight.shape[0] // 2
        down_x = send(mixer_down_weight, b=1)
        down_y = send(mixer_down_weight, y=1)
        down_xy = []
        for k in range(2):
            lanes = slice(k * part, (k + 1) * part)
            cut = half if k else half // 2
            down_xy.append([send(down_x[:cut, lanes], y=1), send(down_y[cut:, lanes], b=1)])
        whole = [mixer_down_weight, down_x, down_y]

        beside = send(packed, b=1)
        pair = kernel_call(pair_body, packed_shape, smem=1, n_in=3)(place, packed, beside)
        states = [send(pair, a=d, cyclic=False) for d in range(1, n_a)]
        local = kernel_call(
            local_body, jax.ShapeDtypeStruct((rows, width), F32), n_in=4
        )(query, gate, cum, written_values)
        first, second, away = kernel_call(
            lambda *refs: mix_body(n_c, *refs),
            [
                jax.ShapeDtypeStruct((own, model), F32),
                jax.ShapeDtypeStruct((own, model), F32),
                jax.ShapeDtypeStruct((n_y * own, model), BF16),
            ],
            scratch=[pltpu.VMEM((rows, width), F32)],
            smem=1,
            n_in=8 + len(states),
        )(
            place,
            query,
            cum,
            local,
            output_gate_logits,
            head_norm_gain[None, :],
            output_weight,
            beside,
            *states,
        )
        got = send(away, c=1)
        second = (second + got[own:].astype(F32)).astype(BF16)
        other = send(second, y=1)
        stream, normed = kernel_call(
            norm_body,
            [
                jax.ShapeDtypeStruct((own, model), F32),
                jax.ShapeDtypeStruct((n_sp, own, model // n_sp), BF16),
            ],
            n_in=5,
        )(first, got, other, residual, mixer_norm_gain[None, :])

        late = lax.optimization_barrier((mine[2], mine[3], normed))[:2]
        up_x, up_y = [], []
        for members in [mine[0], mine[1], jnp.concatenate(late, axis=0)]:
            up_x.append(send(members, b=1))
            up_y.append(send(members, y=1))
        up_xy = [send(up_x[0], y=1), send(up_x[1], y=1), send(up_y[2], b=1)]

        line = [normed] + [send(normed, flip=d) for d in range(1, n_a)]
        toks = line + [send(u, c=1) for u in line]
        group = n_a * own
        tokens = n_c * group
        units = n_y * piece
        cols = model // n_sp
        sizes = [
            jax.ShapeDtypeStruct((group, part), F32),
            jax.ShapeDtypeStruct((tokens - group, part), BF16),
        ]

        def first_half(*refs):
            t = 1 + len(toks)
            ups = [(refs[t + e], 0) for e in range(n_a)] + grouped(refs[t + n_a : t + n_a + 3])
            first_body(n_a, n_c, refs[0], refs[1:t], ups, *refs[-3:])

        rows_x, early = kernel_call(
            first_half,
            [
                jax.ShapeDtypeStruct((tokens, model), BF16),
                jax.ShapeDtypeStruct((tokens, piece), BF16),
            ],
            scratch=[pltpu.VMEM((model, piece), BF16)],
            smem=1,
            n_in=1 + len(toks) + n_a + 3,
            mib=24,
        )(place, *toks, *mine, *up_x)

        def second_half(*refs):
            ups = grouped(refs[3:6]) + grouped(refs[6:9])
            pieces = [[(r, 0)] for r in refs[9:12]] + [[(refs[12], 0), (refs[13], 0)]]
            lower_body(cols, *refs[:3], ups, pieces, *refs[14:])

        keep0, away0, hidden = kernel_call(
            second_half,
            sizes + [jax.ShapeDtypeStruct((tokens, units), BF16)],
            scratch=[
                pltpu.VMEM((model, piece), BF16),
                pltpu.VMEM((tokens, piece), BF16),
                pltpu.VMEM((units, part), BF16),
            ],
            smem=1,
            n_in=14,
            mib=30,
        )(place, rows_x, early, *up_y, *up_xy, *whole, *down_xy[0])
        got0 = send(away0, c=1)

        def last_columns(hidden_ref, own_ref, x_ref, y_ref, r0_ref, r1_ref, keep, away, down_all):
            pieces = [[(r, part)] for r in (own_ref, x_ref, y_ref)]
            pieces.append([(r0_ref, 0), (r1_ref, 0)])
            down_product(keep, away, hidden_ref[...], pieces, down_all)

        keep1, away1 = kernel_call(
            last_columns, sizes, scratch=[pltpu.VMEM((units, part), BF16)], n_in=6
        )(hidden, *whole, *down_xy[1])
        got1 = send(away1, c=1)
        halves = []
        for k, (keep, got) in enumerate([(keep0, got0), (keep1, got1)]):
            near, held = kernel_call(
                fold_body,
                [
                    jax.ShapeDtypeStruct((n_b * own, part), BF16),
                    jax.ShapeDtypeStruct((n_b * own, part), F32),
                ],
                n_in=2,
            )(keep, got)
            near = send(near, flip=1)
            far = (held[own:] + near[own:].astype(F32)).astype(BF16)
            far = send(far, flip=2)
            total = stream[:, k * part : (k + 1) * part] + held[:own] + near[:own].astype(F32)
            total = total + far.astype(F32)
            halves.append(total.astype(BF16))
        return jnp.concatenate(halves, axis=1)


    return jax.shard_map(on_device, **specs)
```
